32 devices in a mesh: grp: 2 (over y), tp: 4 (over z), dp: 4 (over x, core).
Axes of the slice: x: 2, y: 2, z: 4, core: 2. Of those that a mesh axis runs over, the one named last changes fastest.
Arguments:
- residual_slot_vectors: bfloat16 [128, 4, 4096], P('grp', None, 'dp'), parts along dimension 0, may hold values from -25 to 25
- active_counts: int32 [128], P(('grp', 'dp')), parts along dimension 0, may hold values from 1 to 4, 96 in all
- lookup_map: bfloat16 [2, 4096, 4096], P(None, 'dp', 'tp'), may hold values from -0.09375 to 0.09375
- address_map: bfloat16 [2, 4096, 4096], P(None, 'dp', 'tp'), may hold values from -0.09375 to 0.09375
- content_map: bfloat16 [2, 4096, 4096], P(None, 'dp', 'tp'), may hold values from -0.09375 to 0.09375
- result_valve_map: bfloat16 [2, 4096, 4096], P(None, 'dp', 'tp'), may hold values from -0.09375 to 0.09375
- fading_map_coefficients: bfloat16 [2, 4096, 64], replicated, may hold values from -0.09375 to 0.09375
- writing_intensity_map: bfloat16 [2, 4096, 64], replicated, may hold values from -0.09375 to 0.09375
- result_map: bfloat16 [2, 4096, 4096], P(None, 'tp', 'dp'), may hold values from -0.09375 to 0.09375
- fading_speed_exponent: float32 [2, 64], P(None, 'tp'), may hold values from 0 to 2.3
- fading_bias: float32 [2, 64], P(None, 'tp'), may hold values from -5 to -1
- entry_scaling: bfloat16 [2, 4096], P(None, 'dp'), may hold values from 0.099609375 to 1.8984375
- per_channel_scaling: bfloat16 [2, 64], replicated, may hold values from 0.099609375 to 1.8984375
- extra_shrink_exponent: float32 [2, 128, 4, 64], P(None, ('grp', 'dp'), None, 'tp'), parts along dimension 1, may hold values from -0.7 to 0
- memory_tensors: float32 [2, 128, 64, 4096], P(None, ('grp', 'dp'), None, 'tp'), parts along dimension 1, may hold values from -0.6 to 0.6
Outputs:
- mixed_tokens: bfloat16 [128, 4, 4096], P('grp', None, 'dp'), parts along dimension 0
- new_states: float32 [2, 128, 64, 4096], P(None, ('grp', 'dp'), None, 'tp'), parts along dimension 1
The draws below stay inside these ranges and needn't reach their ends.
There are 2 independent parts, one for each index of `grp`. The reference program is written for one: setup_inputs(seed, part) draws one part's arguments, and reference() takes and returns one part's arrays. A program takes and returns all parts, laid end to end along the dimension named above; an argument that names none is the same for every part. Nothing has to cross between parts.
Inputs may be any that keep to these rules, and one draw needn't show every extreme that they name: `active_counts`: every sequence has at least one live slot, at least one sequence has 4.
All inputs are finite; a program needn't handle non-finite values. No bound on the sum of `active_counts` on one device may be relied on, other than what follows from the above.
Results may differ from the reference program's by a relative error of at most 0.018.
Values may be sent and summed in bfloat16 or wider, within the bound.
A program may use at most 128 MiB of HBM per device.

```python
import math
import jax
import jax.numpy as jnp
import numpy as np
from jax import lax

D = 4096
HEADS = 64
HEAD = 64
BLOCKS = 2
NEW = 4
SEQS = 64
N_DP = 4


def draw_residual_slot_vectors(key, part):
    base_key, column_key = jax.random.split(jax.random.fold_in(key, 11), 2)
    column = jnp.arange(D, dtype=jnp.float32) / D
    rough = jnp.exp(jax.random.uniform(column_key, (D,), jnp.float32, -0.35, 0.35))
    scale = 0.5 * jnp.exp(column * math.log(6.0)) * rough
    values = jax.random.truncated_normal(base_key, -4.0, 4.0, (SEQS, NEW, D), jnp.float32)
    return (values * scale).astype(jnp.bfloat16)


def draw_extra_shrink_exponent(key, part):
    hit_key, depth_key = jax.random.split(jax.random.fold_in(key, 23))
    shape = (BLOCKS, SEQS, NEW, HEADS)
    hits = jax.random.bernoulli(hit_key, 0.1, shape)
    depth = jax.random.uniform(depth_key, shape, jnp.float32, -0.7, -0.22)
    return jnp.where(hits, depth, 0.0).astype(jnp.float32)


def block_scale(own_key, extent, shards, low, largest):
    def one(dim, parts):
        steps = jax.random.uniform(jax.random.fold_in(jax.random.fold_in(own_key, 6), dim), (parts,), jnp.float32, low / len(shards), largest / len(shards))
        return jnp.repeat(jnp.exp(steps), extent[dim] // parts).reshape((-1,) + (1,) * (len(extent) - dim - 1))

    gain = one(*shards[0])
    for cut in shards[1:]:
        gain = gain * one(*cut)
    return gain


def length_profile(count, total, most, lean):
    weights = [(1 << 20) // math.isqrt(rank ** lean) + 1 for rank in range(2, count + 1)]
    spare, holding = total - most - (count - 1), [1] * (count - 1)
    while spare > 0:
        candidates = [i for i in range(count - 1) if holding[i] < most]
        mass, left = sum([weights[i] for i in candidates]), spare
        for i in candidates:
            extra = min(most - holding[i], max(1, left * weights[i] // mass), spare)
            holding[i] = holding[i] + extra
            spare = spare - extra
    return np.array([most] + holding)


def ragged_sizes(rng, count, total, most, skew):
    if count == 2:
        one = jax.random.randint(rng, (), max(1, total - most), min(most, total - 1) + 1)
        return jnp.stack([one, total - one])
    tallies = jnp.asarray(length_profile(count, total, most, skew), jnp.int32)
    couples = (count - 1) // 2
    source_of, receiver = tallies[1:1 + 2 * couples:2], tallies[2:2 + 2 * couples:2]
    slack = jnp.minimum(source_of - 1, most - receiver)
    moved = jax.random.randint(jax.random.fold_in(rng, 1), (couples,), 0, 1 << 20) % (slack + 1)
    tallies = tallies.at[1:1 + 2 * couples:2].set(source_of - moved).at[2:2 + 2 * couples:2].set(receiver + moved)
    return tallies[jax.random.permutation(jax.random.fold_in(rng, 2), count)]


def scatter_about(key, extent, scale, most, cuts=(), kind=jnp.bfloat16):
    gain = block_scale(key, extent, cuts, -0.22, 0.18) if cuts else 1.0
    drawn = jax.random.normal(key, extent, jnp.float32) * scale * gain
    return jnp.minimum(jnp.maximum(drawn, -most), most).astype(kind)


def setup_inputs(seed: int = 0, part: int = 0) -> dict:
    splits = jax.random.split(jax.random.key(seed), 16)
    part_splits = jax.random.split(jax.random.fold_in(splits[15], part), 16)
    residual_slot_vectors = draw_residual_slot_vectors(jax.random.fold_in(jax.random.fold_in(splits[15], part), 71), part)
    active_counts = ragged_sizes(part_splits[1], SEQS, SEQS * 3 // 2, NEW, 1).astype(jnp.int32)
    lookup_map = scatter_about(splits[2], (BLOCKS, D, HEADS * HEAD), D ** -0.5, 0.09375, ((1, 4), (2, 4)))
    address_map = scatter_about(splits[3], (BLOCKS, D, HEADS * HEAD), D ** -0.5, 0.09375, ((1, 4), (2, 4)))
    content_map = scatter_about(splits[4], (BLOCKS, D, HEADS * HEAD), D ** -0.5, 0.09375, ((1, 4), (2, 4)))
    result_valve_map = scatter_about(splits[5], (BLOCKS, D, HEADS * HEAD), D ** -0.5, 0.09375, ((1, 4), (2, 4)))
    fading_map_coefficients = scatter_about(splits[6], (BLOCKS, D, HEADS), D ** -0.5, 0.09375)
    writing_intensity_map = scatter_about(splits[7], (BLOCKS, D, HEADS), D ** -0.5, 0.09375)
    result_map = scatter_about(splits[8], (BLOCKS, HEADS * HEAD, D), (HEADS * HEAD) ** -0.5, 0.09375, ((1, 4), (2, 4)))
    fading_speed_exponent = jnp.clip(2.3 * jax.random.uniform(splits[9], (BLOCKS, HEADS), jnp.float32) ** block_scale(splits[9], (BLOCKS, HEADS), ((1, 4),), -0.2, 0.2), 0.0, 2.3)
    fading_bias = jnp.clip(-5.0 + 4.0 * jax.random.uniform(splits[10], (BLOCKS, HEADS), jnp.float32) ** block_scale(splits[10], (BLOCKS, HEADS), ((1, 4),), -0.2, 0.2), -5.0, -1.0)
    entry_scaling = jnp.clip(1.0 + 0.18 * jax.random.normal(splits[11], (BLOCKS, D), jnp.float32), 0.099609375, 1.8984375).astype(jnp.bfloat16)
    per_channel_scaling = jnp.clip(1.0 + 0.18 * jax.random.normal(splits[12], (BLOCKS, HEAD), jnp.float32), 0.099609375, 1.8984375).astype(jnp.bfloat16)
    extra_shrink_exponent = draw_extra_shrink_exponent(jax.random.fold_in(jax.random.fold_in(splits[15], part), 71), part)
    memory_tensors = scatter_about(part_splits[14], (BLOCKS, SEQS, HEAD, HEADS * HEAD), 0.1, 0.6, ((1, 4), (3, 4)), jnp.float32)
    return dict(residual_slot_vectors=residual_slot_vectors, active_counts=active_counts, lookup_map=lookup_map, address_map=address_map, content_map=content_map, result_valve_map=result_valve_map, fading_map_coefficients=fading_map_coefficients, writing_intensity_map=writing_intensity_map, result_map=result_map, fading_speed_exponent=fading_speed_exponent, fading_bias=fading_bias, entry_scaling=entry_scaling, per_channel_scaling=per_channel_scaling, extra_shrink_exponent=extra_shrink_exponent, memory_tensors=memory_tensors)


EPS = 1e-06

def unit_rows(values):
    return values * lax.rsqrt(lax.optimization_barrier(jnp.sum(values * values, axis=-1, keepdims=True)) + EPS)

def recur(query, keyvec, value, fading_multiplier, beta, live, state):
    reads = []
    for step in range(query.shape[1]):
        decayed = state * jnp.exp(fading_multiplier[:, step])[:, None, :, None]
        guess = jnp.einsum('skhe,shk->she', decayed, keyvec[:, step], precision=lax.Precision.HIGHEST)
        fresh = beta[:, step][..., None] * (value[:, step] - guess)
        updated = decayed + jnp.einsum('shk,she->skhe', keyvec[:, step], fresh, precision=lax.Precision.HIGHEST)
        read = jnp.einsum('skhe,shk->she', updated, query[:, step], precision=lax.Precision.HIGHEST)
        alive = live[:, step]
        state = jnp.where(alive[:, None, None, None], updated, state)
        reads.append(jnp.where(alive[:, None, None], read, 0.0))
    return (jnp.stack(reads, axis=1), state)

def reference(residual_slot_vectors, active_counts, lookup_map, address_map, content_map, result_valve_map, fading_map_coefficients, writing_intensity_map, result_map, fading_speed_exponent, fading_bias, entry_scaling, per_channel_scaling, extra_shrink_exponent, memory_tensors):
    rows = SEQS * NEW
    width = HEADS * HEAD
    resid = residual_slot_vectors.reshape(rows, D)
    position = lax.broadcasted_iota(jnp.int32, (SEQS, NEW), 1)
    live = position < active_counts.astype(jnp.int32)[:, None]
    fresh_states = []
    for block_coefficients in range(BLOCKS):
        widened = resid.astype(jnp.float32)
        factor = lax.rsqrt(lax.optimization_barrier(jnp.sum(widened * widened, axis=1)) / D + EPS)
        scaled = (widened * entry_scaling[block_coefficients].astype(jnp.float32)).astype(jnp.bfloat16)
        pieces = scaled.reshape(rows, N_DP, D // N_DP).astype(jnp.float32)

        def split_product(weight):
            blocked = weight.reshape(N_DP, D // N_DP, weight.shape[1]).astype(jnp.float32)
            part = jnp.einsum('rnd,ndc->nrc', pieces, blocked).astype(jnp.bfloat16)
            part = lax.optimization_barrier(part)
            return lax.optimization_barrier(jnp.sum(part.astype(jnp.float32), axis=0)) * factor[:, None]
        proj_q = split_product(lookup_map[block_coefficients])
        proj_k = split_product(address_map[block_coefficients])
        proj_v = split_product(content_map[block_coefficients])
        proj_z = split_product(result_valve_map[block_coefficients])
        fading_mapped = split_product(fading_map_coefficients[block_coefficients]).reshape(SEQS, NEW, HEADS)
        proj_b = split_product(writing_intensity_map[block_coefficients]).reshape(SEQS, NEW, HEADS)
        query = unit_rows(jax.nn.silu(proj_q).reshape(SEQS, NEW, HEADS, HEAD)) * HEAD ** (-0.5)
        keyvec = unit_rows(jax.nn.silu(proj_k).reshape(SEQS, NEW, HEADS, HEAD))
        value = jax.nn.silu(proj_v).reshape(SEQS, NEW, HEADS, HEAD)
        fading_multiplier = -jnp.exp(fading_speed_exponent[block_coefficients]) * jax.nn.softplus(fading_mapped + fading_bias[block_coefficients]) + extra_shrink_exponent[block_coefficients]
        beta = jax.nn.sigmoid(proj_b)
        state = memory_tensors[block_coefficients].reshape(SEQS, HEAD, HEADS, HEAD)
        reads, state = recur(query, keyvec, value, fading_multiplier, beta, live, state)
        fresh_states.append(state.reshape(SEQS, HEAD, width))
        normed = reads * lax.rsqrt(lax.optimization_barrier(jnp.mean(reads * reads, axis=-1, keepdims=True)) + EPS)
        normed = normed * per_channel_scaling[block_coefficients].astype(jnp.float32)
        gated = (normed.reshape(rows, width) * jax.nn.silu(proj_z)).astype(jnp.bfloat16)
        mixed = jnp.dot(gated, result_map[block_coefficients], preferred_element_type=jnp.float32)
        resid = (resid.astype(jnp.float32) + mixed).astype(jnp.bfloat16)
    return (resid.reshape(SEQS, NEW, D), jnp.stack(fresh_states))
```

```python
import functools
import types

import jax
import jax.numpy as jnp
from jax import lax
from jax.experimental import pallas as pl
from jax.experimental.pallas import tpu as pltpu
from jax.sharding import PartitionSpec as P

BLOCKS = 2
EPS = 1e-06
F32 = jnp.float32
BF16 = jnp.bfloat16
MESH = pl.DeviceIdType.MESH
VMEM = pl.BlockSpec(memory_space=pltpu.VMEM)
HBM = pl.BlockSpec(memory_space=pltpu.HBM)
SMEM = pl.BlockSpec(memory_space=pltpu.SMEM)


def iota(shape, dim):
    return lax.broadcasted_iota(jnp.int32, shape, dim)


def dot(a, b):
    return jnp.dot(a, b, preferred_element_type=F32)


def exact(a, b):
    return jnp.dot(a, b, precision=lax.Precision.HIGHEST, preferred_element_type=F32)


def tiles(ref, count):
    return jnp.concatenate([ref] * count, axis=0)


def sizes(n, m, resid, counts, wq, speed):
    c = types.SimpleNamespace(n=n, m=m)
    c.seqs, c.slots, c.feat = resid.shape
    c.own_seqs = counts.shape[0]
    c.cols = wq.shape[2]
    c.heads = speed.shape[1]
    c.size = c.cols // c.heads
    c.own = c.own_seqs * c.slots
    c.rows = c.seqs * c.slots
    c.packed = c.seqs * 3 // 2
    c.chips = n // 2
    c.per_chip = 2 * c.own_seqs
    c.chip_win = c.packed - (c.chips - 1) * c.per_chip
    c.win = c.packed - (n - 1) * c.own_seqs
    c.tile = min(256, c.cols)
    c.chunks = c.cols // c.tile
    c.per_tile = c.tile // c.size
    c.groups = c.own_seqs // c.per_tile
    c.parts = 4
    c.part = c.feat // c.parts
    c.lanes = -(-c.seqs // 128) * 128
    return c


def main_kernel(
    c, counts, flat, wq, wk, wv, wz, wa, wb, wo, speed, bias, scaling, channel, shrink, states,
    kx, wx, gx, hx, hot, *scratch,
):
    s = types.SimpleNamespace(**dict(zip(c.names, scratch)))
    n, m, chips, tile = c.n, c.m, c.chips, c.tile
    me = lax.axis_index("dp")
    z = lax.axis_index("tp")
    core = lax.rem(me, 2)
    chip = lax.div(me, 2)
    partner = me + 1 - 2 * core
    others = [lax.rem(me + 2 * d, n) for d in range(1, chips)]
    sources = [lax.rem(me + n - 2 * d, n) for d in range(1, chips)]
    half = m // 2
    left = z < half
    depth = jnp.where(left, z, m - 1 - z)
    toward = jnp.where(left, z + 1, z - 1)
    away = lax.rem(jnp.where(left, z - 1, z + 1) + m, m)
    centre = depth == half - 1

    def remote(src, dst, send_sem, recv_sem, axis, peer):
        return pltpu.make_async_remote_copy(
            src_ref=src, dst_ref=dst, send_sem=send_sem, recv_sem=recv_sem,
            device_id={axis: peer}, device_id_type=MESH,
        )

    def load(src, dst, sem):
        copy = pltpu.make_async_copy(src, dst, sem)
        copy.start()
        return copy

    feats = pl.ds(pl.multiple_of(me * c.feat, 16), c.feat)
    early = [
        load(src, dst, s.small_sem.at[i])
        for i, (src, dst) in enumerate(
            [
                (flat, s.flat), (scaling, s.scaling), (wa.at[:, feats, :], s.wa), (wb.at[:, feats, :], s.wb),
                (speed, s.speed), (bias, s.bias), (channel, s.channel), (shrink, s.shrink),
            ]
        )
    ]
    w_loads, wo_loads, state_loads = {}, {}, {}

    def load_weights(l):
        for j in range(c.chunks):
            for i, w in enumerate((wq, wk, wv, wz)):
                at = pl.ds(j * tile, tile)
                w_loads[l, j, i] = load(w.at[l, :, at], s.w.at[l, i, :, at], s.w_sem.at[l, j, i])

    def load_rest(l):
        state_loads[l] = load(states.at[l], s.states.at[l], s.state_sem.at[l])
        wo_loads[l] = load(wo.at[l], s.wo.at[l], s.wo_sem.at[l])

    load_weights(0)

    barrier = pltpu.get_barrier_semaphore()
    dp_peers = [lax.rem(me + d, n) for d in range(1, n)]
    for axis, peers in (("dp", dp_peers), ("tp", [lax.rem(z + 1, m), lax.rem(z + m - 1, m)])):
        for peer in peers:
            pl.semaphore_signal(barrier, inc=1, device_id={axis: peer}, device_id_type=MESH)
    pl.semaphore_wait(barrier, n + 1)

    lane = iota((8, c.lanes), 1) - me * c.own_seqs
    mine = jnp.zeros((8, c.lanes), jnp.int32)
    for i in range(c.own_seqs):
        mine = jnp.where(lane == i, counts[i], mine)
    s.counts[me] = mine
    swaps = [
        remote(s.counts.at[me], s.counts.at[me], s.count_s.at[d], s.count_r.at[d], "dp", peer)
        for d, peer in enumerate(dp_peers)
    ]
    for copy in swaps:
        copy.start()

    row = lax.div(iota((tile, tile), 0), c.size)
    col = lax.div(iota((tile, tile), 1), c.size)
    s.blocks[...] = (row == col).astype(BF16)
    for h in range(c.per_tile):
        s.spread[h] = (
            iota((tile, tile), 0) == h * c.size + lax.rem(iota((tile, tile), 1), c.size)
        ).astype(BF16)
    for g in range(c.groups):
        r = lax.rem(iota((2 * c.own, tile), 0), c.own_seqs)
        k = g * c.per_tile + lax.div(iota((2 * c.own, tile), 1), c.size)
        s.mask[g] = (r == k).astype(BF16)
    load_rest(0)
    for copy in early:
        copy.wait()
    all_heads = wa.shape[2]
    ab = 2 * all_heads
    for l in range(BLOCKS):
        at_a = (iota((all_heads, ab), 0) == iota((all_heads, ab), 1)).astype(BF16)
        at_b = (iota((all_heads, ab), 0) + all_heads == iota((all_heads, ab), 1)).astype(BF16)
        s.wab[l] = (dot(s.wa[l], at_a) + dot(s.wb[l], at_b)).astype(BF16)

    for copy in swaps:
        copy.wait()
    total = s.counts[0]
    for d in range(1, n):
        total = total + s.counts[d]
    row_counts = total.astype(F32)
    row_bf16 = row_counts.astype(BF16)

    def columns(count, seq, slot):
        lanes = iota((count, c.lanes), 1)
        all_counts = jnp.broadcast_to(row_counts[:1], (count, c.lanes))
        start = jnp.sum(jnp.where(lanes < seq, all_counts, 0.0), axis=1, keepdims=True)
        size = jnp.sum(jnp.where(lanes == seq, all_counts, 0.0), axis=1, keepdims=True)
        slot = slot[:, :1].astype(F32)
        return start + slot, slot < size

    def rows_of(seq, slot):
        index = iota(seq.shape, 0)
        start = dot(row_bf16, (index < seq).astype(BF16))[:1]
        size = dot(row_bf16, (index == seq).astype(BF16))[:1]
        slot = slot[:1].astype(F32)
        return start + slot, slot < size

    shape = (c.lanes, c.rows)
    pos, live = rows_of(lax.div(iota(shape, 1), c.slots), lax.rem(iota(shape, 1), c.slots))
    into = jnp.where((iota((c.packed, c.rows), 0).astype(F32) == pos) & live, 1.0, 0.0).astype(BF16)
    h0 = dot(into, s.flat[...])
    s.h[...] = h0
    s.scaled[0] = (h0 * s.scaling[...].astype(F32)[:1]).astype(BF16)

    def produce(l, j, acc):
        for i in range(4):
            if acc is None:
                w_loads[l, j, i].wait()
                val = dot(s.scaled[l], s.w[l, i, :, j * tile : (j + 1) * tile])
            else:
                val = acc(j, i)
            s.x[l, j, i // 2, :, (i % 2) * tile : (i % 2 + 1) * tile] = val.astype(BF16)
        first(l, j).start()

    def produce_small(l):
        h = s.h[...]
        s.x_small[l, 0] = dot(s.scaled[l], s.wab[l]).astype(BF16)
        squares = jnp.sum(h * h, axis=1, keepdims=True)
        s.x_small[l, 1] = jnp.broadcast_to(squares, (c.packed, ab)).astype(BF16)
        first(l, -1).start()

    def bufs(l, j):
        if j < 0:
            return s.x_small.at[l], s.pair_small.at[l], s.sum_small.at[l], s.far_small.at[l], s.out_small.at[l], s.fin_small.at[l]
        return s.x.at[l, j], s.pair.at[l, j], s.sum.at[l, j], s.far.at[l, j], s.out.at[l, j], s.fin.at[l, j]

    def first(l, j):
        x, pair, *_ = bufs(l, j)
        return remote(x.at[1 - core], pair, s.first_s.at[l, j + 1], s.first_r.at[l, j + 1], "dp", partner)

    def second(l, j, d):
        _, _, own, far, *_ = bufs(l, j)
        there = pl.multiple_of(lax.div(others[d], 2) * c.per_chip, 16)
        return remote(
            own.at[pl.ds(there, c.chip_win)], far.at[d], s.second_s.at[l, j + 1, d], s.second_r.at[l, j + 1, d],
            "dp", others[d],
        )

    def third(l, j):
        *_, out, fin = bufs(l, j)
        return remote(out, fin.at[core], s.third_s.at[l, j + 1], s.third_r.at[l, j + 1], "dp", partner)

    def cross(l, j):
        x, pair, own, *_ = bufs(l, j)
        first(l, j).wait()
        own[...] = (x[core].astype(F32) + pair[...].astype(F32)).astype(BF16)
        for d in range(chips - 1):
            second(l, j, d).start()

    def finish(l, j):
        x, pair, own, far, out, fin = bufs(l, j)
        for d in range(chips - 1):
            second(l, j, d).wait()

        def reduced(which):
            at = pl.multiple_of(which * c.own_seqs, 16)
            val = own[pl.ds(pl.multiple_of(chip * c.per_chip + at, 16), c.win), :].astype(F32)
            for d in range(chips - 1):
                val = val + far[d, pl.ds(at, c.win), :].astype(F32)
            return val.astype(BF16)

        out[...] = reduced(1 - core)
        third(l, j).start()
        fin[core] = reduced(core)

    def prepare(l):
        third(l, -1).wait()
        pick = s.pick[...]
        heads = c.heads
        few = dot(pick, s.fin_small[l, 0]).astype(BF16)
        squares = dot(pick, s.fin_small[l, 1])[:, :1]
        factor = lax.rsqrt(squares / (c.feat * n) + EPS)
        s.factor[...] = jnp.broadcast_to(factor, s.factor.shape)
        at = iota((ab, heads), 1) + z * heads
        pa = dot(few, (iota((ab, heads), 0) == at).astype(BF16)) * factor
        pb = dot(few, (iota((ab, heads), 0) == at + all_heads).astype(BF16)) * factor
        arg = pa + s.bias[...][l : l + 1]
        soft = jnp.maximum(arg, 0.0) + jnp.log1p(jnp.exp(-jnp.abs(arg)))
        extra = jnp.concatenate([s.shrink[l, :, t, :] for t in range(c.slots)], axis=0)
        dec = jnp.exp(extra - jnp.exp(s.speed[...][l : l + 1]) * soft)
        dec = jnp.where(s.live[:, :1] > 0.0, dec, 1.0)
        wide = (iota((heads, c.cols), 0) == lax.div(iota((heads, c.cols), 1), c.size)).astype(F32)
        s.dec[...] = exact(dec, wide)
        s.beta[...] = exact(jax.nn.sigmoid(pb), wide)

    def recur(l, j):
        at = slice(j * tile, (j + 1) * tile)
        third(l, j).wait()
        pick = s.pick[...]
        factor = s.factor[:, :1]
        kept = []
        for i in range(4):
            val = dot(pick, s.fin[l, j, i // 2, :, (i % 2) * tile : (i % 2 + 1) * tile]) * factor
            val = val * jax.nn.sigmoid(val)
            if i < 2:
                total = dot((val * val).astype(BF16), s.blocks[...])
                val = val * lax.rsqrt(total + EPS)
                if i == 0:
                    val = val * c.size ** (-0.5)
            kept.append(val)
        q, k, v, zed = kept
        both = jnp.concatenate([k, q], axis=0).astype(BF16)
        kx[l, :, at] = both[: c.own]
        lane_head = lax.div(iota((2 * c.own, tile), 1), c.size)
        reads = None
        for h in range(c.per_tile):
            wide = dot(both, s.spread[h]).astype(BF16)
            lhs = jnp.concatenate([wide * s.mask[g] for g in range(c.groups)], axis=1)
            part = dot(lhs, s.states16[l, :, at])
            reads = part if reads is None else jnp.where(lane_head == h, part, reads)
        step = lambda x, t: x[t * c.own_seqs : (t + 1) * c.own_seqs]
        rk = reads[: c.own]
        rq = reads[c.own :]
        dec = s.dec[:, at]
        beta = s.beta[:, at]
        names, prods = [], []
        for t in range(c.slots):
            for i in range(t + 1):
                names.append(("q", i, t))
                prods.append(step(k, i) * step(q, t))
                if i < t:
                    names.append(("k", i, t))
                    prods.append(step(k, i) * step(k, t))
        pairs = dot(jnp.concatenate(prods, axis=0).astype(BF16), s.blocks[...])
        pairs = {name: step(pairs, i) for i, name in enumerate(names)}
        fresh, outs = [], []
        whole = None
        for t in range(c.slots):
            g = step(dec, t)
            whole = g if whole is None else whole * g
            fresh = [(u * g) for u in fresh]
            guess = whole * step(rk, t)
            for i in range(t):
                guess = guess + pairs["k", i, t] * fresh[i]
            fresh.append(step(beta, t) * (step(v, t) - guess))
            o = whole * step(rq, t)
            for i in range(t + 1):
                o = o + pairs["q", i, t] * fresh[i]
            outs.append(o)
        wx[l, :, at] = jnp.concatenate(fresh, axis=0).astype(BF16)
        gx[l, :, at] = whole
        o = jnp.concatenate(outs, axis=0)
        total = dot((o * o).astype(BF16), s.blocks[...])
        o = o * lax.rsqrt(total / c.size + EPS) * s.gain[l, :1] * zed
        s.y[l, j, me] = dot(s.place[...], o.astype(BF16)).astype(BF16)
        for d in range(chips - 1):
            y_far(l, j, d).start()
        y_near(l, j, 0).start()

    def y_far(l, j, d):
        return remote(s.y.at[l, j, me], s.y.at[l, j, me], s.yf_s.at[l, j, d], s.yf_r.at[l, j, d], "dp", others[d])

    def y_near(l, j, d):
        source = me if d == 0 else sources[d - 1]
        return remote(
            s.y.at[l, j, source], s.y.at[l, j, source], s.yn_s.at[l, j, d], s.yn_r.at[l, j, d], "dp", partner
        )

    def forward(l, j):
        for d in range(chips - 1):
            y_far(l, j, d).wait()
            y_near(l, j, d + 1).start()

    def gather(l, j):
        for d in range(chips):
            y_near(l, j, d).wait()
        at = slice(j * tile, (j + 1) * tile)
        s.gated[:, at] = jnp.zeros((c.packed, tile), BF16)
        for d in range(n):
            here = slice(d * c.own_seqs, d * c.own_seqs + c.win)
            s.gated[here, at] = s.gated[here, at] + s.y[l, j, d]

    def inward(l, p):
        return remote(s.sent.at[l, p], s.came.at[l, p], s.in_s.at[l, p], s.in_r.at[l, p], "tp", toward)

    def across(l, p):
        return remote(s.sent.at[l, p], s.over.at[l, p], s.over_s.at[l, p], s.over_r.at[l, p], "tp", toward)

    def outward(l, p):
        return remote(s.full.at[l, p], s.full.at[l, p], s.full_s.at[l, p], s.full_r.at[l, p], "tp", away)

    def mix_out(l, p):
        at = slice(p * c.part, (p + 1) * c.part)
        s.sent[l, p] = dot(s.gated[...], s.wo[l, :, at]).astype(BF16)
        if half > 1:

            @pl.when(depth > 0)
            def _():
                inward(l, p).wait_recv()
                s.sent[l, p] = (s.sent[l, p].astype(F32) + s.came[l, p].astype(F32)).astype(BF16)

        @pl.when(centre)
        def _():
            across(l, p).start()

        if half > 1:

            @pl.when(jnp.logical_not(centre))
            def _():
                inward(l, p).start()

    def mix_in(l, p):
        @pl.when(centre)
        def _():
            across(l, p).wait_recv()
            s.full[l, p] = (s.sent[l, p].astype(F32) + s.over[l, p].astype(F32)).astype(BF16)

        if half > 1:

            @pl.when(jnp.logical_not(centre))
            def _():
                outward(l, p).wait_recv()

            @pl.when(depth > 0)
            def _():
                outward(l, p).start()

        at = slice(p * c.part, (p + 1) * c.part)
        new = (s.h[:, at] + s.full[l, p].astype(F32)).astype(BF16)
        if l + 1 == BLOCKS:
            hx[:, at] = new
        else:
            s.h[:, at] = new.astype(F32)
            s.scaled[l + 1, :, at] = (new.astype(F32) * s.scaling[...].astype(F32)[l + 1 : l + 2, at]).astype(BF16)

    def mix_end(l):
        for p in range(c.parts):

            @pl.when(centre)
            def _():
                across(l, p).wait_send()

            if half > 1:

                @pl.when(jnp.logical_not(centre))
                def _():
                    inward(l, p).wait_send()

                @pl.when(depth > 0)
                def _():
                    outward(l, p).wait_send()

    def setup():
        r = iota((c.own, c.lanes), 0)
        pos, live = columns(c.own, lax.rem(r, c.own_seqs) + me * c.own_seqs, lax.div(r, c.own_seqs))
        offset = (iota((c.own, c.win), 1) + me * c.own_seqs).astype(F32)
        s.pick[...] = jnp.where((offset == pos) & live, 1.0, 0.0).astype(BF16)
        s.live[...] = jnp.broadcast_to(jnp.where(live, 1.0, 0.0), s.live.shape)
        shape = (c.lanes, c.own)
        pos, live = rows_of(
            lax.rem(iota(shape, 1), c.own_seqs) + me * c.own_seqs, lax.div(iota(shape, 1), c.own_seqs)
        )
        offset = (iota((c.win, c.own), 0) + me * c.own_seqs).astype(F32)
        s.place[...] = jnp.where((offset == pos) & live, 1.0, 0.0).astype(BF16)
        r = iota((c.rows, c.lanes), 0)
        pos, live = columns(c.rows, lax.div(r, c.slots), lax.rem(r, c.slots))
        offset = iota((c.rows, c.packed), 1).astype(F32)
        hot[...] = jnp.where((offset == pos) & live, 1.0, 0.0).astype(BF16)
        fold = (iota((c.size, tile), 0) == lax.rem(iota((c.size, tile), 1), c.size)).astype(BF16)
        for l in range(BLOCKS):
            channels = jnp.broadcast_to(s.channel[...].astype(F32)[l : l + 1], (8, c.size)).astype(BF16)
            s.gain[l] = dot(channels, fold)

    def round_states(l):
        state_loads[l].wait()
        for i in range(c.own_seqs):
            s.states16[l, i * c.size : (i + 1) * c.size] = s.states[l, i].astype(BF16)

    for l in range(BLOCKS):
        acc = None
        if l:
            for p in range(c.parts):
                mix_in(l - 1, p)
                at = slice(p * c.part, (p + 1) * c.part)
                piece = s.scaled[l, :, at]
                if p == 0:
                    for j in range(c.chunks):
                        for i in range(4):
                            w_loads[l, j, i].wait()
                last = p + 1 == c.parts
                if not last:
                    for j in range(c.chunks):
                        for i in range(4):
                            val = dot(piece, s.w[l, i, at, j * tile : (j + 1) * tile])
                            s.acc[j, i] = val if p == 0 else s.acc[j, i] + val

            def acc(j, i, piece=piece, at=at, l=l):
                return s.acc[j, i] + dot(piece, s.w[l, i, at, j * tile : (j + 1) * tile])

        produce(l, 0, acc)
        produce_small(l)
        for j in range(1, c.chunks):
            produce(l, j, acc)
            if j == 1:
                cross(l, 0)
            elif j == 2:
                cross(l, -1)
        for j in ([] if c.chunks > 2 else [-1]) + list(range(0 if c.chunks == 1 else 1, c.chunks)):
            cross(l, j)
        if l == 0:
            load_weights(1)
            load_rest(1)
            setup()
            round_states(0)
        finish(l, -1)
        prepare(l)
        finish(l, 0)
        for j in range(1, c.chunks):
            finish(l, j)
            recur(l, j - 1)
        if l:
            mix_end(l - 1)
        recur(l, c.chunks - 1)
        for j in range(c.chunks):
            forward(l, j)
        wo_loads[l].wait()
        for j in range(c.chunks):
            gather(l, j)
        for p in range(c.parts):
            mix_out(l, p)
        if l == 0:
            round_states(1)
    for p in range(c.parts):
        mix_in(BLOCKS - 1, p)
    mix_end(BLOCKS - 1)


def run_main(c, args):
    ab = 2 * args[6].shape[2]
    half = 2 * c.tile
    chips, n = c.chips, c.n
    dma = lambda *shape: pltpu.SemaphoreType.DMA(shape)
    buf = lambda *shape: pltpu.VMEM(shape, BF16)
    wide = lambda *shape: pltpu.VMEM(shape, F32)
    every = 1 + c.chunks
    scratch = dict(
        flat=buf(c.rows, c.feat),
        scaling=buf(BLOCKS, c.feat),
        wa=buf(BLOCKS, c.feat, ab // 2),
        wb=buf(BLOCKS, c.feat, ab // 2),
        wab=buf(BLOCKS, c.feat, ab),
        speed=wide(BLOCKS, c.heads),
        bias=wide(BLOCKS, c.heads),
        channel=buf(BLOCKS, c.size),
        shrink=wide(BLOCKS, c.own_seqs, c.slots, c.heads),
        w=buf(BLOCKS, 4, c.feat, c.cols),
        wo=buf(BLOCKS, c.cols, c.feat),
        states=wide(BLOCKS, c.own_seqs, c.size, c.cols),
        states16=buf(BLOCKS, c.own_seqs * c.size, c.cols),
        counts=pltpu.VMEM((n, 8, c.lanes), jnp.int32),
        blocks=buf(c.tile, c.tile),
        spread=buf(c.per_tile, c.tile, c.tile),
        mask=buf(c.groups, 2 * c.own, c.tile),
        gain=wide(BLOCKS, 8, c.tile),
        pick=buf(c.own, c.win),
        place=buf(c.win, c.own),
        live=wide(c.own, 128),
        factor=wide(c.own, 128),
        dec=wide(c.own, c.cols),
        beta=wide(c.own, c.cols),
        h=wide(c.packed, c.feat),
        scaled=buf(BLOCKS, c.packed, c.feat),
        acc=wide(c.chunks, 4, c.packed, c.tile),
        x=buf(BLOCKS, c.chunks, 2, c.packed, half),
        pair=buf(BLOCKS, c.chunks, c.packed, half),
        sum=buf(BLOCKS, c.chunks, c.packed, half),
        far=buf(BLOCKS, c.chunks, chips - 1, c.chip_win, half),
        out=buf(BLOCKS, c.chunks, c.win, half),
        fin=buf(BLOCKS, c.chunks, 2, c.win, half),
        x_small=buf(BLOCKS, 2, c.packed, ab),
        pair_small=buf(BLOCKS, c.packed, ab),
        sum_small=buf(BLOCKS, c.packed, ab),
        far_small=buf(BLOCKS, chips - 1, c.chip_win, ab),
        out_small=buf(BLOCKS, c.win, ab),
        fin_small=buf(BLOCKS, 2, c.win, ab),
        y=buf(BLOCKS, c.chunks, n, c.win, c.tile),
        gated=buf(c.packed, c.cols),
        sent=buf(BLOCKS, c.parts, c.packed, c.part),
        came=buf(BLOCKS, c.parts, c.packed, c.part),
        over=buf(BLOCKS, c.parts, c.packed, c.part),
        full=buf(BLOCKS, c.parts, c.packed, c.part),
        small_sem=dma(8),
        w_sem=dma(BLOCKS, c.chunks, 4),
        wo_sem=dma(BLOCKS),
        state_sem=dma(BLOCKS),
        count_s=dma(n - 1),
        count_r=dma(n - 1),
        first_s=dma(BLOCKS, every),
        first_r=dma(BLOCKS, every),
        second_s=dma(BLOCKS, every, chips - 1),
        second_r=dma(BLOCKS, every, chips - 1),
        third_s=dma(BLOCKS, every),
        third_r=dma(BLOCKS, every),
        yf_s=dma(BLOCKS, c.chunks, chips - 1),
        yf_r=dma(BLOCKS, c.chunks, chips - 1),
        yn_s=dma(BLOCKS, c.chunks, chips),
        yn_r=dma(BLOCKS, c.chunks, chips),
        in_s=dma(BLOCKS, c.parts),
        in_r=dma(BLOCKS, c.parts),
        over_s=dma(BLOCKS, c.parts),
        over_r=dma(BLOCKS, c.parts),
        full_s=dma(BLOCKS, c.parts),
        full_r=dma(BLOCKS, c.parts),
    )
    c.names = list(scratch)
    return pl.pallas_call(
        functools.partial(main_kernel, c),
        out_shape=[
            jax.ShapeDtypeStruct((BLOCKS, c.own, c.cols), BF16),
            jax.ShapeDtypeStruct((BLOCKS, c.own, c.cols), BF16),
            jax.ShapeDtypeStruct((BLOCKS, c.own_seqs, c.cols), F32),
            jax.ShapeDtypeStruct((c.packed, c.feat), BF16),
            jax.ShapeDtypeStruct((c.rows, c.packed), BF16),
        ],
        in_specs=[SMEM] + [HBM] * 14,
        out_specs=[VMEM] * 5,
        scratch_shapes=list(scratch.values()),
        compiler_params=pltpu.CompilerParams(
            collective_id=1, has_side_effects=True, vmem_limit_bytes=50 * 1024 * 1024
        ),
        name="blocks",
    )(*args)


def write_kernel(c, group, kx, wx, gx, hx, hot, flat, states, new, tokens, keys, fresh):
    step = pl.program_id(1)
    tile = c.tile
    row_head = lax.div(iota((c.per_tile * c.own, tile), 0), c.own)
    lane_head = lax.div(iota((c.per_tile * c.own, tile), 1), c.size)
    same = (row_head == lane_head).astype(BF16)

    @pl.when((step == 0) & (pl.program_id(0) == 0))
    def _():
        live = hot[...]
        back = dot(live, hx[...])
        count = jnp.sum(live.astype(F32), axis=1, keepdims=True)
        tokens[...] = jnp.where(count > 0.0, back, flat[...].astype(F32)).astype(BF16)

    @pl.when(step == 0)
    def _():
        fold = (iota((c.size, tile), 0) == lax.rem(iota((c.size, tile), 1), c.size)).astype(BF16)
        for j in range(c.chunks):
            at = slice(j * tile, (j + 1) * tile)
            keys[j] = lax.dot_general(
                fold, tiles(kx[0, :, at], c.per_tile) * same, (((1,), (1,)), ((), ())),
                preferred_element_type=F32,
            ).astype(BF16)
            fresh[j] = tiles(wx[0, :, at], c.per_tile) * same

    shape = (c.size, c.per_tile * c.own)
    owner = lax.rem(iota(shape, 1), c.own_seqs)
    for j in range(c.chunks):
        at = slice(j * tile, (j + 1) * tile)
        lhs = jnp.concatenate(
            [keys[j] * (owner == step * group + i).astype(BF16) for i in range(group)], axis=0
        )
        added = dot(lhs, fresh[j])
        for i in range(group):
            decay = gx[0, pl.ds(step * group + i, 1), at]
            new[0, i, :, at] = states[0, i, :, at] * decay + added[i * c.size : (i + 1) * c.size]


def run_write(c, kx, wx, gx, hx, hot, flat, states):
    group = 4
    layer = lambda a: pl.BlockSpec((1,) + a.shape[1:], lambda l, g: (l, 0, 0))
    whole = lambda a: pl.BlockSpec(a.shape, lambda l, g: (0, 0))
    block = pl.BlockSpec((1, group) + states.shape[2:], lambda l, g: (l, g, 0, 0))
    return pl.pallas_call(
        functools.partial(write_kernel, c, group),
        out_shape=[
            jax.ShapeDtypeStruct(states.shape, F32),
            jax.ShapeDtypeStruct(flat.shape, BF16),
        ],
        grid=(BLOCKS, c.own_seqs // group),
        in_specs=[layer(kx), layer(wx), layer(gx), whole(hx), whole(hot), whole(flat), block],
        out_specs=[block, whole(flat)],
        scratch_shapes=[
            pltpu.VMEM((c.chunks, c.size, c.per_tile * c.own), BF16),
            pltpu.VMEM((c.chunks, c.per_tile * c.own, c.tile), BF16),
        ],
        name="write",
    )(kx, wx, gx, hx, hot, flat, states)


def body(
    n, m, resid, counts, wq, wk, wv, wz, wa, wb, wo, speed, bias, scaling, channel, shrink, states,
):
    c = sizes(n, m, resid, counts, wq, speed)
    flat = resid.reshape(c.rows, c.feat)
    outs = run_main(
        c, (counts, flat, wq, wk, wv, wz, wa, wb, wo, speed, bias, scaling, channel, shrink, states)
    )
    new, tokens = run_write(c, *outs, flat, states)
    return tokens.reshape(resid.shape), new


def solution(mesh):
    in_specs = (
        P("grp", None, "dp"),
        P(("grp", "dp")),
        P(None, "dp", "tp"),
        P(None, "dp", "tp"),
        P(None, "dp", "tp"),
        P(None, "dp", "tp"),
        P(),
        P(),
        P(None, "tp", "dp"),
        P(None, "tp"),
        P(None, "tp"),
        P(None, "dp"),
        P(),
        P(None, ("grp", "dp"), None, "tp"),
        P(None, ("grp", "dp"), None, "tp"),
    )
    out_specs = (P("grp", None, "dp"), P(None, ("grp", "dp"), None, "tp"))
    run = functools.partial(body, mesh.shape["dp"], mesh.shape["tp"])
    return jax.shard_map(run, mesh=mesh, in_specs=in_specs, out_specs=out_specs, check_vma=False)
```

```python
import functools
import types

import jax
import jax.numpy as jnp
from jax import lax
from jax.experimental import pallas as pl
from jax.experimental.pallas import tpu as pltpu
from jax.sharding import PartitionSpec as P

BLOCKS = 2
EPS = 1e-06
F32 = jnp.float32
BF16 = jnp.bfloat16
MESH = pl.DeviceIdType.MESH
VMEM = pl.BlockSpec(memory_space=pltpu.VMEM)
HBM = pl.BlockSpec(memory_space=pltpu.HBM)
SMEM = pl.BlockSpec(memory_space=pltpu.SMEM)


def iota(shape, dim):
    return lax.broadcasted_iota(jnp.int32, shape, dim)


def dot(a, b):
    return jnp.dot(a, b, preferred_element_type=F32)


def exact(a, b):
    return jnp.dot(a, b, precision=lax.Precision.HIGHEST, preferred_element_type=F32)


def tiles(ref, count):
    return jnp.concatenate([ref] * count, axis=0)


def sizes(n, m, resid, counts, wq, speed):
    c = types.SimpleNamespace(n=n, m=m)
    c.seqs, c.slots, c.feat = resid.shape
    c.own_seqs = counts.shape[0]
    c.cols = wq.shape[2]
    c.heads = speed.shape[1]
    c.size = c.cols // c.heads
    c.own = c.own_seqs * c.slots
    c.rows = c.seqs * c.slots
    c.packed = c.seqs * 3 // 2
    c.chips = n // 2
    c.per_chip = 2 * c.own_seqs
    c.chip_win = c.packed - (c.chips - 1) * c.per_chip
    c.win = c.packed - (n - 1) * c.own_seqs
    c.tile = min(256, c.cols)
    c.chunks = c.cols // c.tile
    c.per_tile = c.tile // c.size
    c.groups = c.own_seqs // c.per_tile
    c.parts = 4
    c.part = c.feat // c.parts
    c.lanes = -(-c.seqs // 128) * 128
    return c


def main_kernel(
    c, counts, resid, wq, wk, wv, wz, wa, wb, wo, speed, bias, scaling, channel, shrink, states,
    tokens, new, *scratch,
):
    s = types.SimpleNamespace(**dict(zip(c.names, scratch)))
    n, m, chips, tile = c.n, c.m, c.chips, c.tile
    me = lax.axis_index("dp")
    z = lax.axis_index("tp")
    core = lax.rem(me, 2)
    chip = lax.div(me, 2)
    partner = me + 1 - 2 * core
    others = [lax.rem(me + 2 * d, n) for d in range(1, chips)]
    sources = [lax.rem(me + n - 2 * d, n) for d in range(1, chips)]
    half = m // 2
    left = z < half
    depth = jnp.where(left, z, m - 1 - z)
    toward = jnp.where(left, z + 1, z - 1)
    away = lax.rem(jnp.where(left, z - 1, z + 1) + m, m)
    centre = depth == half - 1

    def remote(src, dst, send_sem, recv_sem, axis, peer):
        return pltpu.make_async_remote_copy(
            src_ref=src, dst_ref=dst, send_sem=send_sem, recv_sem=recv_sem,
            device_id={axis: peer}, device_id_type=MESH,
        )

    def load(src, dst, sem):
        copy = pltpu.make_async_copy(src, dst, sem)
        copy.start()
        return copy

    all_heads = wa.shape[1]
    ab = 2 * all_heads
    feats = pl.ds(pl.multiple_of(me * c.feat, 128), c.feat)
    early = [
        load(src, dst, s.small_sem.at[i])
        for i, (src, dst) in enumerate(
            [
                (resid, s.resid), (scaling, s.scaling),
                (wa.at[:, :, feats], s.wab.at[:, pl.ds(0, all_heads)]),
                (wb.at[:, :, feats], s.wab.at[:, pl.ds(all_heads, all_heads)]),
                (speed, s.speed), (bias, s.bias), (channel, s.channel), (shrink, s.shrink),
            ]
        )
    ]
    w_loads, wo_loads, state_loads = {}, {}, {}

    def load_weights(l):
        for j in range(c.chunks):
            for i, w in enumerate((wq, wk, wv, wz)):
                at = pl.ds(j * tile, tile)
                w_loads[l, j, i] = load(w.at[l, :, at], s.w.at[l, i, :, at], s.w_sem.at[l, j, i])

    def load_rest(l):
        state_loads[l] = load(states.at[l], new.at[l], s.state_sem.at[l])
        wo_loads[l] = load(wo.at[l], s.wo.at[l], s.wo_sem.at[l])

    load_weights(0)

    barrier = pltpu.get_barrier_semaphore()
    dp_peers = [lax.rem(me + d, n) for d in range(1, n)]
    for axis, peers in (("dp", dp_peers), ("tp", [lax.rem(z + 1, m), lax.rem(z + m - 1, m)])):
        for peer in peers:
            pl.semaphore_signal(barrier, inc=1, device_id={axis: peer}, device_id_type=MESH)
    pl.semaphore_wait(barrier, n + 1)

    lane = iota((8, c.lanes), 1) - me * c.own_seqs
    mine = jnp.zeros((8, c.lanes), jnp.int32)
    for i in range(c.own_seqs):
        mine = jnp.where(lane == i, counts[i], mine)
    s.counts[me] = mine
    swaps = [
        remote(s.counts.at[me], s.counts.at[me], s.count_s.at[d], s.count_r.at[d], "dp", peer)
        for d, peer in enumerate(dp_peers)
    ]
    for copy in swaps:
        copy.start()

    row = lax.div(iota((tile, tile), 0), c.size)
    col = lax.div(iota((tile, tile), 1), c.size)
    s.blocks[...] = (row == col).astype(BF16)
    for h in range(c.per_tile):
        s.spread[h] = (
            iota((tile, tile), 0) == h * c.size + lax.rem(iota((tile, tile), 1), c.size)
        ).astype(BF16)
    for g in range(c.groups):
        r = lax.rem(iota((2 * c.own, tile), 0), c.own_seqs)
        k = g * c.per_tile + lax.div(iota((2 * c.own, tile), 1), c.size)
        s.mask[g] = (r == k).astype(BF16)
    load_rest(0)
    for copy in early:
        copy.wait()

    for copy in swaps:
        copy.wait()
    total = s.counts[0]
    for d in range(1, n):
        total = total + s.counts[d]
    row_counts = total.astype(F32)
    row_bf16 = row_counts.astype(BF16)

    def columns(count, seq, slot):
        lanes = iota((count, c.lanes), 1)
        all_counts = jnp.broadcast_to(row_counts[:1], (count, c.lanes))
        start = jnp.sum(jnp.where(lanes < seq, all_counts, 0.0), axis=1, keepdims=True)
        size = jnp.sum(jnp.where(lanes == seq, all_counts, 0.0), axis=1, keepdims=True)
        slot = slot[:, :1].astype(F32)
        return start + slot, slot < size

    def rows_of(seq, slot):
        index = iota(seq.shape, 0)
        start = dot(row_bf16, (index < seq).astype(BF16))[:1]
        size = dot(row_bf16, (index == seq).astype(BF16))[:1]
        slot = slot[:1].astype(F32)
        return start + slot, slot < size

    shape = (c.lanes, c.rows)
    pos, live = rows_of(lax.div(iota(shape, 1), c.slots), lax.rem(iota(shape, 1), c.slots))
    into = jnp.where((iota((c.packed, c.rows), 0).astype(F32) == pos) & live, 1.0, 0.0).astype(BF16)
    h0 = dot(into, s.resid[...].reshape(c.rows, c.feat))
    s.h[...] = h0
    s.scaled[0] = (h0 * s.scaling[...].astype(F32)[:1]).astype(BF16)

    def produce(l, j, acc):
        for i in range(4):
            if acc is None:
                w_loads[l, j, i].wait()
                val = dot(s.scaled[l], s.w[l, i, :, j * tile : (j + 1) * tile])
            else:
                val = acc(j, i)
            s.x[l, j, i // 2, :, (i % 2) * tile : (i % 2 + 1) * tile] = val.astype(BF16)
        first(l, j).start()

    def produce_small(l):
        h = s.h[...]
        s.x_small[l, 0] = lax.dot_general(
            s.scaled[l], s.wab[l], (((1,), (1,)), ((), ())), preferred_element_type=F32
        ).astype(BF16)
        squares = jnp.sum(h * h, axis=1, keepdims=True)
        s.x_small[l, 1] = jnp.broadcast_to(squares, (c.packed, ab)).astype(BF16)
        first(l, -1).start()

    def bufs(l, j):
        if j < 0:
            return s.x_small.at[l], s.pair_small.at[l], s.sum_small.at[l], s.far_small.at[l], s.out_small.at[l], s.fin_small.at[l]
        return s.x.at[l, j], s.pair.at[l, j], s.sum.at[l, j], s.far.at[l, j], s.out.at[l, j], s.fin.at[l, j]

    def first(l, j):
        x, pair, *_ = bufs(l, j)
        return remote(x.at[1 - core], pair, s.first_s.at[l, j + 1], s.first_r.at[l, j + 1], "dp", partner)

    def second(l, j, d):
        _, _, own, far, *_ = bufs(l, j)
        there = pl.multiple_of(lax.div(others[d], 2) * c.per_chip, 16)
        return remote(
            own.at[pl.ds(there, c.chip_win)], far.at[d], s.second_s.at[l, j + 1, d], s.second_r.at[l, j + 1, d],
            "dp", others[d],
        )

    def third(l, j):
        *_, out, fin = bufs(l, j)
        return remote(out, fin.at[core], s.third_s.at[l, j + 1], s.third_r.at[l, j + 1], "dp", partner)

    def cross(l, j):
        x, pair, own, *_ = bufs(l, j)
        first(l, j).wait()
        own[...] = (x[core].astype(F32) + pair[...].astype(F32)).astype(BF16)
        for d in range(chips - 1):
            second(l, j, d).start()

    def finish(l, j):
        x, pair, own, far, out, fin = bufs(l, j)
        for d in range(chips - 1):
            second(l, j, d).wait()

        def reduced(which):
            at = pl.multiple_of(which * c.own_seqs, 16)
            val = own[pl.ds(pl.multiple_of(chip * c.per_chip + at, 16), c.win), :].astype(F32)
            for d in range(chips - 1):
                val = val + far[d, pl.ds(at, c.win), :].astype(F32)
            return val.astype(BF16)

        out[...] = reduced(1 - core)
        third(l, j).start()
        fin[core] = reduced(core)

    def prepare(l):
        third(l, -1).wait()
        pick = s.pick[...]
        heads = c.heads
        few = dot(pick, s.fin_small[l, 0]).astype(BF16)
        squares = dot(pick, s.fin_small[l, 1])[:, :1]
        factor = lax.rsqrt(squares / (c.feat * n) + EPS)
        s.factor[...] = jnp.broadcast_to(factor, s.factor.shape)
        at = iota((ab, heads), 1) + z * heads
        pa = dot(few, (iota((ab, heads), 0) == at).astype(BF16)) * factor
        pb = dot(few, (iota((ab, heads), 0) == at + all_heads).astype(BF16)) * factor
        arg = pa + s.bias[...][l : l + 1]
        soft = jnp.maximum(arg, 0.0) + jnp.log1p(jnp.exp(-jnp.abs(arg)))
        extra = jnp.concatenate([s.shrink[l, :, t, :] for t in range(c.slots)], axis=0)
        dec = jnp.exp(extra - jnp.exp(s.speed[...][l : l + 1]) * soft)
        dec = jnp.where(s.live[:, :1] > 0.0, dec, 1.0)
        wide = (iota((heads, c.cols), 0) == lax.div(iota((heads, c.cols), 1), c.size)).astype(F32)
        s.dec[...] = exact(dec, wide)
        s.beta[...] = exact(jax.nn.sigmoid(pb), wide)

    def recur(l, j):
        at = slice(j * tile, (j + 1) * tile)
        third(l, j).wait()
        pick = s.pick[...]
        factor = s.factor[:, :1]
        kept = []
        for i in range(4):
            val = dot(pick, s.fin[l, j, i // 2, :, (i % 2) * tile : (i % 2 + 1) * tile]) * factor
            val = val * jax.nn.sigmoid(val)
            if i < 2:
                total = dot((val * val).astype(BF16), s.blocks[...])
                val = val * lax.rsqrt(total + EPS)
                if i == 0:
                    val = val * c.size ** (-0.5)
            kept.append(val)
        q, k, v, zed = kept
        both = jnp.concatenate([k, q], axis=0).astype(BF16)
        s.k[l, :, at] = both[: c.own]
        lane_head = lax.div(iota((2 * c.own, tile), 1), c.size)
        reads = None
        for h in range(c.per_tile):
            wide = dot(both, s.spread[h]).astype(BF16)
            lhs = jnp.concatenate([wide * s.mask[g] for g in range(c.groups)], axis=1)
            part = dot(lhs, s.states16[l, :, at])
            reads = part if reads is None else jnp.where(lane_head == h, part, reads)
        step = lambda x, t: x[t * c.own_seqs : (t + 1) * c.own_seqs]
        rk = reads[: c.own]
        rq = reads[c.own :]
        dec = s.dec[:, at]
        beta = s.beta[:, at]
        names, prods = [], []
        for t in range(c.slots):
            for i in range(t + 1):
                names.append(("q", i, t))
                prods.append(step(k, i) * step(q, t))
                if i < t:
                    names.append(("k", i, t))
                    prods.append(step(k, i) * step(k, t))
        pairs = dot(jnp.concatenate(prods, axis=0).astype(BF16), s.blocks[...])
        pairs = {name: step(pairs, i) for i, name in enumerate(names)}
        fresh, outs = [], []
        whole = None
        for t in range(c.slots):
            g = step(dec, t)
            whole = g if whole is None else whole * g
            fresh = [(u * g) for u in fresh]
            guess = whole * step(rk, t)
            for i in range(t):
                guess = guess + pairs["k", i, t] * fresh[i]
            fresh.append(step(beta, t) * (step(v, t) - guess))
            o = whole * step(rq, t)
            for i in range(t + 1):
                o = o + pairs["q", i, t] * fresh[i]
            outs.append(o)
        s.u[l, :, at] = jnp.concatenate(fresh, axis=0).astype(BF16)
        s.decay[l, :, at] = whole
        o = jnp.concatenate(outs, axis=0)
        total = dot((o * o).astype(BF16), s.blocks[...])
        o = o * lax.rsqrt(total / c.size + EPS) * s.gain[l, :1] * zed
        s.y[l, j, me] = dot(s.place[...], o.astype(BF16)).astype(BF16)
        for d in range(chips - 1):
            y_far(l, j, d).start()
        y_near(l, j, 0).start()

    def y_far(l, j, d):
        return remote(s.y.at[l, j, me], s.y.at[l, j, me], s.yf_s.at[l, j, d], s.yf_r.at[l, j, d], "dp", others[d])

    def y_near(l, j, d):
        source = me if d == 0 else sources[d - 1]
        return remote(
            s.y.at[l, j, source], s.y.at[l, j, source], s.yn_s.at[l, j, d], s.yn_r.at[l, j, d], "dp", partner
        )

    def forward(l, j):
        for d in range(chips - 1):
            y_far(l, j, d).wait()
            y_near(l, j, d + 1).start()

    def gather(l, j):
        for d in range(chips):
            y_near(l, j, d).wait()
        at = slice(j * tile, (j + 1) * tile)
        s.gated[:, at] = jnp.zeros((c.packed, tile), BF16)
        for d in range(n):
            here = slice(d * c.own_seqs, d * c.own_seqs + c.win)
            s.gated[here, at] = s.gated[here, at] + s.y[l, j, d]

    def inward(l, p):
        return remote(s.sent.at[l, p], s.came.at[l, p], s.in_s.at[l, p], s.in_r.at[l, p], "tp", toward)

    def across(l, p):
        return remote(s.sent.at[l, p], s.over.at[l, p], s.over_s.at[l, p], s.over_r.at[l, p], "tp", toward)

    def outward(l, p):
        return remote(s.full.at[l, p], s.full.at[l, p], s.full_s.at[l, p], s.full_r.at[l, p], "tp", away)

    def mix_out(l, p):
        at = slice(p * c.part, (p + 1) * c.part)
        s.sent[l, p] = dot(s.gated[...], s.wo[l, :, at]).astype(BF16)
        if half > 1:

            @pl.when(depth > 0)
            def _():
                inward(l, p).wait_recv()
                s.sent[l, p] = (s.sent[l, p].astype(F32) + s.came[l, p].astype(F32)).astype(BF16)

        @pl.when(centre)
        def _():
            across(l, p).start()

        if half > 1:

            @pl.when(jnp.logical_not(centre))
            def _():
                inward(l, p).start()

    def mix_in(l, p):
        @pl.when(centre)
        def _():
            across(l, p).wait_recv()
            s.full[l, p] = (s.sent[l, p].astype(F32) + s.over[l, p].astype(F32)).astype(BF16)

        if half > 1:

            @pl.when(jnp.logical_not(centre))
            def _():
                outward(l, p).wait_recv()

            @pl.when(depth > 0)
            def _():
                outward(l, p).start()

        at = slice(p * c.part, (p + 1) * c.part)
        mixed = (s.h[:, at] + s.full[l, p].astype(F32)).astype(BF16)
        if l + 1 == BLOCKS:
            s.last[:, at] = mixed
        else:
            s.h[:, at] = mixed.astype(F32)
            s.scaled[l + 1, :, at] = (mixed.astype(F32) * s.scaling[...].astype(F32)[l + 1 : l + 2, at]).astype(BF16)

    def mix_end(l):
        for p in range(c.parts):

            @pl.when(centre)
            def _():
                across(l, p).wait_send()

            if half > 1:

                @pl.when(jnp.logical_not(centre))
                def _():
                    inward(l, p).wait_send()

                @pl.when(depth > 0)
                def _():
                    outward(l, p).wait_send()

    def setup():
        r = iota((c.own, c.lanes), 0)
        pos, live = columns(c.own, lax.rem(r, c.own_seqs) + me * c.own_seqs, lax.div(r, c.own_seqs))
        offset = (iota((c.own, c.win), 1) + me * c.own_seqs).astype(F32)
        s.pick[...] = jnp.where((offset == pos) & live, 1.0, 0.0).astype(BF16)
        s.live[...] = jnp.broadcast_to(jnp.where(live, 1.0, 0.0), s.live.shape)
        shape = (c.lanes, c.own)
        pos, live = rows_of(
            lax.rem(iota(shape, 1), c.own_seqs) + me * c.own_seqs, lax.div(iota(shape, 1), c.own_seqs)
        )
        offset = (iota((c.win, c.own), 0) + me * c.own_seqs).astype(F32)
        s.place[...] = jnp.where((offset == pos) & live, 1.0, 0.0).astype(BF16)
        r = iota((c.rows, c.lanes), 0)
        pos, live = columns(c.rows, lax.div(r, c.slots), lax.rem(r, c.slots))
        offset = iota((c.rows, c.packed), 1).astype(F32)
        s.hot[...] = jnp.where((offset == pos) & live, 1.0, 0.0).astype(BF16)
        s.alive[...] = jnp.broadcast_to(jnp.where(live, 1.0, 0.0), s.alive.shape)
        fold = (iota((c.size, tile), 0) == lax.rem(iota((c.size, tile), 1), c.size)).astype(BF16)
        for l in range(BLOCKS):
            channels = jnp.broadcast_to(s.channel[...].astype(F32)[l : l + 1], (8, c.size)).astype(BF16)
            s.gain[l] = dot(channels, fold)

    def write_states(l, j):
        at = slice(j * tile, (j + 1) * tile)
        shape = (c.per_tile * c.own, tile)
        same = (lax.div(iota(shape, 0), c.own) == lax.div(iota(shape, 1), c.size)).astype(BF16)
        fold = (iota((c.size, tile), 0) == lax.rem(iota((c.size, tile), 1), c.size)).astype(BF16)
        keys = lax.dot_general(
            fold, tiles(s.k[l, :, at], c.per_tile) * same, (((1,), (1,)), ((), ())), preferred_element_type=F32
        ).astype(BF16)
        fresh = tiles(s.u[l, :, at], c.per_tile) * same
        owner = lax.rem(iota((c.size, c.per_tile * c.own), 1), c.own_seqs)
        batch = 4
        for first_seq in range(0, c.own_seqs, batch):
            lhs = jnp.concatenate(
                [keys * (owner == first_seq + i).astype(BF16) for i in range(batch)], axis=0
            )
            added = dot(lhs, fresh)
            for i in range(batch):
                seq = first_seq + i
                new[l, seq, :, at] = (
                    new[l, seq, :, at] * s.decay[l, seq : seq + 1, at] + added[i * c.size : (i + 1) * c.size]
                )

    def round_states(l):
        state_loads[l].wait()
        for i in range(c.own_seqs):
            s.states16[l, i * c.size : (i + 1) * c.size] = new[l, i].astype(BF16)

    for l in range(BLOCKS):
        acc = None
        if l:
            for p in range(c.parts):
                mix_in(l - 1, p)
                at = slice(p * c.part, (p + 1) * c.part)
                piece = s.scaled[l, :, at]
                if p == 0:
                    for j in range(c.chunks):
                        for i in range(4):
                            w_loads[l, j, i].wait()
                last = p + 1 == c.parts
                if not last:
                    for j in range(c.chunks):
                        for i in range(4):
                            val = dot(piece, s.w[l, i, at, j * tile : (j + 1) * tile])
                            s.acc[j, i] = val if p == 0 else s.acc[j, i] + val

            def acc(j, i, piece=piece, at=at, l=l):
                return s.acc[j, i] + dot(piece, s.w[l, i, at, j * tile : (j + 1) * tile])

        produce(l, 0, acc)
        produce_small(l)
        for j in range(1, c.chunks):
            produce(l, j, acc)
            if j == 1:
                cross(l, 0)
            elif j == 2:
                cross(l, -1)
        for j in ([] if c.chunks > 2 else [-1]) + list(range(0 if c.chunks == 1 else 1, c.chunks)):
            cross(l, j)
        if l == 0:
            load_weights(1)
            load_rest(1)
            setup()
            round_states(0)
        finish(l, -1)
        prepare(l)
        finish(l, 0)
        for j in range(1, c.chunks):
            finish(l, j)
            recur(l, j - 1)
        if l:
            mix_end(l - 1)
        recur(l, c.chunks - 1)
        for j in range(c.chunks):
            forward(l, j)
        wo_loads[l].wait()
        for j in range(c.chunks):
            gather(l, j)
        for p in range(c.parts):
            mix_out(l, p)
        for j in range(c.chunks):
            write_states(l, j)
        if l == 0:
            round_states(1)
    for p in range(c.parts):
        mix_in(BLOCKS - 1, p)
    back = dot(s.hot[...], s.last[...])
    old = s.resid[...].reshape(c.rows, c.feat).astype(F32)
    tokens[...] = jnp.where(s.alive[:, :1] > 0.0, back, old).astype(BF16).reshape(tokens.shape)
    mix_end(BLOCKS - 1)


def run_main(c, args):
    ab = 2 * args[6].shape[1]
    half = 2 * c.tile
    chips, n = c.chips, c.n
    dma = lambda *shape: pltpu.SemaphoreType.DMA(shape)
    buf = lambda *shape: pltpu.VMEM(shape, BF16)
    wide = lambda *shape: pltpu.VMEM(shape, F32)
    every = 1 + c.chunks
    scratch = dict(
        resid=buf(c.seqs, c.slots, c.feat),
        last=buf(c.packed, c.feat),
        hot=buf(c.rows, c.packed),
        alive=wide(c.rows, 128),
        k=buf(BLOCKS, c.own, c.cols),
        u=buf(BLOCKS, c.own, c.cols),
        decay=wide(BLOCKS, c.own_seqs, c.cols),
        scaling=buf(BLOCKS, c.feat),
        wab=buf(BLOCKS, ab, c.feat),
        speed=wide(BLOCKS, c.heads),
        bias=wide(BLOCKS, c.heads),
        channel=buf(BLOCKS, c.size),
        shrink=wide(BLOCKS, c.own_seqs, c.slots, c.heads),
        w=buf(BLOCKS, 4, c.feat, c.cols),
        wo=buf(BLOCKS, c.cols, c.feat),
        states16=buf(BLOCKS, c.own_seqs * c.size, c.cols),
        counts=pltpu.VMEM((n, 8, c.lanes), jnp.int32),
        blocks=buf(c.tile, c.tile),
        spread=buf(c.per_tile, c.tile, c.tile),
        mask=buf(c.groups, 2 * c.own, c.tile),
        gain=wide(BLOCKS, 8, c.tile),
        pick=buf(c.own, c.win),
        place=buf(c.win, c.own),
        live=wide(c.own, 128),
        factor=wide(c.own, 128),
        dec=wide(c.own, c.cols),
        beta=wide(c.own, c.cols),
        h=wide(c.packed, c.feat),
        scaled=buf(BLOCKS, c.packed, c.feat),
        acc=wide(c.chunks, 4, c.packed, c.tile),
        x=buf(BLOCKS, c.chunks, 2, c.packed, half),
        pair=buf(BLOCKS, c.chunks, c.packed, half),
        sum=buf(BLOCKS, c.chunks, c.packed, half),
        far=buf(BLOCKS, c.chunks, chips - 1, c.chip_win, half),
        out=buf(BLOCKS, c.chunks, c.win, half),
        fin=buf(BLOCKS, c.chunks, 2, c.win, half),
        x_small=buf(BLOCKS, 2, c.packed, ab),
        pair_small=buf(BLOCKS, c.packed, ab),
        sum_small=buf(BLOCKS, c.packed, ab),
        far_small=buf(BLOCKS, chips - 1, c.chip_win, ab),
        out_small=buf(BLOCKS, c.win, ab),
        fin_small=buf(BLOCKS, 2, c.win, ab),
        y=buf(BLOCKS, c.chunks, n, c.win, c.tile),
        gated=buf(c.packed, c.cols),
        sent=buf(BLOCKS, c.parts, c.packed, c.part),
        came=buf(BLOCKS, c.parts, c.packed, c.part),
        over=buf(BLOCKS, c.parts, c.packed, c.part),
        full=buf(BLOCKS, c.parts, c.packed, c.part),
        small_sem=dma(8),
        w_sem=dma(BLOCKS, c.chunks, 4),
        wo_sem=dma(BLOCKS),
        state_sem=dma(BLOCKS),
        count_s=dma(n - 1),
        count_r=dma(n - 1),
        first_s=dma(BLOCKS, every),
        first_r=dma(BLOCKS, every),
        second_s=dma(BLOCKS, every, chips - 1),
        second_r=dma(BLOCKS, every, chips - 1),
        third_s=dma(BLOCKS, every),
        third_r=dma(BLOCKS, every),
        yf_s=dma(BLOCKS, c.chunks, chips - 1),
        yf_r=dma(BLOCKS, c.chunks, chips - 1),
        yn_s=dma(BLOCKS, c.chunks, chips),
        yn_r=dma(BLOCKS, c.chunks, chips),
        in_s=dma(BLOCKS, c.parts),
        in_r=dma(BLOCKS, c.parts),
        over_s=dma(BLOCKS, c.parts),
        over_r=dma(BLOCKS, c.parts),
        full_s=dma(BLOCKS, c.parts),
        full_r=dma(BLOCKS, c.parts),
    )
    c.names = list(scratch)
    return pl.pallas_call(
        functools.partial(main_kernel, c),
        out_shape=[
            pltpu.VMEM(args[1].shape, BF16),
            pltpu.VMEM(args[-1].shape, F32),
        ],
        in_specs=[SMEM] + [HBM] * 14,
        out_specs=[VMEM] * 2,
        scratch_shapes=list(scratch.values()),
        compiler_params=pltpu.CompilerParams(
            collective_id=1, has_side_effects=True, vmem_limit_bytes=38 * 1024 * 1024
        ),
        name="blocks",
    )(*[args[0]] + [pltpu.with_memory_space_constraint(x, pltpu.HBM) for x in args[1:]])


def body(
    n, m, resid, counts, wq, wk, wv, wz, wa, wb, wo, speed, bias, scaling, channel, shrink, states,
):
    c = sizes(n, m, resid, counts, wq, speed)
    turned = [jnp.swapaxes(w, 1, 2) for w in (wa, wb)]
    tokens, new = run_main(
        c, (counts, resid, wq, wk, wv, wz, *turned, wo, speed, bias, scaling, channel, shrink, states)
    )
    return tokens, new


def solution(mesh):
    in_specs = (
        P("grp", None, "dp"),
        P(("grp", "dp")),
        P(None, "dp", "tp"),
        P(None, "dp", "tp"),
        P(None, "dp", "tp"),
        P(None, "dp", "tp"),
        P(),
        P(),
        P(None, "tp", "dp"),
        P(None, "tp"),
        P(None, "tp"),
        P(None, "dp"),
        P(),
        P(None, ("grp", "dp"), None, "tp"),
        P(None, ("grp", "dp"), None, "tp"),
    )
    out_specs = (P("grp", None, "dp"), P(None, ("grp", "dp"), None, "tp"))
    run = functools.partial(body, mesh.shape["dp"], mesh.shape["tp"])
    return jax.shard_map(run, mesh=mesh, in_specs=in_specs, out_specs=out_specs, check_vma=False)
```

```python
import functools
import types

import jax
import jax.numpy as jnp
from jax import lax
from jax.experimental import pallas as pl
from jax.experimental.pallas import tpu as pltpu
from jax.sharding import PartitionSpec as P

BLOCKS = 2
EPS = 1e-06
F32 = jnp.float32
BF16 = jnp.bfloat16
MESH = pl.DeviceIdType.MESH
VMEM = pl.BlockSpec(memory_space=pltpu.VMEM)
HBM = pl.BlockSpec(memory_space=pltpu.HBM)
SMEM = pl.BlockSpec(memory_space=pltpu.SMEM)


def iota(shape, dim):
    return lax.broadcasted_iota(jnp.int32, shape, dim)


def dot(a, b):
    return jnp.dot(a, b, preferred_element_type=F32)


def narrow(a, b):
    return lax.dot_general(a, b, (((1,), (1,)), ((), ())), preferred_element_type=F32)


def tiles(ref, count):
    return jnp.concatenate([ref] * count, axis=0)


def sizes(n, m, resid, counts, wq, speed):
    c = types.SimpleNamespace(n=n, m=m)
    c.seqs, c.slots, c.feat = resid.shape
    c.own_seqs = counts.shape[0]
    c.cols = wq.shape[2]
    c.heads = speed.shape[1]
    c.size = c.cols // c.heads
    c.own = c.own_seqs * c.slots
    c.rows = c.seqs * c.slots
    c.packed = c.seqs * 3 // 2
    c.chips = n // 2
    c.per_chip = 2 * c.own_seqs
    c.chip_win = c.packed - (c.chips - 1) * c.per_chip
    c.win = c.packed - (n - 1) * c.own_seqs
    c.tile = min(256, c.cols)
    c.chunks = c.cols // c.tile
    c.per_tile = c.tile // c.size
    c.groups = c.own_seqs // c.per_tile
    c.parts = 8
    c.pairs = c.parts // 2
    c.part = c.feat // c.parts
    c.lanes = -(-c.seqs // 128) * 128
    return c


def remote(src, dst, send_sem, recv_sem, axis, peer):
    return pltpu.make_async_remote_copy(
        src_ref=src, dst_ref=dst, send_sem=send_sem, recv_sem=recv_sem,
        device_id={axis: peer}, device_id_type=MESH,
    )


def line(m, sent, mid, came, over, full, sems, over_r):
    z = lax.axis_index("tp")
    half = m // 2
    left = z < half
    depth = jnp.where(left, z, m - 1 - z)
    toward = jnp.where(left, z + 1, z - 1)
    away = lax.rem(jnp.where(left, z - 1, z + 1) + m, m)
    centre = depth == half - 1
    in_s, over_s, full_s, in_r, full_r = sems
    own = sent if half == 1 else mid

    def inward(src, p):
        return remote(src.at[p], came.at[p], in_s, in_r.at[p], "tp", toward)

    def across(p):
        return remote(own.at[p], over.at[p], over_s, over_r.at[p], "tp", toward)

    def outward(p):
        return remote(full.at[p], full.at[p], full_s, full_r.at[p], "tp", away)

    def start(p):
        if half > 1:

            @pl.when(depth == 0)
            def _():
                inward(sent, p).start()

    def relay(p):
        if half > 1:

            @pl.when(depth > 0)
            def _():
                inward(mid, p).wait_recv()
                mid[p] = (sent[p].astype(F32) + came[p].astype(F32)).astype(BF16)

        @pl.when(centre)
        def _():
            across(p).start()

        if half > 2:

            @pl.when((depth > 0) & jnp.logical_not(centre))
            def _():
                inward(mid, p).start()

    def take(p):
        @pl.when(centre)
        def _():
            across(p).wait_recv()
            full[p] = (own[p].astype(F32) + over[p].astype(F32)).astype(BF16)

        if half > 1:

            @pl.when(jnp.logical_not(centre))
            def _():
                outward(p).wait_recv()

            @pl.when(depth > 0)
            def _():
                outward(p).start()

    def end():
        @pl.when(centre)
        def _():
            remote(own, over, over_s, over_r.at[0], "tp", toward).wait_send()

        if half > 1:

            @pl.when(jnp.logical_not(centre))
            def _():
                remote(sent, came, in_s, in_r.at[0], "tp", toward).wait_send()

            @pl.when(depth > 0)
            def _():
                remote(full, full, full_s, full_r.at[0], "tp", away).wait_send()

    return types.SimpleNamespace(start=start, relay=relay, take=take, end=end)


def main_kernel(
    c, counts, resid, wq, wk, wv, wz, wa, wb, wo, speed, bias, scaling, channel, shrink, states,
    tokens, new, *scratch,
):
    s = types.SimpleNamespace(**dict(zip(c.names, scratch)))
    lines = [
        line(
            c.m, s.sent.at[l], s.mid.at[l], s.came.at[l], s.over.at[l], s.full.at[l],
            (s.line_s.at[0], s.line_s.at[1], s.line_s.at[2], s.in_r, s.full_r), s.over_r.at[l],
        )
        for l in range(BLOCKS)
    ]
    n, m, chips, tile = c.n, c.m, c.chips, c.tile
    me = lax.axis_index("dp")
    z = lax.axis_index("tp")
    core = lax.rem(me, 2)
    chip = lax.div(me, 2)
    partner = me + 1 - 2 * core
    others = [lax.rem(me + 2 * d, n) for d in range(1, chips)]
    sources = [lax.rem(me + n - 2 * d, n) for d in range(1, chips)]
    def load(src, dst, sem):
        copy = pltpu.make_async_copy(src, dst, sem)
        copy.start()
        return copy

    all_heads = wa.shape[1]
    ab = 2 * all_heads
    feats = pl.ds(pl.multiple_of(me * c.feat, 128), c.feat)
    early = [
        load(src, dst, s.small_sem.at[i])
        for i, (src, dst) in enumerate(
            [
                (resid, s.resid), (scaling, s.scaling),
                (wa.at[:, :, feats], s.wab.at[:, pl.ds(0, all_heads)]),
                (wb.at[:, :, feats], s.wab.at[:, pl.ds(all_heads, all_heads)]),
            ]
        )
    ]
    wo_loads, state_loads = {}, {}

    def load_weights(l, j):
        for i, w in enumerate((wq, wk, wv, wz)):
            load(w.at[l, :, pl.ds(j * tile, tile)], s.w.at[l, j, :, pl.ds(i * tile, tile)], s.w_sem.at[j])

    def wait_weights(l, j):
        pltpu.make_async_copy(s.w.at[l, j], s.w.at[l, j], s.w_sem.at[j]).wait()

    def load_rest(l):
        state_loads[l] = load(states.at[l], new.at[l], s.state_sem.at[l])
        wo_loads[l] = load(wo.at[l], s.wo.at[l], s.wo_sem.at[l])

    load_weights(0, 0)
    late = [
        load(src, dst, s.small_sem.at[len(early) + i])
        for i, (src, dst) in enumerate(
            [(speed, s.speed), (bias, s.bias), (channel, s.channel), (shrink, s.shrink)]
        )
    ]
    dp_peers = [lax.rem(me + d, n) for d in range(1, n)]
    swaps = [
        remote(s.counts.at[me], s.counts.at[me], s.count_sem.at[0], s.count_sem.at[1], "dp", peer)
        for peer in dp_peers
    ]
    barrier = pltpu.get_barrier_semaphore()

    def greet():
        for axis, peers in (("dp", dp_peers), ("tp", [lax.rem(z + 1, m), lax.rem(z + m - 1, m)])):
            for peer in peers:
                pl.semaphore_signal(barrier, inc=1, device_id={axis: peer}, device_id_type=MESH)

    def fill_counts():
        lane = iota((8, c.lanes), 1) - me * c.own_seqs
        mine = jnp.zeros((8, c.lanes), jnp.int32)
        for i in range(c.own_seqs):
            mine = jnp.where(lane == i, counts[i], mine)
        s.counts[me] = mine

    def swap_counts():
        pl.semaphore_wait(barrier, n + 1)
        for copy in swaps:
            copy.start()

    greet()
    fill_counts()
    swap_counts()

    def constants():
        row = lax.div(iota((tile, tile), 0), c.size)
        col = lax.div(iota((tile, tile), 1), c.size)
        s.blocks[...] = (row == col).astype(BF16)
        for g in range(c.groups):
            r = lax.rem(iota((2 * c.own, tile), 0), c.own_seqs)
            k = g * c.per_tile + lax.div(iota((2 * c.own, tile), 1), c.size)
            s.mask[g] = (r == k).astype(BF16)

    for j in range(1, c.chunks):
        load_weights(0, j)
    constants()
    load_early = lambda: [copy.wait() for copy in early]
    flat = lambda: s.resid[...].reshape(c.rows, c.feat)

    def raw_small():
        load_early()
        wide = flat().astype(F32)
        bent = (wide * s.scaling[...].astype(F32)[:1]).astype(BF16)
        s.bent[...] = bent
        s.raw_small[0] = narrow(bent, s.wab[0]).astype(BF16)
        squares = jnp.sum(wide * wide, axis=1, keepdims=True)
        s.raw_small[1] = jnp.broadcast_to(squares, (c.rows, ab)).astype(BF16)
        raw_swap(-1).start()

    def raw_swap(j):
        x, pair = (s.raw_small, s.raw_pair_small) if j < 0 else (s.raw, s.raw_pair)
        return remote(x.at[1 - core], pair, s.raw_s.at[j + 1], s.first_r.at[j + 1], "dp", partner)

    def raw_first():
        wait_weights(0, 0)
        val = dot(s.bent[...], s.w[0, 0]).astype(BF16)
        s.raw[0] = val[:, : 2 * tile]
        s.raw[1] = val[:, 2 * tile :]
        raw_swap(0).start()

    def wait_counts():
        every = s.counts.at[pl.ds(0, n - 1)]
        swap = remote(every, every, s.count_sem.at[0], s.count_sem.at[1], "dp", partner)
        swap.wait()

    def raw_cross(j):
        x, pair = (s.raw_small, s.raw_pair_small) if j < 0 else (s.raw, s.raw_pair)
        raw_swap(j).wait_recv()
        total = (x[core].astype(F32) + pair[...].astype(F32)).astype(BF16)
        bufs(0, j)[2][...] = dot(s.into[...], total).astype(BF16)
        for d in range(chips - 1):
            second(0, j, d).start()

    raw_small()
    raw_first()
    load_rest(0)
    wait_counts()
    total = s.counts[0]
    for d in range(1, n):
        total = total + s.counts[d]
    row_counts = total.astype(F32)
    row_bf16 = row_counts.astype(BF16)

    def columns(count, seq, slot):
        lanes = iota((count, c.lanes), 1)
        all_counts = jnp.broadcast_to(row_counts[:1], (count, c.lanes))
        start = jnp.sum(jnp.where(lanes < seq, all_counts, 0.0), axis=1, keepdims=True)
        size = jnp.sum(jnp.where(lanes == seq, all_counts, 0.0), axis=1, keepdims=True)
        slot = slot[:, :1].astype(F32)
        return start + slot, slot < size

    def rows_of(seq, slot):
        index = iota(seq.shape, 0)
        start = dot(row_bf16, (index < seq).astype(BF16))[:1]
        size = dot(row_bf16, (index == seq).astype(BF16))[:1]
        slot = slot[:1].astype(F32)
        return start + slot, slot < size

    def pack():
        shape = (c.lanes, c.rows)
        pos, live = rows_of(lax.div(iota(shape, 1), c.slots), lax.rem(iota(shape, 1), c.slots))
        s.into[...] = jnp.where((iota((c.packed, c.rows), 0).astype(F32) == pos) & live, 1.0, 0.0).astype(BF16)

    pack()

    def produce(l, j):
        at = slice((c.pairs - 1) * 2 * c.part, c.feat)
        if l:
            val = s.acc[j] + dot(s.scaled[:, at], s.w[l, j, at])
        else:
            wait_weights(l, j)
            val = dot(s.scaled[...], s.w[l, j])
        val = val.astype(BF16)
        s.x[l, j, 0] = val[:, : 2 * tile]
        s.x[l, j, 1] = val[:, 2 * tile :]
        first(l, j).start()

    def pack_rest():
        h = dot(s.into[...], flat())
        s.h[...] = h
        s.scaled[...] = (h * s.scaling[...].astype(F32)[:1]).astype(BF16)

    def produce_small(l):
        at = slice((c.pairs - 1) * 2 * c.part, c.feat)
        h = s.h[...]
        s.x_small[l, 0] = (s.acc_small[...] + narrow(s.scaled[:, at], s.wab[l, :, at])).astype(BF16)
        squares = jnp.sum(h * h, axis=1, keepdims=True)
        s.x_small[l, 1] = jnp.broadcast_to(squares, (c.packed, ab)).astype(BF16)
        first(l, -1).start()

    def bufs(l, j):
        if j < 0:
            return s.x_small.at[l], s.pair_small.at[l], s.sum_small.at[l], s.far_small.at[l], s.out_small.at[l], s.fin_small.at[l]
        return s.x.at[l, j], s.pair.at[l, j], s.sum.at[l, j], s.far.at[l, j], s.out.at[l, j], s.fin.at[l, j]

    def kind(j):
        return min(j + 1, 1)

    def first(l, j):
        x, pair, *_ = bufs(l, j)
        return remote(x.at[1 - core], pair, s.first_s.at[kind(j)], s.first_r.at[j + 1], "dp", partner)

    def second(l, j, d):
        _, _, own, far, *_ = bufs(l, j)
        there = pl.multiple_of(lax.div(others[d], 2) * c.per_chip, 16)
        return remote(
            own.at[pl.ds(there, c.chip_win)], far.at[d], s.second_s.at[kind(j), d], s.second_r.at[j + 1, d],
            "dp", others[d],
        )

    def third(l, j):
        *_, out, fin = bufs(l, j)
        return remote(out, fin.at[core], s.third_s.at[kind(j)], s.third_r.at[j + 1], "dp", partner)

    def cross(l, j):
        x, pair, own, *_ = bufs(l, j)
        first(l, j).wait_recv()
        own[...] = (x[core].astype(F32) + pair[...].astype(F32)).astype(BF16)
        for d in range(chips - 1):
            second(l, j, d).start()

    def finish(l, j):
        x, pair, own, far, out, fin = bufs(l, j)
        for d in range(chips - 1):
            second(l, j, d).wait_recv()

        def reduced(which):
            at = pl.multiple_of(which * c.own_seqs, 16)
            val = own[pl.ds(pl.multiple_of(chip * c.per_chip + at, 16), c.win), :].astype(F32)
            for d in range(chips - 1):
                val = val + far[d, pl.ds(at, c.win), :].astype(F32)
            return val.astype(BF16)

        out[...] = reduced(1 - core)
        third(l, j).start()
        fin[core] = reduced(core)

    def prepare(l):
        third(l, -1).wait_recv()
        pick = s.pick[...]
        heads = c.heads
        few = dot(pick, s.fin_small[l, 0]).astype(BF16)
        squares = dot(pick, s.fin_small[l, 1])[:, :1]
        factor = lax.rsqrt(squares / (c.feat * n) + EPS)
        s.factor[...] = jnp.broadcast_to(factor, s.factor.shape)
        at = iota((ab, heads), 1) + z * heads
        pa = dot(few, (iota((ab, heads), 0) == at).astype(BF16)) * factor
        pb = dot(few, (iota((ab, heads), 0) == at + all_heads).astype(BF16)) * factor
        arg = pa + s.bias[...][l : l + 1]
        soft = jnp.maximum(arg, 0.0) + jnp.log1p(jnp.exp(-jnp.abs(arg)))
        extra = jnp.concatenate([s.shrink[l, :, t, :] for t in range(c.slots)], axis=0)
        dec = jnp.exp(extra - jnp.exp(s.speed[...][l : l + 1]) * soft)
        dec = jnp.where(s.live[:, :1] > 0.0, dec, 1.0)
        wide = (iota((heads, c.cols), 0) == lax.div(iota((heads, c.cols), 1), c.size)).astype(BF16)
        both = jnp.concatenate([dec, jax.nn.sigmoid(pb)], axis=0)
        high = both.astype(BF16)
        low = (both - high.astype(F32)).astype(BF16)
        spread = dot(jnp.concatenate([high, low], axis=0), wide)
        s.dec[...] = spread[: c.own] + spread[2 * c.own : 3 * c.own]
        s.beta[...] = spread[c.own : 2 * c.own] + spread[3 * c.own :]

    def recur(l, j):
        at = slice(j * tile, (j + 1) * tile)
        third(l, j).wait_recv()
        pick = s.pick[...]
        factor = s.factor[:, :1]
        qk = dot(pick, s.fin[l, j, 0]) * factor
        vz = dot(pick, s.fin[l, j, 1]) * factor
        qk = qk * jax.nn.sigmoid(qk)
        vz = vz * jax.nn.sigmoid(vz)
        q, k = qk[:, :tile], qk[:, tile:]
        v, zed = vz[:, :tile], vz[:, tile:]
        both = jnp.concatenate([k, q], axis=0)
        low = iota((2 * c.own, 128), 1) < c.size
        copies = []
        for i in range(tile // 128):
            here = both[:, i * 128 : (i + 1) * 128]
            turned = pltpu.roll(here, c.size, 1)
            copies += [jnp.where(low, here, turned), jnp.where(low, turned, here)]
        lhs = []
        for one in copies:
            wide = jnp.concatenate([one.astype(BF16)] * (tile // 128), axis=1)
            lhs.append(jnp.concatenate([wide * s.mask[g] for g in range(c.groups)], axis=1))
        read = dot(jnp.concatenate(lhs, axis=0), s.states16[l, :, at])
        step = lambda x, t: x[t * c.own_seqs : (t + 1) * c.own_seqs]
        names, prods = [], []
        for t in range(c.slots):
            names.append(("n", t, t))
            prods.append(step(q, t) * step(q, t))
            for i in range(t + 1):
                names.append(("q", i, t))
                prods.append(step(k, i) * step(q, t))
                names.append(("k", i, t))
                prods.append(step(k, i) * step(k, t))
        pairs = dot(jnp.concatenate(prods, axis=0).astype(BF16), s.blocks[...])
        pairs = {name: step(pairs, i) for i, name in enumerate(names)}
        nk = [lax.rsqrt(pairs["k", t, t] + EPS) for t in range(c.slots)]
        nq = [lax.rsqrt(pairs["n", t, t] + EPS) * c.size ** (-0.5) for t in range(c.slots)]
        s.k[l, :, at] = (k * jnp.concatenate(nk, axis=0)).astype(BF16)
        lane_head = lax.div(iota((2 * c.own, tile), 1), c.size)
        reads = read[: 2 * c.own]
        for h in range(1, c.per_tile):
            reads = jnp.where(lane_head == h, read[2 * c.own * h : 2 * c.own * (h + 1)], reads)
        rk = reads[: c.own]
        rq = reads[c.own :]
        dec = s.dec[:, at]
        beta = s.beta[:, at]
        fresh, outs = [], []
        whole = None
        for t in range(c.slots):
            g = step(dec, t)
            whole = g if whole is None else whole * g
            fresh = [(u * g) for u in fresh]
            guess = whole * step(rk, t)
            for i in range(t):
                guess = guess + pairs["k", i, t] * nk[i] * fresh[i]
            fresh.append(step(beta, t) * (step(v, t) - guess * nk[t]))
            o = whole * step(rq, t)
            for i in range(t + 1):
                o = o + pairs["q", i, t] * nk[i] * fresh[i]
            outs.append(o * nq[t])
        s.u[l, :, at] = jnp.concatenate(fresh, axis=0).astype(BF16)
        s.decay[l, :, at] = whole
        o = jnp.concatenate(outs, axis=0)
        total = dot((o * o).astype(BF16), s.blocks[...])
        o = o * lax.rsqrt(total / c.size + EPS) * s.gain[l, :1] * zed
        s.y[l, me, j] = dot(s.place[...], o.astype(BF16)).astype(BF16)
        for d in range(chips - 1):
            y_far(l, j, d).start()
        y_near(l, j, 0).start()

    def y_far(l, j, d):
        here = s.y.at[l, me, j]
        return remote(here, here, s.yf_s.at[d], s.yf_r.at[j, d], "dp", others[d])

    def y_near(l, j, d):
        source = me if d == 0 else sources[d - 1]
        here = s.y.at[l, source, j]
        return remote(here, here, s.yn_s.at[d], s.yn_r.at[0], "dp", partner)

    def forward(l, j):
        for d in range(chips - 1):
            y_far(l, j, d).wait_recv()
            y_near(l, j, d + 1).start()

    def near_all(l):
        every = s.y.at[l, pl.ds(0, chips)]
        remote(every, every, s.yn_s.at[0], s.yn_r.at[0], "dp", partner).wait_recv()

    def sent_all(l):
        if l:
            first(l, -1).wait_send()
        else:
            for j in (-1, 0):
                raw_swap(j).wait_send()
        if l or c.chunks > 1:
            done = s.pair.at[l] if l else s.pair.at[l, pl.ds(1, c.chunks - 1)]
            remote(done, done, s.first_s.at[1], s.first_r.at[0], "dp", partner).wait_send()
        for d in range(chips - 1):
            second(l, -1, d).wait_send()
            done = s.far.at[l, :, d]
            remote(done, done, s.second_s.at[1, d], s.second_r.at[0, d], "dp", others[d]).wait_send()
            done = s.y.at[l, me]
            remote(done, done, s.yf_s.at[d], s.yf_r.at[0, d], "dp", others[d]).wait_send()
        third(l, -1).wait_send()
        done = s.out.at[l]
        remote(done, done, s.third_s.at[1], s.third_r.at[0], "dp", partner).wait_send()
        for d in range(chips):
            done = s.y.at[l, me]
            remote(done, done, s.yn_s.at[d], s.yn_r.at[0], "dp", partner).wait_send()

    def gather(l, j):
        at = slice(j * tile, (j + 1) * tile)
        s.gated[:, at] = jnp.zeros((c.packed, tile), BF16)
        for d in range(n):
            here = slice(d * c.own_seqs, d * c.own_seqs + c.win)
            s.gated[here, at] = s.gated[here, at] + s.y[l, d, j]

    def mix_mul(l, run):
        per = c.parts // 2
        at = slice(run * per * c.part, (run + 1) * per * c.part)
        val = dot(s.gated[...], s.wo[l, :, at]).astype(BF16)
        for i in range(per):
            s.sent[l, run * per + i] = val[:, i * c.part : (i + 1) * c.part]
        for i in range(per):
            lines[l].start(run * per + i)

    def mix_out(l, p):
        lines[l].relay(p)

    def mix_in(l, p):
        lines[l].take(p)
        at = slice(p * c.part, (p + 1) * c.part)
        mixed = (s.h[:, at] + s.full[l, p].astype(F32)).astype(BF16)
        s.scaled[:, at] = mixed
        if l + 1 < BLOCKS:
            mixed = mixed.astype(F32)
            s.h[:, at] = mixed
            s.scaled[:, at] = (mixed * s.scaling[...].astype(F32)[l + 1 : l + 2, at]).astype(BF16)

    def place_tokens(p):
        at = slice((p - 1) * c.part, (p + 1) * c.part)
        back = dot(s.hot[...], s.scaled[:, at])
        kept = s.resid[:, :, at].reshape(c.rows, 2 * c.part).astype(F32)
        mixed = jnp.where(s.alive[:, :1] > 0.0, back, kept).astype(BF16)
        tokens[:, :, at] = mixed.reshape(c.seqs, c.slots, 2 * c.part)

    def setup():
        r = iota((c.own, c.lanes), 0)
        pos, live = columns(c.own, lax.rem(r, c.own_seqs) + me * c.own_seqs, lax.div(r, c.own_seqs))
        offset = (iota((c.own, c.win), 1) + me * c.own_seqs).astype(F32)
        s.pick[...] = jnp.where((offset == pos) & live, 1.0, 0.0).astype(BF16)
        s.live[...] = jnp.broadcast_to(jnp.where(live, 1.0, 0.0), s.live.shape)
        shape = (c.lanes, c.own)
        pos, live = rows_of(
            lax.rem(iota(shape, 1), c.own_seqs) + me * c.own_seqs, lax.div(iota(shape, 1), c.own_seqs)
        )
        offset = (iota((c.win, c.own), 0) + me * c.own_seqs).astype(F32)
        s.place[...] = jnp.where((offset == pos) & live, 1.0, 0.0).astype(BF16)
        r = iota((c.rows, c.lanes), 0)
        pos, live = columns(c.rows, lax.div(r, c.slots), lax.rem(r, c.slots))
        offset = iota((c.rows, c.packed), 1).astype(F32)
        s.alive[...] = jnp.broadcast_to(jnp.where(live, 1.0, 0.0), s.alive.shape)
        s.hot[...] = jnp.where((offset == pos) & live, 1.0, 0.0).astype(BF16)
        fold = (iota((c.size, tile), 0) == lax.rem(iota((c.size, tile), 1), c.size)).astype(BF16)
        for l in range(BLOCKS):
            channels = jnp.broadcast_to(s.channel[...].astype(F32)[l : l + 1], (8, c.size)).astype(BF16)
            s.gain[l] = dot(channels, fold)

    def write_states(l, j):
        at = slice(j * tile, (j + 1) * tile)
        shape = (c.per_tile * c.own, tile)
        same = (lax.div(iota(shape, 0), c.own) == lax.div(iota(shape, 1), c.size)).astype(BF16)
        fold = (iota((c.size, tile), 0) == lax.rem(iota((c.size, tile), 1), c.size)).astype(BF16)
        keys = lax.dot_general(
            fold, tiles(s.k[l, :, at], c.per_tile) * same, (((1,), (1,)), ((), ())), preferred_element_type=F32
        ).astype(BF16)
        fresh = tiles(s.u[l, :, at], c.per_tile) * same
        owner = lax.rem(iota((c.size, c.per_tile * c.own), 1), c.own_seqs)
        batch = 4
        for first_seq in range(0, c.own_seqs, batch):
            lhs = jnp.concatenate(
                [keys * (owner == first_seq + i).astype(BF16) for i in range(batch)], axis=0
            )
            added = dot(lhs, fresh)
            for i in range(batch):
                seq = first_seq + i
                new[l, seq, :, at] = (
                    new[l, seq, :, at] * s.decay[l, seq : seq + 1, at] + added[i * c.size : (i + 1) * c.size]
                )

    def round_states(l):
        state_loads[l].wait()
        for i in range(c.own_seqs):
            s.states16[l, i * c.size : (i + 1) * c.size] = new[l, i].astype(BF16)

    for l in range(BLOCKS):
        if l:
            for j in range(c.chunks):
                wait_weights(l, j)
            for p in range(c.parts):
                mix_in(l - 1, p)
                if p % 2 and p + 1 < c.parts:
                    at = slice((p - 1) * c.part, (p + 1) * c.part)
                    piece = s.scaled[:, at]
                    for j in range(c.chunks):
                        val = dot(piece, s.w[l, j, at])
                        s.acc[j] = val if p == 1 else s.acc[j] + val
                    val = narrow(piece, s.wab[l, :, at])
                    s.acc_small[...] = val if p == 1 else s.acc_small[...] + val
        if l:
            produce_small(l)
            produce(l, 0)
        else:
            raw_cross(-1)
            raw_cross(0)
            pack_rest()
        for j in range(1, c.chunks):
            produce(l, j)
            if l:
                cross(l, j - 2)
            elif j > 1:
                cross(l, j - 1)
        if l:
            cross(l, c.chunks - 2)
        if l or c.chunks > 1:
            cross(l, c.chunks - 1)
        if l == 0:
            for j in range(c.chunks):
                load_weights(1, j)
            load_rest(1)
            for copy in late:
                copy.wait()
            setup()
            round_states(0)
        finish(l, -1)
        prepare(l)
        finish(l, 0)
        for j in range(1, c.chunks):
            finish(l, j)
            recur(l, j - 1)
        recur(l, c.chunks - 1)
        for j in range(c.chunks):
            forward(l, j)
            if j >= 1:
                write_states(l, j - 1)
        wo_loads[l].wait()
        near_all(l)
        for j in range(c.chunks):
            gather(l, j)
        mix_mul(l, 0)
        mix_mul(l, 1)
        write_states(l, c.chunks - 1)
        if l == 0:
            round_states(1)
        if l:
            lines[l - 1].end()
        for p in range(c.parts):
            mix_out(l, p)
        sent_all(l)
    for p in range(c.parts):
        mix_in(BLOCKS - 1, p)
        if p % 2:
            place_tokens(p)
    lines[BLOCKS - 1].end()


def run_main(c, args):
    ab = 2 * args[6].shape[1]
    half = 2 * c.tile
    chips, n = c.chips, c.n
    dma = lambda *shape: pltpu.SemaphoreType.DMA(shape)
    buf = lambda *shape: pltpu.VMEM(shape, BF16)
    wide = lambda *shape: pltpu.VMEM(shape, F32)
    every = 1 + c.chunks
    scratch = dict(
        resid=buf(c.seqs, c.slots, c.feat),
        k=buf(BLOCKS, c.own, c.cols),
        u=buf(BLOCKS, c.own, c.cols),
        decay=wide(BLOCKS, c.own_seqs, c.cols),
        scaling=buf(BLOCKS, c.feat),
        wab=buf(BLOCKS, ab, c.feat),
        speed=wide(BLOCKS, c.heads),
        bias=wide(BLOCKS, c.heads),
        channel=buf(BLOCKS, c.size),
        shrink=wide(BLOCKS, c.own_seqs, c.slots, c.heads),
        w=buf(BLOCKS, c.chunks, c.feat, 4 * c.tile),
        raw=buf(2, c.rows, half),
        raw_small=buf(2, c.rows, ab),
        raw_pair=buf(c.rows, half),
        raw_pair_small=buf(c.rows, ab),
        hot=buf(c.rows, c.packed),
        alive=wide(c.rows, 128),
        **{name: buf(BLOCKS, c.parts, c.packed, c.part) for name in ("sent", "mid", "came", "over", "full")},
        bent=buf(c.rows, c.feat),
        into=buf(c.packed, c.rows),
        wo=buf(BLOCKS, c.cols, c.feat),
        states16=buf(BLOCKS, c.own_seqs * c.size, c.cols),
        counts=pltpu.VMEM((n, 8, c.lanes), jnp.int32),
        blocks=buf(c.tile, c.tile),
        mask=buf(c.groups, 2 * c.own, c.tile),
        gain=wide(BLOCKS, 8, c.tile),
        pick=buf(c.own, c.win),
        place=buf(c.win, c.own),
        live=wide(c.own, 128),
        factor=wide(c.own, 128),
        dec=wide(c.own, c.cols),
        beta=wide(c.own, c.cols),
        h=wide(c.packed, c.feat),
        scaled=buf(c.packed, c.feat),
        acc=wide(c.chunks, c.packed, 4 * c.tile),
        acc_small=wide(c.packed, ab),
        x=buf(BLOCKS, c.chunks, 2, c.packed, half),
        pair=buf(BLOCKS, c.chunks, c.packed, half),
        sum=buf(BLOCKS, c.chunks, c.packed, half),
        far=buf(BLOCKS, c.chunks, chips - 1, c.chip_win, half),
        out=buf(BLOCKS, c.chunks, c.win, half),
        fin=buf(BLOCKS, c.chunks, 2, c.win, half),
        x_small=buf(BLOCKS, 2, c.packed, ab),
        pair_small=buf(BLOCKS, c.packed, ab),
        sum_small=buf(BLOCKS, c.packed, ab),
        far_small=buf(BLOCKS, chips - 1, c.chip_win, ab),
        out_small=buf(BLOCKS, c.win, ab),
        fin_small=buf(BLOCKS, 2, c.win, ab),
        y=buf(BLOCKS, n, c.chunks, c.win, c.tile),
        gated=buf(c.packed, c.cols),
        small_sem=dma(8),
        w_sem=dma(c.chunks),
        wo_sem=dma(BLOCKS),
        state_sem=dma(BLOCKS),
        count_sem=dma(2),
        raw_s=dma(2),
        first_s=dma(2),
        first_r=dma(every),
        second_s=dma(2, chips - 1),
        second_r=dma(every, chips - 1),
        third_s=dma(2),
        third_r=dma(every),
        yf_s=dma(chips - 1),
        yf_r=dma(c.chunks, chips - 1),
        yn_s=dma(chips),
        yn_r=dma(1),
        line_s=dma(3),
        in_r=dma(c.parts),
        full_r=dma(c.parts),
        over_r=dma(BLOCKS, c.parts),
    )
    c.names = list(scratch)
    return pl.pallas_call(
        functools.partial(main_kernel, c),
        out_shape=[
            pltpu.VMEM(args[1].shape, BF16),
            pltpu.VMEM(args[-1].shape, F32),
        ],
        in_specs=[SMEM] + [HBM] * 14,
        out_specs=[VMEM] * 2,
        scratch_shapes=list(scratch.values()),
        compiler_params=pltpu.CompilerParams(
            collective_id=1, has_side_effects=True, vmem_limit_bytes=46 * 1024 * 1024
        ),
        name="blocks",
    )(*[args[0]] + [pltpu.with_memory_space_constraint(x, pltpu.HBM) for x in args[1:]])


def store_kernel(pieces, tokens, new, tokens_out, new_out, sem):
    copies = [pltpu.make_async_copy(tokens, tokens_out, sem.at[pieces])]
    size = new.shape[1] * new.shape[0] // pieces
    for i in range(pieces):
        l, at = divmod(i * size, new.shape[1])
        at = pl.ds(at, size)
        copies.append(pltpu.make_async_copy(new.at[l, at], new_out.at[l, at], sem.at[i]))
    for copy in copies:
        copy.start()
    for copy in copies:
        copy.wait()


def store(tokens, new):
    pieces = 8
    return pl.pallas_call(
        functools.partial(store_kernel, pieces),
        out_shape=[jax.ShapeDtypeStruct(a.shape, a.dtype) for a in (tokens, new)],
        in_specs=[VMEM] * 2,
        out_specs=[HBM] * 2,
        scratch_shapes=[pltpu.SemaphoreType.DMA((pieces + 1,))],
        compiler_params=pltpu.CompilerParams(vmem_limit_bytes=1024 * 1024),
        name="store",
    )(tokens, new)


def body(
    n, m, resid, counts, wq, wk, wv, wz, wa, wb, wo, speed, bias, scaling, channel, shrink, states,
):
    c = sizes(n, m, resid, counts, wq, speed)
    turned = [jnp.swapaxes(w, 1, 2) for w in (wa, wb)]
    tokens, new = run_main(
        c, (counts, resid, wq, wk, wv, wz, *turned, wo, speed, bias, scaling, channel, shrink, states)
    )
    return store(tokens, new)


def solution(mesh):
    in_specs = (
        P("grp", None, "dp"),
        P(("grp", "dp")),
        P(None, "dp", "tp"),
        P(None, "dp", "tp"),
        P(None, "dp", "tp"),
        P(None, "dp", "tp"),
        P(),
        P(),
        P(None, "tp", "dp"),
        P(None, "tp"),
        P(None, "tp"),
        P(None, "dp"),
        P(),
        P(None, ("grp", "dp"), None, "tp"),
        P(None, ("grp", "dp"), None, "tp"),
    )
    out_specs = (P("grp", None, "dp"), P(None, ("grp", "dp"), None, "tp"))
    run = functools.partial(body, mesh.shape["dp"], mesh.shape["tp"])
    return jax.shard_map(run, mesh=mesh, in_specs=in_specs, out_specs=out_specs, check_vma=False)
```

```python
import functools
import types

import jax
import jax.numpy as jnp
from jax import lax
from jax.experimental import pallas as pl
from jax.experimental.pallas import tpu as pltpu
from jax.sharding import PartitionSpec as P

BLOCKS = 2
EPS = 1e-06
F32 = jnp.float32
BF16 = jnp.bfloat16
MESH = pl.DeviceIdType.MESH
VMEM = pl.BlockSpec(memory_space=pltpu.VMEM)
HBM = pl.BlockSpec(memory_space=pltpu.HBM)


def iota(shape, dim):
    return lax.broadcasted_iota(jnp.int32, shape, dim)


def dot(a, b):
    return jnp.dot(a, b, preferred_element_type=F32)


def narrow(a, b):
    return lax.dot_general(a, b, (((1,), (1,)), ((), ())), preferred_element_type=F32)


def tiles(ref, count):
    return jnp.concatenate([ref] * count, axis=0)


def sizes(n, m, resid, counts, wq, speed):
    c = types.SimpleNamespace(n=n, m=m)
    c.seqs, c.slots, c.feat = resid.shape
    c.own_seqs = counts.shape[0]
    c.cols = wq.shape[2]
    c.heads = speed.shape[1]
    c.size = c.cols // c.heads
    c.own = c.own_seqs * c.slots
    c.rows = c.seqs * c.slots
    c.packed = c.seqs * 3 // 2
    c.chips = n // 2
    c.per_chip = 2 * c.own_seqs
    c.chip_win = c.packed - (c.chips - 1) * c.per_chip
    c.win = c.packed - (n - 1) * c.own_seqs
    c.tile = min(256, c.cols)
    c.chunks = c.cols // c.tile
    c.per_tile = c.tile // c.size
    c.groups = c.own_seqs // c.per_tile
    c.parts = 8
    c.pairs = c.parts // 2
    c.direct = 5 if m == 4 else 0
    c.part = c.feat // c.parts
    c.lanes = -(-c.seqs // 128) * 128
    return c


def remote(src, dst, send_sem, recv_sem, axis, peer):
    return pltpu.make_async_remote_copy(
        src_ref=src, dst_ref=dst, send_sem=send_sem, recv_sem=recv_sem,
        device_id={axis: peer}, device_id_type=MESH,
    )


def line(m, direct, sent, mid, came, over, full, sems, over_r, early_r):
    z = lax.axis_index("tp")
    half = m // 2
    left = z < half
    depth = jnp.where(left, z, m - 1 - z)
    toward = jnp.where(left, z + 1, z - 1)
    away = lax.rem(jnp.where(left, z - 1, z + 1) + m, m)
    centre = depth == half - 1
    in_s, over_s, full_s, jump_s, in_r, full_r = sems
    own = sent if half == 1 else mid
    parts = sent.shape[0]
    straight = parts - direct

    def inward(src, p):
        return remote(src.at[p], came.at[p], in_s, in_r.at[p], "tp", toward)

    def across(p):
        return remote(own.at[p], over.at[p], over_s, over_r.at[p], "tp", toward)

    def outward(p):
        return remote(full.at[p], full.at[p], full_s, full_r.at[p], "tp", away)

    def early(p):
        return remote(sent.at[p], came.at[p], in_s, early_r.at[p - straight], "tp", away)

    def jump(p):
        far = 2 * toward - z
        return remote(own.at[p], over.at[p], jump_s, over_r.at[p], "tp", far)

    def start(p):
        if p >= straight:

            @pl.when(centre)
            def _():
                early(p).start()

        if half > 1:

            @pl.when(depth == 0)
            def _():
                inward(sent, p).start()

    def relay(p):
        if half > 1:

            @pl.when(depth > 0)
            def _():
                inward(mid, p).wait_recv()
                mid[p] = (sent[p].astype(F32) + came[p].astype(F32)).astype(BF16)

        @pl.when(centre)
        def _():
            if p >= straight:
                jump(p).start()
            across(p).start()

        if half > 2:

            @pl.when((depth > 0) & jnp.logical_not(centre))
            def _():
                inward(mid, p).start()

    def take(p):
        @pl.when(centre)
        def _():
            across(p).wait_recv()
            full[p] = (own[p].astype(F32) + over[p].astype(F32)).astype(BF16)

        if p >= straight:

            @pl.when(depth == 0)
            def _():
                early(p).wait_recv()
                mid[p] = (sent[p].astype(F32) + came[p].astype(F32)).astype(BF16)
                jump(p).wait_recv()
                full[p] = (mid[p].astype(F32) + over[p].astype(F32)).astype(BF16)

        elif half > 1:

            @pl.when(jnp.logical_not(centre))
            def _():
                outward(p).wait_recv()

            @pl.when(depth > 0)
            def _():
                outward(p).start()

    def end():
        @pl.when(centre)
        def _():
            remote(own, over, over_s, over_r.at[0], "tp", toward).wait_send()
            if direct:
                some = sent.at[pl.ds(0, direct)]
                remote(some, some, in_s, in_r.at[0], "tp", away).wait_send()
                remote(some, some, jump_s, in_r.at[0], "tp", away).wait_send()

        if half > 1:

            @pl.when(jnp.logical_not(centre))
            def _():
                remote(sent, came, in_s, in_r.at[0], "tp", toward).wait_send()

            @pl.when(depth > 0)
            def _():
                some = full.at[pl.ds(0, straight)]
                remote(some, some, full_s, full_r.at[0], "tp", away).wait_send()

    return types.SimpleNamespace(start=start, relay=relay, take=take, end=end)


def main_kernel(
    c, counts, resid, wq, wk, wv, wz, wa, wb, wo, speed, bias, scaling, channel, shrink, states,
    tokens, new, *scratch,
):
    s = types.SimpleNamespace(**dict(zip(c.names, scratch)))
    lines = [
        line(
            c.m, c.direct, s.sent.at[l], s.mid.at[l], s.came.at[l], s.over.at[l], s.full.at[l],
            (s.line_s.at[0], s.line_s.at[1], s.line_s.at[2], s.line_s.at[3], s.in_r, s.full_r),
            s.over_r.at[l], s.early_r.at[l],
        )
        for l in range(BLOCKS)
    ]
    n, m, chips, tile = c.n, c.m, c.chips, c.tile
    me = lax.axis_index("dp")
    z = lax.axis_index("tp")
    core = lax.rem(me, 2)
    chip = lax.div(me, 2)
    partner = me + 1 - 2 * core
    others = [lax.rem(me + 2 * d, n) for d in range(1, chips)]
    across_core = [lax.rem(partner + 2 * d, n) for d in range(1, chips)]
    def load(src, dst, sem):
        copy = pltpu.make_async_copy(src, dst, sem)
        copy.start()
        return copy

    all_heads = wa.shape[1]
    ab = 2 * all_heads
    feats = pl.ds(pl.multiple_of(me * c.feat, 128), c.feat)
    early = [
        load(src, dst, s.small_sem.at[i])
        for i, (src, dst) in enumerate(
            [
                (resid, s.resid), (scaling, s.scaling),
                (wa.at[:, :, feats], s.wab.at[:, pl.ds(0, all_heads)]),
                (wb.at[:, :, feats], s.wab.at[:, pl.ds(all_heads, all_heads)]),
            ]
        )
    ]
    wo_loads, state_loads = {}, {}

    def load_weights(l, j):
        for i, w in enumerate((wq, wk, wv, wz)):
            load(w.at[l, :, pl.ds(j * tile, tile)], s.w.at[l, j, :, pl.ds(i * tile, tile)], s.w_sem.at[j])

    def wait_weights(l, j):
        pltpu.make_async_copy(s.w.at[l, j], s.w.at[l, j], s.w_sem.at[j]).wait()

    def load_rest(l):
        state_loads[l] = load(states.at[l], new.at[l], s.state_sem.at[l])
        wo_loads[l] = load(wo.at[l], s.wo.at[l], s.wo_sem.at[l])

    load_weights(0, 0)
    late = [
        load(src, dst, s.small_sem.at[len(early) + i])
        for i, (src, dst) in enumerate(
            [(speed, s.speed), (bias, s.bias), (channel, s.channel), (shrink, s.shrink)]
        )
    ]
    dp_peers = [lax.rem(me + d, n) for d in range(1, n)]
    swaps = [
        remote(s.counts.at[me], s.counts.at[me], s.count_sem.at[0], s.count_sem.at[1], "dp", peer)
        for peer in dp_peers
    ]
    tp_peers = [lax.rem(z + d, m) for d in ((1, 2, 3) if c.direct else (1, m - 1))]
    barrier = pltpu.get_barrier_semaphore()

    def greet():
        for axis, peers in (("dp", dp_peers), ("tp", tp_peers)):
            for peer in peers:
                pl.semaphore_signal(barrier, inc=1, device_id={axis: peer}, device_id_type=MESH)

    def fill_counts():
        lane = iota((8, c.lanes), 1) - me * c.own_seqs
        mine = jnp.zeros((8, c.lanes), jnp.int32)
        for i in range(c.own_seqs):
            mine = jnp.where(lane == i, s.own_counts[i], mine)
        s.counts[me] = mine

    def swap_counts():
        pl.semaphore_wait(barrier, len(dp_peers) + len(tp_peers))
        for copy in swaps:
            copy.start()

    own_counts = load(counts, s.own_counts, s.small_sem.at[8])
    greet()
    own_counts.wait()
    fill_counts()
    swap_counts()

    def constants():
        row = lax.div(iota((tile, tile), 0), c.size)
        col = lax.div(iota((tile, tile), 1), c.size)
        s.blocks[...] = (row == col).astype(BF16)
        for g in range(c.groups):
            r = lax.rem(iota((2 * c.own, tile), 0), c.own_seqs)
            k = g * c.per_tile + lax.div(iota((2 * c.own, tile), 1), c.size)
            s.mask[g] = (r == k).astype(BF16)

    for j in range(1, c.chunks):
        load_weights(0, j)
    constants()
    load_early = lambda: [copy.wait() for copy in early]
    flat = lambda: s.resid[...].reshape(c.rows, c.feat)

    def raw_small():
        load_early()
        wide = flat().astype(F32)
        bent = (wide * s.scaling[...].astype(F32)[:1]).astype(BF16)
        s.bent[...] = bent
        s.raw_small[0] = narrow(bent, s.wab[0]).astype(BF16)
        squares = jnp.sum(wide * wide, axis=1, keepdims=True)
        s.raw_small[1] = jnp.broadcast_to(squares, (c.rows, ab)).astype(BF16)
        raw_swap(-1).start()

    def raw_swap(j):
        x, pair = (s.raw_small, s.raw_pair_small) if j < 0 else (s.raw, s.raw_pair)
        return remote(x.at[1 - core], pair, s.raw_s.at[j + 1], s.first_r.at[j + 1], "dp", partner)

    def raw_first():
        wait_weights(0, 0)
        val = dot(s.bent[...], s.w[0, 0]).astype(BF16)
        s.raw[0] = val[:, : 2 * tile]
        s.raw[1] = val[:, 2 * tile :]
        raw_swap(0).start()

    def wait_counts():
        every = s.counts.at[pl.ds(0, n - 1)]
        swap = remote(every, every, s.count_sem.at[0], s.count_sem.at[1], "dp", partner)
        swap.wait()

    def raw_cross(j):
        x, pair = (s.raw_small, s.raw_pair_small) if j < 0 else (s.raw, s.raw_pair)
        raw_swap(j).wait_recv()
        total = (x[core].astype(F32) + pair[...].astype(F32)).astype(BF16)
        bufs(0, j)[2][...] = dot(s.into[...], total).astype(BF16)
        for d in range(chips - 1):
            second(0, j, d).start()

    raw_small()
    raw_first()
    load_rest(0)
    wait_counts()
    total = s.counts[0]
    for d in range(1, n):
        total = total + s.counts[d]
    row_counts = total.astype(F32)
    row_bf16 = row_counts.astype(BF16)

    def columns(count, seq, slot):
        lanes = iota((count, c.lanes), 1)
        all_counts = jnp.broadcast_to(row_counts[:1], (count, c.lanes))
        start = jnp.sum(jnp.where(lanes < seq, all_counts, 0.0), axis=1, keepdims=True)
        size = jnp.sum(jnp.where(lanes == seq, all_counts, 0.0), axis=1, keepdims=True)
        slot = slot[:, :1].astype(F32)
        return start + slot, slot < size

    def rows_of(seq, slot):
        index = iota(seq.shape, 0)
        start = dot(row_bf16, (index < seq).astype(BF16))[:1]
        size = dot(row_bf16, (index == seq).astype(BF16))[:1]
        slot = slot[:1].astype(F32)
        return start + slot, slot < size

    def pack():
        shape = (c.lanes, c.rows)
        pos, live = rows_of(lax.div(iota(shape, 1), c.slots), lax.rem(iota(shape, 1), c.slots))
        s.into[...] = jnp.where((iota((c.packed, c.rows), 0).astype(F32) == pos) & live, 1.0, 0.0).astype(BF16)

    pack()

    def produce(l, j):
        at = slice((c.pairs - 1) * 2 * c.part, c.feat)
        if l:
            val = s.acc[j] + dot(s.scaled[:, at], s.w[l, j, at])
        else:
            wait_weights(l, j)
            val = dot(s.scaled[...], s.w[l, j])
        val = val.astype(BF16)
        s.x[l, j, 0] = val[:, : 2 * tile]
        s.x[l, j, 1] = val[:, 2 * tile :]
        first(l, j).start()

    def pack_rest():
        h = dot(s.into[...], flat())
        s.h[...] = h
        s.scaled[...] = (h * s.scaling[...].astype(F32)[:1]).astype(BF16)

    def produce_small(l):
        at = slice((c.pairs - 1) * 2 * c.part, c.feat)
        h = s.h[...]
        s.x_small[l, 0] = (s.acc_small[...] + narrow(s.scaled[:, at], s.wab[l, :, at])).astype(BF16)
        squares = jnp.sum(h * h, axis=1, keepdims=True)
        s.x_small[l, 1] = jnp.broadcast_to(squares, (c.packed, ab)).astype(BF16)
        first(l, -1).start()

    def bufs(l, j):
        if j < 0:
            return s.x_small.at[l], s.pair_small.at[l], s.sum_small.at[l], s.far_small.at[l], s.out_small.at[l], s.fin_small.at[l]
        return s.x.at[l, j], s.pair.at[l, j], s.sum.at[l, j], s.far.at[l, j], s.out.at[l, j], s.fin.at[l, j]

    def kind(j):
        return min(j + 1, 1)

    def first(l, j):
        x, pair, *_ = bufs(l, j)
        return remote(x.at[1 - core], pair, s.first_s.at[kind(j)], s.first_r.at[j + 1], "dp", partner)

    def second(l, j, d):
        _, _, own, far, *_ = bufs(l, j)
        there = pl.multiple_of(lax.div(others[d], 2) * c.per_chip, 16)
        return remote(
            own.at[pl.ds(there, c.chip_win)], far.at[d], s.second_s.at[kind(j), d], s.second_r.at[j + 1, d],
            "dp", others[d],
        )

    def third(l, j):
        *_, out, fin = bufs(l, j)
        return remote(out, fin.at[core], s.third_s.at[kind(j)], s.third_r.at[j + 1], "dp", partner)

    def cross(l, j):
        x, pair, own, *_ = bufs(l, j)
        first(l, j).wait_recv()
        own[...] = (x[core].astype(F32) + pair[...].astype(F32)).astype(BF16)
        for d in range(chips - 1):
            second(l, j, d).start()

    def finish(l, j):
        x, pair, own, far, out, fin = bufs(l, j)
        for d in range(chips - 1):
            second(l, j, d).wait_recv()

        def reduced(which):
            at = pl.multiple_of(which * c.own_seqs, 16)
            val = own[pl.ds(pl.multiple_of(chip * c.per_chip + at, 16), c.win), :].astype(F32)
            for d in range(chips - 1):
                val = val + far[d, pl.ds(at, c.win), :].astype(F32)
            return val.astype(BF16)

        out[...] = reduced(1 - core)
        third(l, j).start()
        fin[core] = reduced(core)

    def prepare(l):
        third(l, -1).wait_recv()
        pick = s.pick[...]
        heads = c.heads
        few = dot(pick, s.fin_small[l, 0]).astype(BF16)
        squares = dot(pick, s.fin_small[l, 1])[:, :1]
        factor = lax.rsqrt(squares / (c.feat * n) + EPS)
        s.factor[...] = jnp.broadcast_to(factor, s.factor.shape)
        at = iota((ab, heads), 1) + z * heads
        pa = dot(few, (iota((ab, heads), 0) == at).astype(BF16)) * factor
        pb = dot(few, (iota((ab, heads), 0) == at + all_heads).astype(BF16)) * factor
        arg = pa + s.bias[...][l : l + 1]
        soft = jnp.maximum(arg, 0.0) + jnp.log1p(jnp.exp(-jnp.abs(arg)))
        extra = jnp.concatenate([s.shrink[l, :, t, :] for t in range(c.slots)], axis=0)
        dec = jnp.exp(extra - jnp.exp(s.speed[...][l : l + 1]) * soft)
        dec = jnp.where(s.live[:, :1] > 0.0, dec, 1.0)
        wide = (iota((heads, c.cols), 0) == lax.div(iota((heads, c.cols), 1), c.size)).astype(BF16)
        both = jnp.concatenate([dec, jax.nn.sigmoid(pb)], axis=0)
        high = both.astype(BF16)
        low = (both - high.astype(F32)).astype(BF16)
        spread = dot(jnp.concatenate([high, low], axis=0), wide)
        s.dec[...] = spread[: c.own] + spread[2 * c.own : 3 * c.own]
        s.beta[...] = spread[c.own : 2 * c.own] + spread[3 * c.own :]

    def recur(l, j):
        at = slice(j * tile, (j + 1) * tile)
        third(l, j).wait_recv()
        pick = s.pick[...]
        factor = s.factor[:, :1]
        qk = dot(pick, s.fin[l, j, 0]) * factor
        vz = dot(pick, s.fin[l, j, 1]) * factor
        qk = qk * jax.nn.sigmoid(qk)
        vz = vz * jax.nn.sigmoid(vz)
        q, k = qk[:, :tile], qk[:, tile:]
        v, zed = vz[:, :tile], vz[:, tile:]
        both = jnp.concatenate([k, q], axis=0)
        low = iota((2 * c.own, 128), 1) < c.size
        copies = []
        for i in range(tile // 128):
            here = both[:, i * 128 : (i + 1) * 128]
            turned = pltpu.roll(here, c.size, 1)
            copies += [jnp.where(low, here, turned), jnp.where(low, turned, here)]
        lhs = []
        for one in copies:
            wide = jnp.concatenate([one.astype(BF16)] * (tile // 128), axis=1)
            lhs.append(jnp.concatenate([wide * s.mask[g] for g in range(c.groups)], axis=1))
        read = dot(jnp.concatenate(lhs, axis=0), s.states16[l, :, at])
        step = lambda x, t: x[t * c.own_seqs : (t + 1) * c.own_seqs]
        names, prods = [], []
        for t in range(c.slots):
            names.append(("n", t, t))
            prods.append(step(q, t) * step(q, t))
            for i in range(t + 1):
                names.append(("q", i, t))
                prods.append(step(k, i) * step(q, t))
                names.append(("k", i, t))
                prods.append(step(k, i) * step(k, t))
        pairs = dot(jnp.concatenate(prods, axis=0).astype(BF16), s.blocks[...])
        pairs = {name: step(pairs, i) for i, name in enumerate(names)}
        nk = [lax.rsqrt(pairs["k", t, t] + EPS) for t in range(c.slots)]
        nq = [lax.rsqrt(pairs["n", t, t] + EPS) * c.size ** (-0.5) for t in range(c.slots)]
        s.k[l, :, at] = (k * jnp.concatenate(nk, axis=0)).astype(BF16)
        lane_head = lax.div(iota((2 * c.own, tile), 1), c.size)
        reads = read[: 2 * c.own]
        for h in range(1, c.per_tile):
            reads = jnp.where(lane_head == h, read[2 * c.own * h : 2 * c.own * (h + 1)], reads)
        rk = reads[: c.own]
        rq = reads[c.own :]
        dec = s.dec[:, at]
        beta = s.beta[:, at]
        fresh, outs = [], []
        whole = None
        for t in range(c.slots):
            g = step(dec, t)
            whole = g if whole is None else whole * g
            fresh = [(u * g) for u in fresh]
            guess = whole * step(rk, t)
            for i in range(t):
                guess = guess + pairs["k", i, t] * nk[i] * fresh[i]
            fresh.append(step(beta, t) * (step(v, t) - guess * nk[t]))
            o = whole * step(rq, t)
            for i in range(t + 1):
                o = o + pairs["q", i, t] * nk[i] * fresh[i]
            outs.append(o * nq[t])
        s.u[l, :, at] = jnp.concatenate(fresh, axis=0).astype(BF16)
        s.decay[l, :, at] = whole
        o = jnp.concatenate(outs, axis=0)
        total = dot((o * o).astype(BF16), s.blocks[...])
        o = o * lax.rsqrt(total / c.size + EPS) * s.gain[l, :1] * zed
        s.y[l, me, j] = dot(s.place[...], o.astype(BF16)).astype(BF16)
        for peer in others + across_core + [partner]:
            here = s.y.at[l, me, j]
            remote(here, here, s.y_s.at[0], s.y_r.at[int(j + 1 == c.chunks)], "dp", peer).start()

    def wait_y(l, last):
        chunks = c.chunks - 1 if last else pl.ds(0, c.chunks - 1)
        every = s.y.at[l, pl.ds(0, n - 1), chunks]
        remote(every, every, s.y_s.at[0], s.y_r.at[int(last)], "dp", partner).wait_recv()

    def sent_all(l):
        if l:
            first(l, -1).wait_send()
        else:
            for j in (-1, 0):
                raw_swap(j).wait_send()
        if l or c.chunks > 1:
            done = s.pair.at[l] if l else s.pair.at[l, pl.ds(1, c.chunks - 1)]
            remote(done, done, s.first_s.at[1], s.first_r.at[0], "dp", partner).wait_send()
        for d in range(chips - 1):
            second(l, -1, d).wait_send()
            done = s.far.at[l, :, d]
            remote(done, done, s.second_s.at[1, d], s.second_r.at[0, d], "dp", others[d]).wait_send()
        third(l, -1).wait_send()
        done = s.out.at[l]
        remote(done, done, s.third_s.at[1], s.third_r.at[0], "dp", partner).wait_send()
        done = s.y.at[l, pl.ds(0, n - 1)]
        remote(done, done, s.y_s.at[0], s.y_r.at[0], "dp", partner).wait_send()

    def gather(l, j):
        at = slice(j * tile, (j + 1) * tile)
        s.gated[:, at] = jnp.zeros((c.packed, tile), BF16)
        for d in range(n):
            here = slice(d * c.own_seqs, d * c.own_seqs + c.win)
            s.gated[here, at] = s.gated[here, at] + s.y[l, d, j]

    def mix_some(l):
        before = slice(0, (c.chunks - 1) * tile)
        s.mixed[...] = dot(s.gated[:, before], s.wo[l, before])

    def mix_mul(l, run):
        per = c.parts // 2
        at = slice(run * per * c.part, (run + 1) * per * c.part)
        after = slice((c.chunks - 1) * tile, c.cols)
        val = dot(s.gated[:, after], s.wo[l, after, at])
        if c.chunks > 1:
            val = val + s.mixed[:, at]
        val = val.astype(BF16)
        for i in range(per):
            s.sent[l, run * per + i] = val[:, i * c.part : (i + 1) * c.part]
        for i in range(per):
            lines[l].start(run * per + i)

    def mix_out(l, p):
        lines[l].relay(p)

    def mix_in(l, p):
        lines[l].take(p)
        at = slice(p * c.part, (p + 1) * c.part)
        mixed = (s.h[:, at] + s.full[l, p].astype(F32)).astype(BF16)
        s.scaled[:, at] = mixed
        if l + 1 < BLOCKS:
            mixed = mixed.astype(F32)
            s.h[:, at] = mixed
            s.scaled[:, at] = (mixed * s.scaling[...].astype(F32)[l + 1 : l + 2, at]).astype(BF16)

    def place_tokens(p):
        at = slice((p - 1) * c.part, (p + 1) * c.part)
        back = dot(s.hot[...], s.scaled[:, at])
        kept = s.resid[:, :, at].reshape(c.rows, 2 * c.part).astype(F32)
        mixed = jnp.where(s.alive[:, :1] > 0.0, back, kept).astype(BF16)
        tokens[:, :, at] = mixed.reshape(c.seqs, c.slots, 2 * c.part)

    def setup():
        r = iota((c.own, c.lanes), 0)
        pos, live = columns(c.own, lax.rem(r, c.own_seqs) + me * c.own_seqs, lax.div(r, c.own_seqs))
        offset = (iota((c.own, c.win), 1) + me * c.own_seqs).astype(F32)
        s.pick[...] = jnp.where((offset == pos) & live, 1.0, 0.0).astype(BF16)
        s.live[...] = jnp.broadcast_to(jnp.where(live, 1.0, 0.0), s.live.shape)
        shape = (c.lanes, c.own)
        pos, live = rows_of(
            lax.rem(iota(shape, 1), c.own_seqs) + me * c.own_seqs, lax.div(iota(shape, 1), c.own_seqs)
        )
        offset = (iota((c.win, c.own), 0) + me * c.own_seqs).astype(F32)
        s.place[...] = jnp.where((offset == pos) & live, 1.0, 0.0).astype(BF16)
        r = iota((c.rows, c.lanes), 0)
        pos, live = columns(c.rows, lax.div(r, c.slots), lax.rem(r, c.slots))
        offset = iota((c.rows, c.packed), 1).astype(F32)
        s.alive[...] = jnp.broadcast_to(jnp.where(live, 1.0, 0.0), s.alive.shape)
        s.hot[...] = jnp.where((offset == pos) & live, 1.0, 0.0).astype(BF16)
        fold = (iota((c.size, tile), 0) == lax.rem(iota((c.size, tile), 1), c.size)).astype(BF16)
        for l in range(BLOCKS):
            channels = jnp.broadcast_to(s.channel[...].astype(F32)[l : l + 1], (8, c.size)).astype(BF16)
            s.gain[l] = dot(channels, fold)

    def write_states(l, j):
        at = slice(j * tile, (j + 1) * tile)
        shape = (c.per_tile * c.own, tile)
        same = (lax.div(iota(shape, 0), c.own) == lax.div(iota(shape, 1), c.size)).astype(BF16)
        fold = (iota((c.size, tile), 0) == lax.rem(iota((c.size, tile), 1), c.size)).astype(BF16)
        keys = lax.dot_general(
            fold, tiles(s.k[l, :, at], c.per_tile) * same, (((1,), (1,)), ((), ())), preferred_element_type=F32
        ).astype(BF16)
        fresh = tiles(s.u[l, :, at], c.per_tile) * same
        owner = lax.rem(iota((c.size, c.per_tile * c.own), 1), c.own_seqs)
        batch = 4
        for first_seq in range(0, c.own_seqs, batch):
            lhs = jnp.concatenate(
                [keys * (owner == first_seq + i).astype(BF16) for i in range(batch)], axis=0
            )
            added = dot(lhs, fresh)
            for i in range(batch):
                seq = first_seq + i
                new[l, seq, :, at] = (
                    new[l, seq, :, at] * s.decay[l, seq : seq + 1, at] + added[i * c.size : (i + 1) * c.size]
                )

    def round_states(l):
        state_loads[l].wait()
        for i in range(c.own_seqs):
            s.states16[l, i * c.size : (i + 1) * c.size] = new[l, i].astype(BF16)

    for l in range(BLOCKS):
        if l:
            for j in range(c.chunks):
                wait_weights(l, j)
            for p in range(c.parts):
                mix_in(l - 1, p)
                if p % 2 and p + 1 < c.parts:
                    at = slice((p - 1) * c.part, (p + 1) * c.part)
                    piece = s.scaled[:, at]
                    for j in range(c.chunks):
                        val = dot(piece, s.w[l, j, at])
                        s.acc[j] = val if p == 1 else s.acc[j] + val
                    val = narrow(piece, s.wab[l, :, at])
                    s.acc_small[...] = val if p == 1 else s.acc_small[...] + val
        if l:
            produce_small(l)
            produce(l, 0)
        else:
            raw_cross(-1)
            raw_cross(0)
            pack_rest()
        for j in range(1, c.chunks):
            produce(l, j)
            if l:
                cross(l, j - 2)
            elif j > 1:
                cross(l, j - 1)
        if l:
            cross(l, c.chunks - 2)
        if l or c.chunks > 1:
            cross(l, c.chunks - 1)
        if l == 0:
            for j in range(c.chunks):
                load_weights(1, j)
            load_rest(1)
            for copy in late:
                copy.wait()
            setup()
            round_states(0)
        finish(l, -1)
        finish(l, 0)
        prepare(l)
        for j in range(1, c.chunks):
            finish(l, j)
            recur(l, j - 1)
        recur(l, c.chunks - 1)
        for j in range(c.chunks - 1):
            write_states(l, j)
        wo_loads[l].wait()
        if c.chunks > 1:
            wait_y(l, False)
            for j in range(c.chunks - 1):
                gather(l, j)
            mix_some(l)
        wait_y(l, True)
        gather(l, c.chunks - 1)
        mix_mul(l, 0)
        mix_mul(l, 1)
        write_states(l, c.chunks - 1)
        if l == 0:
            round_states(1)
        if l:
            lines[l - 1].end()
        for p in range(c.parts):
            mix_out(l, p)
        sent_all(l)
    for p in range(c.parts):
        mix_in(BLOCKS - 1, p)
        if p % 2:
            place_tokens(p)
    lines[BLOCKS - 1].end()


def run_main(c, args):
    ab = 2 * args[6].shape[1]
    half = 2 * c.tile
    chips, n = c.chips, c.n
    dma = lambda *shape: pltpu.SemaphoreType.DMA(shape)
    buf = lambda *shape: pltpu.VMEM(shape, BF16)
    wide = lambda *shape: pltpu.VMEM(shape, F32)
    every = 1 + c.chunks
    scratch = dict(
        resid=buf(c.seqs, c.slots, c.feat),
        k=buf(BLOCKS, c.own, c.cols),
        u=buf(BLOCKS, c.own, c.cols),
        decay=wide(BLOCKS, c.own_seqs, c.cols),
        scaling=buf(BLOCKS, c.feat),
        wab=buf(BLOCKS, ab, c.feat),
        speed=wide(BLOCKS, c.heads),
        bias=wide(BLOCKS, c.heads),
        channel=buf(BLOCKS, c.size),
        shrink=wide(BLOCKS, c.own_seqs, c.slots, c.heads),
        w=buf(BLOCKS, c.chunks, c.feat, 4 * c.tile),
        raw=buf(2, c.rows, half),
        raw_small=buf(2, c.rows, ab),
        raw_pair=buf(c.rows, half),
        raw_pair_small=buf(c.rows, ab),
        hot=buf(c.rows, c.packed),
        alive=wide(c.rows, 128),
        **{name: buf(BLOCKS, c.parts, c.packed, c.part) for name in ("sent", "mid", "came", "over", "full")},
        bent=buf(c.rows, c.feat),
        into=buf(c.packed, c.rows),
        wo=buf(BLOCKS, c.cols, c.feat),
        states16=buf(BLOCKS, c.own_seqs * c.size, c.cols),
        counts=pltpu.VMEM((n, 8, c.lanes), jnp.int32),
        blocks=buf(c.tile, c.tile),
        mask=buf(c.groups, 2 * c.own, c.tile),
        gain=wide(BLOCKS, 8, c.tile),
        pick=buf(c.own, c.win),
        place=buf(c.win, c.own),
        live=wide(c.own, 128),
        factor=wide(c.own, 128),
        dec=wide(c.own, c.cols),
        beta=wide(c.own, c.cols),
        h=wide(c.packed, c.feat),
        scaled=buf(c.packed, c.feat),
        acc=wide(c.chunks, c.packed, 4 * c.tile),
        acc_small=wide(c.packed, ab),
        x=buf(BLOCKS, c.chunks, 2, c.packed, half),
        pair=buf(BLOCKS, c.chunks, c.packed, half),
        sum=buf(BLOCKS, c.chunks, c.packed, half),
        far=buf(BLOCKS, c.chunks, chips - 1, c.chip_win, half),
        out=buf(BLOCKS, c.chunks, c.win, half),
        fin=buf(BLOCKS, c.chunks, 2, c.win, half),
        x_small=buf(BLOCKS, 2, c.packed, ab),
        pair_small=buf(BLOCKS, c.packed, ab),
        sum_small=buf(BLOCKS, c.packed, ab),
        far_small=buf(BLOCKS, chips - 1, c.chip_win, ab),
        out_small=buf(BLOCKS, c.win, ab),
        fin_small=buf(BLOCKS, 2, c.win, ab),
        y=buf(BLOCKS, n, c.chunks, c.win, c.tile),
        gated=buf(c.packed, c.cols),
        mixed=wide(c.packed, c.feat),
        own_counts=pltpu.SMEM((c.own_seqs,), jnp.int32),
        small_sem=dma(9),
        w_sem=dma(c.chunks),
        wo_sem=dma(BLOCKS),
        state_sem=dma(BLOCKS),
        count_sem=dma(2),
        raw_s=dma(2),
        first_s=dma(2),
        first_r=dma(every),
        second_s=dma(2, chips - 1),
        second_r=dma(every, chips - 1),
        third_s=dma(2),
        third_r=dma(every),
        y_s=dma(1),
        y_r=dma(2),
        line_s=dma(4),
        early_r=dma(BLOCKS, max(c.direct, 1)),
        in_r=dma(c.parts),
        full_r=dma(c.parts),
        over_r=dma(BLOCKS, c.parts),
    )
    c.names = list(scratch)
    return pl.pallas_call(
        functools.partial(main_kernel, c),
        out_shape=[
            pltpu.VMEM(args[1].shape, BF16),
            pltpu.VMEM(args[-1].shape, F32),
        ],
        in_specs=[HBM] * 15,
        out_specs=[VMEM] * 2,
        scratch_shapes=list(scratch.values()),
        compiler_params=pltpu.CompilerParams(
            collective_id=1, has_side_effects=True, vmem_limit_bytes=46 * 1024 * 1024
        ),
        name="blocks",
    )(*[pltpu.with_memory_space_constraint(x, pltpu.HBM) for x in args])


def store_kernel(pieces, tokens, new, tokens_out, new_out, sem):
    copies = [pltpu.make_async_copy(tokens, tokens_out, sem.at[pieces])]
    size = new.shape[1] * new.shape[0] // pieces
    for i in range(pieces):
        l, at = divmod(i * size, new.shape[1])
        at = pl.ds(at, size)
        copies.append(pltpu.make_async_copy(new.at[l, at], new_out.at[l, at], sem.at[i]))
    for copy in copies:
        copy.start()
    for copy in copies:
        copy.wait()


def store(tokens, new):
    pieces = 8
    return pl.pallas_call(
        functools.partial(store_kernel, pieces),
        out_shape=[jax.ShapeDtypeStruct(a.shape, a.dtype) for a in (tokens, new)],
        in_specs=[VMEM] * 2,
        out_specs=[HBM] * 2,
        scratch_shapes=[pltpu.SemaphoreType.DMA((pieces + 1,))],
        compiler_params=pltpu.CompilerParams(vmem_limit_bytes=1024 * 1024),
        name="store",
    )(tokens, new)


def body(
    n, m, resid, counts, wq, wk, wv, wz, wa, wb, wo, speed, bias, scaling, channel, shrink, states,
):
    c = sizes(n, m, resid, counts, wq, speed)
    turned = [jnp.swapaxes(w, 1, 2) for w in (wa, wb)]
    tokens, new = run_main(
        c, (counts, resid, wq, wk, wv, wz, *turned, wo, speed, bias, scaling, channel, shrink, states)
    )
    return store(tokens, new)


def solution(mesh):
    in_specs = (
        P("grp", None, "dp"),
        P(("grp", "dp")),
        P(None, "dp", "tp"),
        P(None, "dp", "tp"),
        P(None, "dp", "tp"),
        P(None, "dp", "tp"),
        P(),
        P(),
        P(None, "tp", "dp"),
        P(None, "tp"),
        P(None, "tp"),
        P(None, "dp"),
        P(),
        P(None, ("grp", "dp"), None, "tp"),
        P(None, ("grp", "dp"), None, "tp"),
    )
    out_specs = (P("grp", None, "dp"), P(None, ("grp", "dp"), None, "tp"))
    run = functools.partial(body, mesh.shape["dp"], mesh.shape["tp"])
    return jax.shard_map(run, mesh=mesh, in_specs=in_specs, out_specs=out_specs, check_vma=False)
```

```python
import functools
import types

import jax
import jax.numpy as jnp
from jax import lax
from jax.experimental import pallas as pl
from jax.experimental.pallas import tpu as pltpu
from jax.sharding import PartitionSpec as P

BLOCKS = 2
EPS = 1e-06
F32 = jnp.float32
BF16 = jnp.bfloat16
MESH = pl.DeviceIdType.MESH
VMEM = pl.BlockSpec(memory_space=pltpu.VMEM)
HBM = pl.BlockSpec(memory_space=pltpu.HBM)


def iota(shape, dim):
    return lax.broadcasted_iota(jnp.int32, shape, dim)


def dot(a, b):
    return jnp.dot(a, b, preferred_element_type=F32)


def narrow(a, b):
    return lax.dot_general(a, b, (((1,), (1,)), ((), ())), preferred_element_type=F32)


def tiles(ref, count):
    return jnp.concatenate([ref] * count, axis=0)


def sizes(n, m, resid, counts, wq, speed):
    c = types.SimpleNamespace(n=n, m=m)
    c.seqs, c.slots, c.feat = resid.shape
    c.own_seqs = counts.shape[0]
    c.cols = wq.shape[2]
    c.heads = speed.shape[1]
    c.size = c.cols // c.heads
    c.own = c.own_seqs * c.slots
    c.rows = c.seqs * c.slots
    c.packed = c.seqs * 3 // 2
    c.chips = n // 2
    c.per_chip = 2 * c.own_seqs
    c.chip_win = c.packed - (c.chips - 1) * c.per_chip
    c.win = c.packed - (n - 1) * c.own_seqs
    c.tile = min(256, c.cols)
    c.chunks = c.cols // c.tile
    c.per_tile = c.tile // c.size
    c.groups = c.own_seqs // c.per_tile
    c.parts = 8
    c.pairs = c.parts // 2
    c.direct = 3 if m == 4 else 0
    c.part = c.feat // c.parts
    c.lanes = -(-c.seqs // 128) * 128
    return c


def remote(src, dst, send_sem, recv_sem, axis, peer):
    return pltpu.make_async_remote_copy(
        src_ref=src, dst_ref=dst, send_sem=send_sem, recv_sem=recv_sem,
        device_id={axis: peer}, device_id_type=MESH,
    )


def line(m, direct, sent, mid, came, over, full, sems, over_r, early_r):
    z = lax.axis_index("tp")
    half = m // 2
    left = z < half
    depth = jnp.where(left, z, m - 1 - z)
    toward = jnp.where(left, z + 1, z - 1)
    away = lax.rem(jnp.where(left, z - 1, z + 1) + m, m)
    centre = depth == half - 1
    in_s, over_s, full_s, jump_s, in_r, full_r = sems
    own = sent if half == 1 else mid
    parts = sent.shape[0]
    straight = parts - direct

    def inward(src, p):
        return remote(src.at[p], came.at[p], in_s, in_r.at[p], "tp", toward)

    def across(p):
        return remote(own.at[p], over.at[p], over_s, over_r.at[p], "tp", toward)

    def outward(p):
        return remote(full.at[p], full.at[p], full_s, full_r.at[p], "tp", away)

    def early(p):
        return remote(sent.at[p], came.at[p], in_s, early_r, "tp", away)

    def early_all():
        some = sent.at[pl.ds(0, direct)]
        return remote(some, some, in_s, early_r, "tp", away)

    def jump(p):
        far = 2 * toward - z
        return remote(own.at[p], over.at[p], jump_s, over_r.at[p], "tp", far)

    def start(p):
        if p >= straight:

            @pl.when(centre)
            def _():
                early(p).start()

        if half > 1:

            @pl.when(depth == 0)
            def _():
                inward(sent, p).start()

    def relay(p):
        if half > 1:

            @pl.when(depth > 0)
            def _():
                inward(mid, p).wait_recv()
                mid[p] = (sent[p].astype(F32) + came[p].astype(F32)).astype(BF16)

        @pl.when(centre)
        def _():
            if p >= straight:
                jump(p).start()
            across(p).start()

        if half > 2:

            @pl.when((depth > 0) & jnp.logical_not(centre))
            def _():
                inward(mid, p).start()

    def take(p):
        @pl.when(centre)
        def _():
            across(p).wait_recv()
            full[p] = (own[p].astype(F32) + over[p].astype(F32)).astype(BF16)

        if p >= straight:

            @pl.when(depth == 0)
            def _():
                if p == straight:
                    early_all().wait_recv()
                mid[p] = (sent[p].astype(F32) + came[p].astype(F32)).astype(BF16)
                jump(p).wait_recv()
                full[p] = (mid[p].astype(F32) + over[p].astype(F32)).astype(BF16)

        elif half > 1:

            @pl.when(jnp.logical_not(centre))
            def _():
                outward(p).wait_recv()

            @pl.when(depth > 0)
            def _():
                outward(p).start()

    def end():
        @pl.when(centre)
        def _():
            remote(own, over, over_s, over_r.at[0], "tp", toward).wait_send()
            if direct:
                some = sent.at[pl.ds(0, direct)]
                remote(some, some, in_s, in_r.at[0], "tp", away).wait_send()
                remote(some, some, jump_s, in_r.at[0], "tp", away).wait_send()

        if half > 1:

            @pl.when(jnp.logical_not(centre))
            def _():
                remote(sent, came, in_s, in_r.at[0], "tp", toward).wait_send()

            @pl.when(depth > 0)
            def _():
                some = full.at[pl.ds(0, straight)]
                remote(some, some, full_s, full_r.at[0], "tp", away).wait_send()

    return types.SimpleNamespace(start=start, relay=relay, take=take, end=end)


def main_kernel(
    c, counts, resid, wq, wk, wv, wz, wa, wb, wo, speed, bias, scaling, channel, shrink, states,
    tokens, new, *scratch,
):
    s = types.SimpleNamespace(**dict(zip(c.names, scratch)))
    lines = [
        line(
            c.m, c.direct, s.sent.at[l], s.mid.at[l], s.came.at[l], s.over.at[l], s.full.at[l],
            (s.line_s.at[0], s.line_s.at[1], s.line_s.at[2], s.line_s.at[3], s.in_r, s.full_r),
            s.over_r.at[l], s.early_r.at[l],
        )
        for l in range(BLOCKS)
    ]
    n, m, chips, tile = c.n, c.m, c.chips, c.tile
    me = lax.axis_index("dp")
    z = lax.axis_index("tp")
    core = lax.rem(me, 2)
    chip = lax.div(me, 2)
    partner = me + 1 - 2 * core
    others = [lax.rem(me + 2 * d, n) for d in range(1, chips)]
    across_core = [lax.rem(partner + 2 * d, n) for d in range(1, chips)]
    def load(src, dst, sem):
        copy = pltpu.make_async_copy(src, dst, sem)
        copy.start()
        return copy

    all_heads = wa.shape[1]
    ab = 2 * all_heads
    feats = pl.ds(pl.multiple_of(me * c.feat, 128), c.feat)
    early = [
        load(src, dst, s.small_sem.at[i])
        for i, (src, dst) in enumerate(
            [
                (resid, s.resid), (scaling, s.scaling),
                (wa.at[:, :, feats], s.wab.at[:, pl.ds(0, all_heads)]),
                (wb.at[:, :, feats], s.wab.at[:, pl.ds(all_heads, all_heads)]),
            ]
        )
    ]
    wo_loads, state_loads = {}, {}

    def load_weights(l, j):
        for i, w in enumerate((wq, wk, wv, wz)):
            load(w.at[l, :, pl.ds(j * tile, tile)], s.w.at[l, j, :, pl.ds(i * tile, tile)], s.w_sem.at[j])

    def wait_weights(l, j):
        pltpu.make_async_copy(s.w.at[l, j], s.w.at[l, j], s.w_sem.at[j]).wait()

    def load_rest(l):
        state_loads[l] = load(states.at[l], new.at[l], s.state_sem.at[l])
        wo_loads[l] = load(wo.at[l], s.wo.at[l], s.wo_sem.at[l])

    load_weights(0, 0)
    late = [
        load(src, dst, s.small_sem.at[len(early) + i])
        for i, (src, dst) in enumerate(
            [(speed, s.speed), (bias, s.bias), (channel, s.channel), (shrink, s.shrink)]
        )
    ]
    dp_peers = [lax.rem(me + d, n) for d in range(1, n)]
    swaps = [
        remote(s.counts.at[me], s.counts.at[me], s.count_sem.at[0], s.count_sem.at[1], "dp", peer)
        for peer in dp_peers
    ]
    tp_peers = [lax.rem(z + d, m) for d in ((1, 2, 3) if c.direct else (1, m - 1))]
    barrier = pltpu.get_barrier_semaphore()

    def greet():
        for axis, peers in (("dp", dp_peers), ("tp", tp_peers)):
            for peer in peers:
                pl.semaphore_signal(barrier, inc=1, device_id={axis: peer}, device_id_type=MESH)

    def fill_counts():
        lane = iota((8, c.lanes), 1) - me * c.own_seqs
        mine = jnp.zeros((8, c.lanes), jnp.int32)
        for i in range(c.own_seqs):
            mine = jnp.where(lane == i, s.own_counts[i], mine)
        s.counts[me] = mine

    def swap_counts():
        pl.semaphore_wait(barrier, len(dp_peers) + len(tp_peers))
        for copy in swaps:
            copy.start()

    own_counts = load(counts, s.own_counts, s.small_sem.at[8])
    greet()
    own_counts.wait()
    fill_counts()
    swap_counts()

    def constants():
        row = lax.div(iota((tile, tile), 0), c.size)
        col = lax.div(iota((tile, tile), 1), c.size)
        s.blocks[...] = (row == col).astype(BF16)
        for g in range(c.groups):
            r = lax.rem(iota((2 * c.own, tile), 0), c.own_seqs)
            k = g * c.per_tile + lax.div(iota((2 * c.own, tile), 1), c.size)
            s.mask[g] = (r == k).astype(BF16)

    for j in range(1, c.chunks):
        load_weights(0, j)
    constants()
    load_early = lambda: [copy.wait() for copy in early]
    flat = lambda: s.resid[...].reshape(c.rows, c.feat)

    def raw_small():
        load_early()
        wide = flat().astype(F32)
        bent = (wide * s.scaling[...].astype(F32)[:1]).astype(BF16)
        s.bent[...] = bent
        s.raw_small[0] = narrow(bent, s.wab[0]).astype(BF16)
        squares = jnp.sum(wide * wide, axis=1, keepdims=True)
        s.raw_small[1] = jnp.broadcast_to(squares, (c.rows, ab)).astype(BF16)
        raw_swap(-1).start()

    raws = min(2, c.chunks)

    def raw_swap(j):
        x, pair = (s.raw_small, s.raw_pair_small) if j < 0 else (s.raw.at[j], s.raw_pair.at[j])
        return remote(x.at[1 - core], pair, s.raw_s.at[j + 1], s.first_r.at[j + 1], "dp", partner)

    def raw_first(j):
        wait_weights(0, j)
        val = dot(s.bent[...], s.w[0, j]).astype(BF16)
        s.raw[j, 0] = val[:, : 2 * tile]
        s.raw[j, 1] = val[:, 2 * tile :]
        raw_swap(j).start()

    def wait_counts():
        every = s.counts.at[pl.ds(0, n - 1)]
        swap = remote(every, every, s.count_sem.at[0], s.count_sem.at[1], "dp", partner)
        swap.wait()

    def raw_cross(j):
        x, pair = (s.raw_small, s.raw_pair_small) if j < 0 else (s.raw.at[j], s.raw_pair.at[j])
        raw_swap(j).wait_recv()
        total = (x[core].astype(F32) + pair[...].astype(F32)).astype(BF16)
        bufs(0, j)[2][...] = dot(s.into[...], total).astype(BF16)
        for d in range(chips - 1):
            second(0, j, d).start()

    raw_small()
    for j in range(raws):
        raw_first(j)
    load_rest(0)
    wait_counts()
    total = s.counts[0]
    for d in range(1, n):
        total = total + s.counts[d]
    row_counts = total.astype(F32)
    row_bf16 = row_counts.astype(BF16)

    def columns(count, seq, slot):
        lanes = iota((count, c.lanes), 1)
        all_counts = jnp.broadcast_to(row_counts[:1], (count, c.lanes))
        start = jnp.sum(jnp.where(lanes < seq, all_counts, 0.0), axis=1, keepdims=True)
        size = jnp.sum(jnp.where(lanes == seq, all_counts, 0.0), axis=1, keepdims=True)
        slot = slot[:, :1].astype(F32)
        return start + slot, slot < size

    def rows_of(seq, slot):
        index = iota(seq.shape, 0)
        start = dot(row_bf16, (index < seq).astype(BF16))[:1]
        size = dot(row_bf16, (index == seq).astype(BF16))[:1]
        slot = slot[:1].astype(F32)
        return start + slot, slot < size

    def pack():
        shape = (c.lanes, c.rows)
        pos, live = rows_of(lax.div(iota(shape, 1), c.slots), lax.rem(iota(shape, 1), c.slots))
        s.into[...] = jnp.where((iota((c.packed, c.rows), 0).astype(F32) == pos) & live, 1.0, 0.0).astype(BF16)

    pack()

    def produce(l, j):
        at = slice((c.pairs - 1) * 2 * c.part, c.feat)
        if l:
            val = s.acc[j] + dot(s.scaled[:, at], s.w[l, j, at])
        else:
            wait_weights(l, j)
            val = dot(s.scaled[...], s.w[l, j])
        val = val.astype(BF16)
        s.x[l, j, 0] = val[:, : 2 * tile]
        s.x[l, j, 1] = val[:, 2 * tile :]
        first(l, j).start()

    def pack_rest():
        h = dot(s.into[...], flat())
        s.h[...] = h
        s.scaled[...] = (h * s.scaling[...].astype(F32)[:1]).astype(BF16)

    def produce_small(l):
        at = slice((c.pairs - 1) * 2 * c.part, c.feat)
        h = s.h[...]
        s.x_small[l, 0] = (s.acc_small[...] + narrow(s.scaled[:, at], s.wab[l, :, at])).astype(BF16)
        squares = jnp.sum(h * h, axis=1, keepdims=True)
        s.x_small[l, 1] = jnp.broadcast_to(squares, (c.packed, ab)).astype(BF16)
        first(l, -1).start()

    def bufs(l, j):
        if j < 0:
            return s.x_small.at[l], s.pair_small.at[l], s.sum_small.at[l], s.far_small.at[l], s.out_small.at[l], s.fin_small.at[l]
        return s.x.at[l, j], s.pair.at[l, j], s.sum.at[l, j], s.far.at[l, j], s.out.at[l, j], s.fin.at[l, j]

    def kind(j):
        return min(j + 1, 1)

    def first(l, j):
        x, pair, *_ = bufs(l, j)
        return remote(x.at[1 - core], pair, s.first_s.at[kind(j)], s.first_r.at[j + 1], "dp", partner)

    def second(l, j, d):
        _, _, own, far, *_ = bufs(l, j)
        there = pl.multiple_of(lax.div(others[d], 2) * c.per_chip, 16)
        return remote(
            own.at[pl.ds(there, c.chip_win)], far.at[d], s.second_s.at[kind(j), d], s.second_r.at[j + 1, d],
            "dp", others[d],
        )

    def third(l, j):
        *_, out, fin = bufs(l, j)
        return remote(out, fin.at[core], s.third_s.at[kind(j)], s.third_r.at[j + 1], "dp", partner)

    def cross(l, j):
        x, pair, own, *_ = bufs(l, j)
        first(l, j).wait_recv()
        own[...] = (x[core].astype(F32) + pair[...].astype(F32)).astype(BF16)
        for d in range(chips - 1):
            second(l, j, d).start()

    def finish(l, j):
        x, pair, own, far, out, fin = bufs(l, j)
        for d in range(chips - 1):
            second(l, j, d).wait_recv()

        def reduced(which):
            at = pl.multiple_of(which * c.own_seqs, 16)
            val = own[pl.ds(pl.multiple_of(chip * c.per_chip + at, 16), c.win), :].astype(F32)
            for d in range(chips - 1):
                val = val + far[d, pl.ds(at, c.win), :].astype(F32)
            return val.astype(BF16)

        out[...] = reduced(1 - core)
        third(l, j).start()
        fin[core] = reduced(core)

    def prepare(l):
        third(l, -1).wait_recv()
        pick = s.pick[...]
        heads = c.heads
        few = dot(pick, s.fin_small[l, 0]).astype(BF16)
        squares = dot(pick, s.fin_small[l, 1])[:, :1]
        factor = lax.rsqrt(squares / (c.feat * n) + EPS)
        s.factor[...] = jnp.broadcast_to(factor, s.factor.shape)
        at = iota((ab, heads), 1) + z * heads
        pa = dot(few, (iota((ab, heads), 0) == at).astype(BF16)) * factor
        pb = dot(few, (iota((ab, heads), 0) == at + all_heads).astype(BF16)) * factor
        arg = pa + s.bias[...][l : l + 1]
        soft = jnp.maximum(arg, 0.0) + jnp.log1p(jnp.exp(-jnp.abs(arg)))
        extra = jnp.concatenate([s.shrink[l, :, t, :] for t in range(c.slots)], axis=0)
        dec = jnp.exp(extra - jnp.exp(s.speed[...][l : l + 1]) * soft)
        dec = jnp.where(s.live[:, :1] > 0.0, dec, 1.0)
        wide = (iota((heads, c.cols), 0) == lax.div(iota((heads, c.cols), 1), c.size)).astype(BF16)
        both = jnp.concatenate([dec, jax.nn.sigmoid(pb)], axis=0)
        high = both.astype(BF16)
        low = (both - high.astype(F32)).astype(BF16)
        spread = dot(jnp.concatenate([high, low], axis=0), wide)
        s.dec[...] = spread[: c.own] + spread[2 * c.own : 3 * c.own]
        s.beta[...] = spread[c.own : 2 * c.own] + spread[3 * c.own :]

    def recur(l, j):
        at = slice(j * tile, (j + 1) * tile)
        third(l, j).wait_recv()
        pick = s.pick[...]
        factor = s.factor[:, :1]
        qk = dot(pick, s.fin[l, j, 0]) * factor
        vz = dot(pick, s.fin[l, j, 1]) * factor
        qk = qk * jax.nn.sigmoid(qk)
        vz = vz * jax.nn.sigmoid(vz)
        q, k = qk[:, :tile], qk[:, tile:]
        v, zed = vz[:, :tile], vz[:, tile:]
        both = jnp.concatenate([k, q], axis=0)
        low = iota((2 * c.own, 128), 1) < c.size
        copies = []
        for i in range(tile // 128):
            here = both[:, i * 128 : (i + 1) * 128]
            turned = pltpu.roll(here, c.size, 1)
            copies += [jnp.where(low, here, turned), jnp.where(low, turned, here)]
        lhs = []
        for one in copies:
            wide = jnp.concatenate([one.astype(BF16)] * (tile // 128), axis=1)
            lhs.append(jnp.concatenate([wide * s.mask[g] for g in range(c.groups)], axis=1))
        read = dot(jnp.concatenate(lhs, axis=0), s.states16[l, :, at])
        step = lambda x, t: x[t * c.own_seqs : (t + 1) * c.own_seqs]
        names, prods = [], []
        for t in range(c.slots):
            names.append(("n", t, t))
            prods.append(step(q, t) * step(q, t))
            for i in range(t + 1):
                names.append(("q", i, t))
                prods.append(step(k, i) * step(q, t))
                names.append(("k", i, t))
                prods.append(step(k, i) * step(k, t))
        pairs = dot(jnp.concatenate(prods, axis=0).astype(BF16), s.blocks[...])
        pairs = {name: step(pairs, i) for i, name in enumerate(names)}
        nk = [lax.rsqrt(pairs["k", t, t] + EPS) for t in range(c.slots)]
        nq = [lax.rsqrt(pairs["n", t, t] + EPS) * c.size ** (-0.5) for t in range(c.slots)]
        s.k[l, :, at] = (k * jnp.concatenate(nk, axis=0)).astype(BF16)
        lane_head = lax.div(iota((2 * c.own, tile), 1), c.size)
        reads = read[: 2 * c.own]
        for h in range(1, c.per_tile):
            reads = jnp.where(lane_head == h, read[2 * c.own * h : 2 * c.own * (h + 1)], reads)
        rk = reads[: c.own]
        rq = reads[c.own :]
        dec = s.dec[:, at]
        beta = s.beta[:, at]
        fresh, outs = [], []
        whole = None
        for t in range(c.slots):
            g = step(dec, t)
            whole = g if whole is None else whole * g
            fresh = [(u * g) for u in fresh]
            guess = whole * step(rk, t)
            for i in range(t):
                guess = guess + pairs["k", i, t] * nk[i] * fresh[i]
            fresh.append(step(beta, t) * (step(v, t) - guess * nk[t]))
            o = whole * step(rq, t)
            for i in range(t + 1):
                o = o + pairs["q", i, t] * nk[i] * fresh[i]
            outs.append(o * nq[t])
        s.u[l, :, at] = jnp.concatenate(fresh, axis=0).astype(BF16)
        s.decay[l, :, at] = whole
        o = jnp.concatenate(outs, axis=0)
        total = dot((o * o).astype(BF16), s.blocks[...])
        o = o * lax.rsqrt(total / c.size + EPS) * s.gain[l, :1] * zed
        s.y[l, me, j] = dot(s.place[...], o.astype(BF16)).astype(BF16)
        for peer in others + across_core + [partner]:
            here = s.y.at[l, me, j]
            remote(here, here, s.y_s.at[0], s.y_r.at[int(j + 1 == c.chunks)], "dp", peer).start()

    def wait_y(l, last):
        chunks = c.chunks - 1 if last else pl.ds(0, c.chunks - 1)
        every = s.y.at[l, pl.ds(0, n - 1), chunks]
        remote(every, every, s.y_s.at[0], s.y_r.at[int(last)], "dp", partner).wait_recv()

    def sent_all(l):
        if l:
            first(l, -1).wait_send()
        else:
            for j in range(-1, raws):
                raw_swap(j).wait_send()
        if l or c.chunks > raws:
            done = s.pair.at[l] if l else s.pair.at[l, pl.ds(raws, c.chunks - raws)]
            remote(done, done, s.first_s.at[1], s.first_r.at[0], "dp", partner).wait_send()
        for d in range(chips - 1):
            second(l, -1, d).wait_send()
            done = s.far.at[l, :, d]
            remote(done, done, s.second_s.at[1, d], s.second_r.at[0, d], "dp", others[d]).wait_send()
        third(l, -1).wait_send()
        done = s.out.at[l]
        remote(done, done, s.third_s.at[1], s.third_r.at[0], "dp", partner).wait_send()
        done = s.y.at[l, pl.ds(0, n - 1)]
        remote(done, done, s.y_s.at[0], s.y_r.at[0], "dp", partner).wait_send()

    def gather(l, j):
        at = slice(j * tile, (j + 1) * tile)
        s.gated[:, at] = jnp.zeros((c.packed, tile), BF16)
        for d in range(n):
            here = slice(d * c.own_seqs, d * c.own_seqs + c.win)
            s.gated[here, at] = s.gated[here, at] + s.y[l, d, j]

    def mix_some(l):
        before = slice(0, (c.chunks - 1) * tile)
        s.mixed[...] = dot(s.gated[:, before], s.wo[l, before])

    def mix_mul(l, run):
        per = c.parts // 2
        at = slice(run * per * c.part, (run + 1) * per * c.part)
        after = slice((c.chunks - 1) * tile, c.cols)
        val = dot(s.gated[:, after], s.wo[l, after, at])
        if c.chunks > 1:
            val = val + s.mixed[:, at]
        val = val.astype(BF16)
        for i in range(per):
            s.sent[l, run * per + i] = val[:, i * c.part : (i + 1) * c.part]
        for i in range(per):
            lines[l].start(run * per + i)

    lead = 5
    early_takes = c.parts - lead if c.direct else 0
    early_takes = min(early_takes, c.parts - c.direct)

    def mix_out(l, p):
        lines[l].relay(p)
        if 0 <= p - lead < early_takes:
            lines[l].take(p - lead)

    def mix_in(l, p):
        if not p < early_takes:
            lines[l].take(p)
        at = slice(p * c.part, (p + 1) * c.part)
        mixed = (s.h[:, at] + s.full[l, p].astype(F32)).astype(BF16)
        s.scaled[:, at] = mixed
        if l + 1 < BLOCKS:
            mixed = mixed.astype(F32)
            s.h[:, at] = mixed
            s.scaled[:, at] = (mixed * s.scaling[...].astype(F32)[l + 1 : l + 2, at]).astype(BF16)

    def place_tokens(p):
        at = slice((p - 1) * c.part, (p + 1) * c.part)
        back = dot(s.hot[...], s.scaled[:, at])
        kept = s.resid[:, :, at].reshape(c.rows, 2 * c.part).astype(F32)
        mixed = jnp.where(s.alive[:, :1] > 0.0, back, kept).astype(BF16)
        tokens[:, :, at] = mixed.reshape(c.seqs, c.slots, 2 * c.part)

    def setup():
        r = iota((c.own, c.lanes), 0)
        pos, live = columns(c.own, lax.rem(r, c.own_seqs) + me * c.own_seqs, lax.div(r, c.own_seqs))
        offset = (iota((c.own, c.win), 1) + me * c.own_seqs).astype(F32)
        s.pick[...] = jnp.where((offset == pos) & live, 1.0, 0.0).astype(BF16)
        s.live[...] = jnp.broadcast_to(jnp.where(live, 1.0, 0.0), s.live.shape)
        shape = (c.lanes, c.own)
        pos, live = rows_of(
            lax.rem(iota(shape, 1), c.own_seqs) + me * c.own_seqs, lax.div(iota(shape, 1), c.own_seqs)
        )
        offset = (iota((c.win, c.own), 0) + me * c.own_seqs).astype(F32)
        s.place[...] = jnp.where((offset == pos) & live, 1.0, 0.0).astype(BF16)
        r = iota((c.rows, c.lanes), 0)
        pos, live = columns(c.rows, lax.div(r, c.slots), lax.rem(r, c.slots))
        offset = iota((c.rows, c.packed), 1).astype(F32)
        s.alive[...] = jnp.broadcast_to(jnp.where(live, 1.0, 0.0), s.alive.shape)
        s.hot[...] = jnp.where((offset == pos) & live, 1.0, 0.0).astype(BF16)
        fold = (iota((c.size, tile), 0) == lax.rem(iota((c.size, tile), 1), c.size)).astype(BF16)
        for l in range(BLOCKS):
            channels = jnp.broadcast_to(s.channel[...].astype(F32)[l : l + 1], (8, c.size)).astype(BF16)
            s.gain[l] = dot(channels, fold)

    def write_states(l, j):
        at = slice(j * tile, (j + 1) * tile)
        shape = (c.per_tile * c.own, tile)
        same = (lax.div(iota(shape, 0), c.own) == lax.div(iota(shape, 1), c.size)).astype(BF16)
        fold = (iota((c.size, tile), 0) == lax.rem(iota((c.size, tile), 1), c.size)).astype(BF16)
        keys = lax.dot_general(
            fold, tiles(s.k[l, :, at], c.per_tile) * same, (((1,), (1,)), ((), ())), preferred_element_type=F32
        ).astype(BF16)
        fresh = tiles(s.u[l, :, at], c.per_tile) * same
        owner = lax.rem(iota((c.size, c.per_tile * c.own), 1), c.own_seqs)
        batch = 4
        for first_seq in range(0, c.own_seqs, batch):
            lhs = jnp.concatenate(
                [keys * (owner == first_seq + i).astype(BF16) for i in range(batch)], axis=0
            )
            added = dot(lhs, fresh)
            for i in range(batch):
                seq = first_seq + i
                new[l, seq, :, at] = (
                    new[l, seq, :, at] * s.decay[l, seq : seq + 1, at] + added[i * c.size : (i + 1) * c.size]
                )

    def round_states(l):
        state_loads[l].wait()
        for i in range(c.own_seqs):
            s.states16[l, i * c.size : (i + 1) * c.size] = new[l, i].astype(BF16)

    for l in range(BLOCKS):
        if l:
            for j in range(c.chunks):
                wait_weights(l, j)
            for p in range(c.parts):
                mix_in(l - 1, p)
                if p % 2 and p + 1 < c.parts:
                    at = slice((p - 1) * c.part, (p + 1) * c.part)
                    piece = s.scaled[:, at]
                    for j in range(c.chunks):
                        val = dot(piece, s.w[l, j, at])
                        s.acc[j] = val if p == 1 else s.acc[j] + val
                    val = narrow(piece, s.wab[l, :, at])
                    s.acc_small[...] = val if p == 1 else s.acc_small[...] + val
        if l:
            produce_small(l)
            for j in range(c.chunks):
                produce(l, j)
                if j:
                    cross(l, j - 2)
            for j in range(c.chunks - 2, c.chunks):
                cross(l, j)
        else:
            for j in range(-1, raws):
                raw_cross(j)
            pack_rest()
            for j in range(raws, c.chunks):
                produce(l, j)
            for copy in late:
                copy.wait()
            setup()
            round_states(0)
            for j in range(raws, c.chunks):
                if j + 1 == c.chunks:
                    finish(l, -1)
                cross(l, j)
            if c.chunks == raws:
                finish(l, -1)
        if l == 0:
            for j in range(c.chunks):
                load_weights(1, j)
            load_rest(1)
        else:
            finish(l, -1)
        finish(l, 0)
        prepare(l)
        for j in range(1, c.chunks):
            finish(l, j)
            recur(l, j - 1)
        recur(l, c.chunks - 1)
        for j in range(c.chunks - 1):
            write_states(l, j)
        wo_loads[l].wait()
        if c.chunks > 1:
            wait_y(l, False)
            for j in range(c.chunks - 1):
                gather(l, j)
            mix_some(l)
        wait_y(l, True)
        gather(l, c.chunks - 1)
        mix_mul(l, 0)
        mix_mul(l, 1)
        write_states(l, c.chunks - 1)
        if l == 0:
            round_states(1)
        if l:
            lines[l - 1].end()
        for p in range(c.parts):
            mix_out(l, p)
        sent_all(l)
    for p in range(c.parts):
        mix_in(BLOCKS - 1, p)
        if p % 2:
            place_tokens(p)
    lines[BLOCKS - 1].end()


def run_main(c, args):
    ab = 2 * args[6].shape[1]
    half = 2 * c.tile
    chips, n = c.chips, c.n
    dma = lambda *shape: pltpu.SemaphoreType.DMA(shape)
    buf = lambda *shape: pltpu.VMEM(shape, BF16)
    wide = lambda *shape: pltpu.VMEM(shape, F32)
    every = 1 + c.chunks
    scratch = dict(
        resid=buf(c.seqs, c.slots, c.feat),
        k=buf(BLOCKS, c.own, c.cols),
        u=buf(BLOCKS, c.own, c.cols),
        decay=wide(BLOCKS, c.own_seqs, c.cols),
        scaling=buf(BLOCKS, c.feat),
        wab=buf(BLOCKS, ab, c.feat),
        speed=wide(BLOCKS, c.heads),
        bias=wide(BLOCKS, c.heads),
        channel=buf(BLOCKS, c.size),
        shrink=wide(BLOCKS, c.own_seqs, c.slots, c.heads),
        w=buf(BLOCKS, c.chunks, c.feat, 4 * c.tile),
        raw=buf(min(2, c.chunks), 2, c.rows, half),
        raw_small=buf(2, c.rows, ab),
        raw_pair=buf(min(2, c.chunks), c.rows, half),
        raw_pair_small=buf(c.rows, ab),
        hot=buf(c.rows, c.packed),
        alive=wide(c.rows, 128),
        **{name: buf(BLOCKS, c.parts, c.packed, c.part) for name in ("sent", "mid", "came", "over", "full")},
        bent=buf(c.rows, c.feat),
        into=buf(c.packed, c.rows),
        wo=buf(BLOCKS, c.cols, c.feat),
        states16=buf(BLOCKS, c.own_seqs * c.size, c.cols),
        counts=pltpu.VMEM((n, 8, c.lanes), jnp.int32),
        blocks=buf(c.tile, c.tile),
        mask=buf(c.groups, 2 * c.own, c.tile),
        gain=wide(BLOCKS, 8, c.tile),
        pick=buf(c.own, c.win),
        place=buf(c.win, c.own),
        live=wide(c.own, 128),
        factor=wide(c.own, 128),
        dec=wide(c.own, c.cols),
        beta=wide(c.own, c.cols),
        h=wide(c.packed, c.feat),
        scaled=buf(c.packed, c.feat),
        acc=wide(c.chunks, c.packed, 4 * c.tile),
        acc_small=wide(c.packed, ab),
        x=buf(BLOCKS, c.chunks, 2, c.packed, half),
        pair=buf(BLOCKS, c.chunks, c.packed, half),
        sum=buf(BLOCKS, c.chunks, c.packed, half),
        far=buf(BLOCKS, c.chunks, chips - 1, c.chip_win, half),
        out=buf(BLOCKS, c.chunks, c.win, half),
        fin=buf(BLOCKS, c.chunks, 2, c.win, half),
        x_small=buf(BLOCKS, 2, c.packed, ab),
        pair_small=buf(BLOCKS, c.packed, ab),
        sum_small=buf(BLOCKS, c.packed, ab),
        far_small=buf(BLOCKS, chips - 1, c.chip_win, ab),
        out_small=buf(BLOCKS, c.win, ab),
        fin_small=buf(BLOCKS, 2, c.win, ab),
        y=buf(BLOCKS, n, c.chunks, c.win, c.tile),
        gated=buf(c.packed, c.cols),
        mixed=wide(c.packed, c.feat),
        own_counts=pltpu.SMEM((c.own_seqs,), jnp.int32),
        small_sem=dma(9),
        w_sem=dma(c.chunks),
        wo_sem=dma(BLOCKS),
        state_sem=dma(BLOCKS),
        count_sem=dma(2),
        raw_s=dma(1 + min(2, c.chunks)),
        first_s=dma(2),
        first_r=dma(every),
        second_s=dma(2, chips - 1),
        second_r=dma(every, chips - 1),
        third_s=dma(2),
        third_r=dma(every),
        y_s=dma(1),
        y_r=dma(2),
        line_s=dma(4),
        early_r=dma(BLOCKS),
        in_r=dma(c.parts),
        full_r=dma(c.parts - c.direct),
        over_r=dma(BLOCKS, c.parts),
    )
    c.names = list(scratch)
    return pl.pallas_call(
        functools.partial(main_kernel, c),
        out_shape=[
            pltpu.VMEM(args[1].shape, BF16),
            pltpu.VMEM(args[-1].shape, F32),
        ],
        in_specs=[HBM] * 15,
        out_specs=[VMEM] * 2,
        scratch_shapes=list(scratch.values()),
        compiler_params=pltpu.CompilerParams(
            collective_id=1, has_side_effects=True, vmem_limit_bytes=46 * 1024 * 1024
        ),
        name="blocks",
    )(*[pltpu.with_memory_space_constraint(x, pltpu.HBM) for x in args])


def store_kernel(pieces, tokens, new, tokens_out, new_out, sem):
    copies = [pltpu.make_async_copy(tokens, tokens_out, sem.at[pieces])]
    size = new.shape[1] * new.shape[0] // pieces
    for i in range(pieces):
        l, at = divmod(i * size, new.shape[1])
        at = pl.ds(at, size)
        copies.append(pltpu.make_async_copy(new.at[l, at], new_out.at[l, at], sem.at[i]))
    for copy in copies:
        copy.start()
    for copy in copies:
        copy.wait()


def store(tokens, new):
    pieces = 8
    return pl.pallas_call(
        functools.partial(store_kernel, pieces),
        out_shape=[jax.ShapeDtypeStruct(a.shape, a.dtype) for a in (tokens, new)],
        in_specs=[VMEM] * 2,
        out_specs=[HBM] * 2,
        scratch_shapes=[pltpu.SemaphoreType.DMA((pieces + 1,))],
        compiler_params=pltpu.CompilerParams(vmem_limit_bytes=1024 * 1024),
        name="store",
    )(tokens, new)


def body(
    n, m, resid, counts, wq, wk, wv, wz, wa, wb, wo, speed, bias, scaling, channel, shrink, states,
):
    c = sizes(n, m, resid, counts, wq, speed)
    turned = [jnp.swapaxes(w, 1, 2) for w in (wa, wb)]
    tokens, new = run_main(
        c, (counts, resid, wq, wk, wv, wz, *turned, wo, speed, bias, scaling, channel, shrink, states)
    )
    return store(tokens, new)


def solution(mesh):
    in_specs = (
        P("grp", None, "dp"),
        P(("grp", "dp")),
        P(None, "dp", "tp"),
        P(None, "dp", "tp"),
        P(None, "dp", "tp"),
        P(None, "dp", "tp"),
        P(),
        P(),
        P(None, "tp", "dp"),
        P(None, "tp"),
        P(None, "tp"),
        P(None, "dp"),
        P(),
        P(None, ("grp", "dp"), None, "tp"),
        P(None, ("grp", "dp"), None, "tp"),
    )
    out_specs = (P("grp", None, "dp"), P(None, ("grp", "dp"), None, "tp"))
    run = functools.partial(body, mesh.shape["dp"], mesh.shape["tp"])
    return jax.shard_map(run, mesh=mesh, in_specs=in_specs, out_specs=out_specs, check_vma=False)
```

```python
import functools
import types

import jax
import jax.numpy as jnp
from jax import lax
from jax.experimental import pallas as pl
from jax.experimental.pallas import tpu as pltpu
from jax.sharding import PartitionSpec as P

BLOCKS = 2
EPS = 1e-06
F32 = jnp.float32
BF16 = jnp.bfloat16
MESH = pl.DeviceIdType.MESH
VMEM = pl.BlockSpec(memory_space=pltpu.VMEM)
HBM = pl.BlockSpec(memory_space=pltpu.HBM)


def iota(shape, dim):
    return lax.broadcasted_iota(jnp.int32, shape, dim)


def dot(a, b):
    return jnp.dot(a, b, preferred_element_type=F32)


def narrow(a, b):
    return lax.dot_general(a, b, (((1,), (1,)), ((), ())), preferred_element_type=F32)


def tiles(ref, count):
    return jnp.concatenate([ref] * count, axis=0)


def sizes(n, m, resid, counts, wq, speed):
    c = types.SimpleNamespace(n=n, m=m)
    c.seqs, c.slots, c.feat = resid.shape
    c.own_seqs = counts.shape[0]
    c.cols = wq.shape[2]
    c.heads = speed.shape[1]
    c.size = c.cols // c.heads
    c.own = c.own_seqs * c.slots
    c.rows = c.seqs * c.slots
    c.packed = c.seqs * 3 // 2
    c.chips = n // 2
    c.per_chip = 2 * c.own_seqs
    c.chip_win = c.packed - (c.chips - 1) * c.per_chip
    c.win = c.packed - (n - 1) * c.own_seqs
    c.tile = min(256, c.cols)
    c.chunks = c.cols // c.tile
    c.per_tile = c.tile // c.size
    c.groups = c.own_seqs // c.per_tile
    c.parts = 8
    c.pairs = c.parts // 2
    c.direct = 3 if m == 4 else 0
    c.part = c.feat // c.parts
    c.lanes = -(-c.seqs // 128) * 128
    return c


def remote(src, dst, send_sem, recv_sem, axis, peer):
    return pltpu.make_async_remote_copy(
        src_ref=src, dst_ref=dst, send_sem=send_sem, recv_sem=recv_sem,
        device_id={axis: peer}, device_id_type=MESH,
    )


def line(m, direct, sent, mid, came, over, full, sems, over_r, early_r):
    z = lax.axis_index("tp")
    half = m // 2
    left = z < half
    depth = jnp.where(left, z, m - 1 - z)
    toward = jnp.where(left, z + 1, z - 1)
    away = lax.rem(jnp.where(left, z - 1, z + 1) + m, m)
    centre = depth == half - 1
    in_s, over_s, full_s, jump_s, in_r, full_r = sems
    own = sent if half == 1 else mid
    parts = sent.shape[0]
    straight = parts - direct

    def inward(src, p):
        return remote(src.at[p], came.at[p], in_s, in_r.at[p], "tp", toward)

    def across(p):
        return remote(own.at[p], over.at[p], over_s, over_r.at[p], "tp", toward)

    def outward(p):
        return remote(full.at[p], full.at[p], full_s, full_r.at[p], "tp", away)

    def early(p):
        return remote(sent.at[p], came.at[p], in_s, early_r, "tp", away)

    def early_all():
        some = sent.at[pl.ds(0, direct)]
        return remote(some, some, in_s, early_r, "tp", away)

    def jump(p):
        far = 2 * toward - z
        return remote(own.at[p], over.at[p], jump_s, over_r.at[p], "tp", far)

    def start(p):
        if p >= straight:

            @pl.when(centre)
            def _():
                early(p).start()

        if half > 1:

            @pl.when(depth == 0)
            def _():
                inward(sent, p).start()

    def relay(p):
        if half > 1:

            @pl.when(depth > 0)
            def _():
                inward(mid, p).wait_recv()
                mid[p] = (sent[p].astype(F32) + came[p].astype(F32)).astype(BF16)

        @pl.when(centre)
        def _():
            if p >= straight:
                jump(p).start()
            across(p).start()

        if half > 2:

            @pl.when((depth > 0) & jnp.logical_not(centre))
            def _():
                inward(mid, p).start()

    def take(p):
        @pl.when(centre)
        def _():
            across(p).wait_recv()
            full[p] = (own[p].astype(F32) + over[p].astype(F32)).astype(BF16)

        if p >= straight:

            @pl.when(depth == 0)
            def _():
                if p == straight:
                    early_all().wait_recv()
                mid[p] = (sent[p].astype(F32) + came[p].astype(F32)).astype(BF16)
                jump(p).wait_recv()
                full[p] = (mid[p].astype(F32) + over[p].astype(F32)).astype(BF16)

        elif half > 1:

            @pl.when(jnp.logical_not(centre))
            def _():
                outward(p).wait_recv()

            @pl.when(depth > 0)
            def _():
                outward(p).start()

    def end():
        @pl.when(centre)
        def _():
            remote(own, over, over_s, over_r.at[0], "tp", toward).wait_send()
            if direct:
                some = sent.at[pl.ds(0, direct)]
                remote(some, some, in_s, in_r.at[0], "tp", away).wait_send()
                remote(some, some, jump_s, in_r.at[0], "tp", away).wait_send()

        if half > 1:

            @pl.when(jnp.logical_not(centre))
            def _():
                remote(sent, came, in_s, in_r.at[0], "tp", toward).wait_send()

            @pl.when(depth > 0)
            def _():
                some = full.at[pl.ds(0, straight)]
                remote(some, some, full_s, full_r.at[0], "tp", away).wait_send()

    return types.SimpleNamespace(start=start, relay=relay, take=take, end=end)


def main_kernel(
    c, counts, resid, wq, wk, wv, wz, wa, wb, wo, speed, bias, scaling, channel, shrink, states,
    tokens, new, *scratch,
):
    s = types.SimpleNamespace(**dict(zip(c.names, scratch)))
    lines = [
        line(
            c.m, c.direct, s.sent.at[l], s.mid.at[l], s.came.at[l], s.over.at[l], s.full.at[l],
            (s.line_s.at[0], s.line_s.at[1], s.line_s.at[2], s.line_s.at[3], s.in_r, s.full_r),
            s.over_r.at[l], s.early_r.at[l],
        )
        for l in range(BLOCKS)
    ]
    n, m, chips, tile = c.n, c.m, c.chips, c.tile
    me = lax.axis_index("dp")
    z = lax.axis_index("tp")
    core = lax.rem(me, 2)
    chip = lax.div(me, 2)
    partner = me + 1 - 2 * core
    others = [lax.rem(me + 2 * d, n) for d in range(1, chips)]
    across_core = [lax.rem(partner + 2 * d, n) for d in range(1, chips)]
    def load(src, dst, sem):
        copy = pltpu.make_async_copy(src, dst, sem)
        copy.start()
        return copy

    all_heads = wa.shape[1]
    ab = 2 * all_heads
    feats = pl.ds(pl.multiple_of(me * c.feat, 128), c.feat)
    early = [
        load(src, dst, s.small_sem.at[i])
        for i, (src, dst) in enumerate(
            [
                (resid, s.resid), (scaling, s.scaling),
                (wa.at[:, :, feats], s.wab.at[:, pl.ds(0, all_heads)]),
                (wb.at[:, :, feats], s.wab.at[:, pl.ds(all_heads, all_heads)]),
            ]
        )
    ]
    wo_loads, state_loads = {}, {}

    def load_weights(l, j):
        for i, w in enumerate((wq, wk, wv, wz)):
            load(w.at[l, :, pl.ds(j * tile, tile)], s.w.at[l, j, :, pl.ds(i * tile, tile)], s.w_sem.at[j])

    def wait_weights(l, j):
        pltpu.make_async_copy(s.w.at[l, j], s.w.at[l, j], s.w_sem.at[j]).wait()

    def load_rest(l):
        state_loads[l] = load(states.at[l], new.at[l], s.state_sem.at[l])
        wo_loads[l] = load(wo.at[l], s.wo.at[l], s.wo_sem.at[l])

    load_weights(0, 0)
    late = [
        load(src, dst, s.small_sem.at[len(early) + i])
        for i, (src, dst) in enumerate(
            [(speed, s.speed), (bias, s.bias), (channel, s.channel), (shrink, s.shrink)]
        )
    ]
    dp_peers = [lax.rem(me + d, n) for d in range(1, n)]
    swaps = [
        remote(s.counts.at[me], s.counts.at[me], s.count_sem.at[0], s.count_sem.at[1], "dp", peer)
        for peer in dp_peers
    ]
    tp_peers = [lax.rem(z + d, m) for d in ((1, 2, 3) if c.direct else (1, m - 1))]
    barrier = pltpu.get_barrier_semaphore()

    def greet():
        for axis, peers in (("dp", dp_peers), ("tp", tp_peers)):
            for peer in peers:
                pl.semaphore_signal(barrier, inc=1, device_id={axis: peer}, device_id_type=MESH)

    def fill_counts():
        lane = iota((8, c.lanes), 1) - me * c.own_seqs
        mine = jnp.zeros((8, c.lanes), jnp.int32)
        for i in range(c.own_seqs):
            mine = jnp.where(lane == i, s.own_counts[i], mine)
        s.counts[me] = mine

    def swap_counts():
        pl.semaphore_wait(barrier, len(dp_peers) + len(tp_peers))
        for copy in swaps:
            copy.start()

    own_counts = load(counts, s.own_counts, s.small_sem.at[8])
    greet()
    own_counts.wait()
    fill_counts()
    swap_counts()

    def constants():
        row = lax.div(iota((tile, tile), 0), c.size)
        col = lax.div(iota((tile, tile), 1), c.size)
        s.blocks[...] = (row == col).astype(BF16)
        shape = s.mask.shape
        s.mask[...] = (lax.rem(iota(shape, 0), c.per_tile) == lax.div(iota(shape, 1), c.size)).astype(BF16)

    for j in range(1, c.chunks):
        load_weights(0, j)
    constants()
    load_early = lambda: [copy.wait() for copy in early]
    flat = lambda: s.resid[...].reshape(c.rows, c.feat)

    def raw_small():
        load_early()
        wide = flat().astype(F32)
        bent = (wide * s.scaling[...].astype(F32)[:1]).astype(BF16)
        s.bent[...] = bent
        s.raw_small[0] = narrow(bent, s.wab[0]).astype(BF16)
        squares = jnp.sum(wide * wide, axis=1, keepdims=True)
        s.raw_small[1] = jnp.broadcast_to(squares, (c.rows, ab)).astype(BF16)
        raw_swap(-1).start()

    raws = min(2, c.chunks)

    def raw_swap(j):
        x, pair = (s.raw_small, s.raw_pair_small) if j < 0 else (s.raw.at[j], s.raw_pair.at[j])
        return remote(x.at[1 - core], pair, s.raw_s.at[j + 1], s.first_r.at[j + 1], "dp", partner)

    def raw_first(j):
        wait_weights(0, j)
        val = dot(s.bent[...], s.w[0, j]).astype(BF16)
        s.raw[j, 0] = val[:, : 2 * tile]
        s.raw[j, 1] = val[:, 2 * tile :]
        raw_swap(j).start()

    def wait_counts():
        every = s.counts.at[pl.ds(0, n - 1)]
        swap = remote(every, every, s.count_sem.at[0], s.count_sem.at[1], "dp", partner)
        swap.wait()

    def raw_cross(j):
        x, pair = (s.raw_small, s.raw_pair_small) if j < 0 else (s.raw.at[j], s.raw_pair.at[j])
        raw_swap(j).wait_recv()
        total = (x[core].astype(F32) + pair[...].astype(F32)).astype(BF16)
        bufs(0, j)[2][...] = dot(s.into[...], total).astype(BF16)
        for d in range(chips - 1):
            second(0, j, d).start()

    raw_small()
    for j in range(raws):
        raw_first(j)
    load_rest(0)
    wait_counts()
    total = s.counts[0]
    for d in range(1, n):
        total = total + s.counts[d]
    row_counts = total.astype(F32)
    row_bf16 = row_counts.astype(BF16)

    def columns(count, seq, slot):
        lanes = iota((count, c.lanes), 1)
        all_counts = jnp.broadcast_to(row_counts[:1], (count, c.lanes))
        start = jnp.sum(jnp.where(lanes < seq, all_counts, 0.0), axis=1, keepdims=True)
        size = jnp.sum(jnp.where(lanes == seq, all_counts, 0.0), axis=1, keepdims=True)
        slot = slot[:, :1].astype(F32)
        return start + slot, slot < size

    def rows_of(seq, slot):
        index = iota(seq.shape, 0)
        start = dot(row_bf16, (index < seq).astype(BF16))[:1]
        size = dot(row_bf16, (index == seq).astype(BF16))[:1]
        slot = slot[:1].astype(F32)
        return start + slot, slot < size

    def pack():
        shape = (c.lanes, c.rows)
        pos, live = rows_of(lax.div(iota(shape, 1), c.slots), lax.rem(iota(shape, 1), c.slots))
        s.into[...] = jnp.where((iota((c.packed, c.rows), 0).astype(F32) == pos) & live, 1.0, 0.0).astype(BF16)

    pack()

    def produce(l, j):
        at = slice((c.pairs - 1) * 2 * c.part, c.feat)
        if l:
            val = s.acc[j] + dot(s.scaled[:, at], s.w[l, j, at])
        else:
            wait_weights(l, j)
            val = dot(s.scaled[...], s.w[l, j])
        val = val.astype(BF16)
        s.x[l, j, 0] = val[:, : 2 * tile]
        s.x[l, j, 1] = val[:, 2 * tile :]
        first(l, j).start()

    def pack_rest():
        h = dot(s.into[...], flat())
        s.h[...] = h
        s.scaled[...] = (h * s.scaling[...].astype(F32)[:1]).astype(BF16)

    def produce_small(l):
        at = slice((c.pairs - 1) * 2 * c.part, c.feat)
        h = s.h[...]
        s.x_small[l, 0] = (s.acc_small[...] + narrow(s.scaled[:, at], s.wab[l, :, at])).astype(BF16)
        squares = jnp.sum(h * h, axis=1, keepdims=True)
        s.x_small[l, 1] = jnp.broadcast_to(squares, (c.packed, ab)).astype(BF16)
        first(l, -1).start()

    def bufs(l, j):
        if j < 0:
            return s.x_small.at[l], s.pair_small.at[l], s.sum_small.at[l], s.far_small.at[l], s.out_small.at[l], s.fin_small.at[l]
        return s.x.at[l, j], s.pair.at[l, j], s.sum.at[l, j], s.far.at[l, j], s.out.at[l, j], s.fin.at[l, j]

    def kind(j):
        return min(j + 1, 1)

    def first(l, j):
        x, pair, *_ = bufs(l, j)
        return remote(x.at[1 - core], pair, s.first_s.at[kind(j)], s.first_r.at[j + 1], "dp", partner)

    def second(l, j, d):
        _, _, own, far, *_ = bufs(l, j)
        there = pl.multiple_of(lax.div(others[d], 2) * c.per_chip, 16)
        return remote(
            own.at[pl.ds(there, c.chip_win)], far.at[d], s.second_s.at[kind(j), d], s.second_r.at[j + 1, d],
            "dp", others[d],
        )

    def third(l, j):
        *_, out, fin = bufs(l, j)
        return remote(out, fin.at[core], s.third_s.at[kind(j)], s.third_r.at[j + 1], "dp", partner)

    def cross(l, j):
        x, pair, own, *_ = bufs(l, j)
        first(l, j).wait_recv()
        own[...] = (x[core].astype(F32) + pair[...].astype(F32)).astype(BF16)
        for d in range(chips - 1):
            second(l, j, d).start()

    def finish(l, j):
        x, pair, own, far, out, fin = bufs(l, j)
        for d in range(chips - 1):
            second(l, j, d).wait_recv()

        def reduced(which):
            at = pl.multiple_of(which * c.own_seqs, 16)
            val = own[pl.ds(pl.multiple_of(chip * c.per_chip + at, 16), c.win), :].astype(F32)
            for d in range(chips - 1):
                val = val + far[d, pl.ds(at, c.win), :].astype(F32)
            return val.astype(BF16)

        out[...] = reduced(1 - core)
        third(l, j).start()
        fin[core] = reduced(core)

    def prepare(l):
        third(l, -1).wait_recv()
        pick = s.pick[...]
        heads = c.heads
        few = dot(pick[: c.own], s.fin_small[l, 0]).astype(BF16)
        squares = dot(pick, s.fin_small[l, 1])[:, :1]
        factor = lax.rsqrt(squares / (c.feat * n) + EPS)
        s.factor[...] = jnp.broadcast_to(factor, s.factor.shape)
        factor = factor[: c.own]
        at = iota((ab, heads), 1) + z * heads
        pa = dot(few, (iota((ab, heads), 0) == at).astype(BF16)) * factor
        pb = dot(few, (iota((ab, heads), 0) == at + all_heads).astype(BF16)) * factor
        arg = pa + s.bias[...][l : l + 1]
        soft = jnp.maximum(arg, 0.0) + jnp.log1p(jnp.exp(-jnp.abs(arg)))
        extra = jnp.concatenate([s.shrink[l, :, t, :] for t in range(c.slots)], axis=0)
        dec = jnp.exp(extra - jnp.exp(s.speed[...][l : l + 1]) * soft)
        dec = jnp.where(s.live[:, :1] > 0.0, dec, 1.0)
        wide = (iota((heads, c.cols), 0) == lax.div(iota((heads, c.cols), 1), c.size)).astype(BF16)
        both = jnp.concatenate([dec, jax.nn.sigmoid(pb)], axis=0)
        high = both.astype(BF16)
        low = (both - high.astype(F32)).astype(BF16)
        spread = dot(jnp.concatenate([high, low], axis=0), wide)
        s.dec[...] = spread[: c.own] + spread[2 * c.own : 3 * c.own]
        s.beta[...] = spread[c.own : 2 * c.own] + spread[3 * c.own :]

    def recur(l, j):
        at = slice(j * tile, (j + 1) * tile)
        third(l, j).wait_recv()
        pick = s.pick[...]
        factor = s.factor[:, :1]
        qk = dot(pick, s.fin[l, j, 0]) * factor
        vz = dot(pick[: c.own], s.fin[l, j, 1]) * factor[: c.own]
        qk = qk * jax.nn.sigmoid(qk)
        vz = vz * jax.nn.sigmoid(vz)
        q, k = qk[: c.own, :tile], qk[: c.own, tile:]
        v, zed = vz[:, :tile], vz[:, tile:]
        both = jnp.concatenate([qk[c.own :, tile:], qk[c.own :, :tile]], axis=0)
        low = iota((2 * c.own, 128), 1) < c.size
        copies = []
        for i in range(tile // 128):
            here = both[:, i * 128 : (i + 1) * 128]
            turned = pltpu.roll(here, c.size, 1)
            copies += [jnp.where(low, here, turned), jnp.where(low, turned, here)]
        heads = [jnp.concatenate([one.astype(BF16)] * (tile // 128), axis=1) for one in copies]
        batch = c.slots * c.per_tile
        lane_head = lax.div(iota((2 * batch, tile), 1), c.size)
        reads = []
        for g in range(c.groups):
            rows = [
                wide[start + g * batch : start + (g + 1) * batch] for wide in heads for start in (0, c.own)
            ]
            read = dot(jnp.concatenate(rows, axis=0) * s.mask[...], s.states16[l, g * tile : (g + 1) * tile, at])
            kept = read[: 2 * batch]
            for h in range(1, c.per_tile):
                kept = jnp.where(lane_head == h, read[2 * batch * h : 2 * batch * (h + 1)], kept)
            reads.append(kept)

        def read_step(first, t):
            rows = slice(first + t * c.per_tile, first + (t + 1) * c.per_tile)
            return jnp.concatenate([kept[rows] for kept in reads], axis=0)

        step = lambda x, t: x[t * c.own_seqs : (t + 1) * c.own_seqs]
        names, prods = [], []
        for t in range(c.slots):
            names.append(("n", t, t))
            prods.append(step(q, t) * step(q, t))
            for i in range(t + 1):
                names.append(("q", i, t))
                prods.append(step(k, i) * step(q, t))
                names.append(("k", i, t))
                prods.append(step(k, i) * step(k, t))
        pairs = dot(jnp.concatenate(prods, axis=0).astype(BF16), s.blocks[...])
        pairs = {name: step(pairs, i) for i, name in enumerate(names)}
        nk = [lax.rsqrt(pairs["k", t, t] + EPS) for t in range(c.slots)]
        nq = [lax.rsqrt(pairs["n", t, t] + EPS) * c.size ** (-0.5) for t in range(c.slots)]
        s.k[l, :, at] = (k * jnp.concatenate(nk, axis=0)).astype(BF16)
        dec = s.dec[:, at]
        beta = s.beta[:, at]
        fresh, outs = [], []
        whole = None
        for t in range(c.slots):
            g = step(dec, t)
            whole = g if whole is None else whole * g
            fresh = [(u * g) for u in fresh]
            guess = whole * read_step(0, t)
            for i in range(t):
                guess = guess + pairs["k", i, t] * nk[i] * fresh[i]
            fresh.append(step(beta, t) * (step(v, t) - guess * nk[t]))
            o = whole * read_step(batch, t)
            for i in range(t + 1):
                o = o + pairs["q", i, t] * nk[i] * fresh[i]
            outs.append(o * nq[t])
        s.u[l, :, at] = jnp.concatenate(fresh, axis=0).astype(BF16)
        s.decay[l, :, at] = whole
        o = jnp.concatenate(outs, axis=0)
        total = dot((o * o).astype(BF16), s.blocks[...])
        o = o * lax.rsqrt(total / c.size + EPS) * s.gain[l, :1] * zed
        s.y[l, me, j] = dot(s.place[...], o.astype(BF16)).astype(BF16)
        for peer in others + across_core + [partner]:
            here = s.y.at[l, me, j]
            remote(here, here, s.y_s.at[0], s.y_r.at[int(j + 1 == c.chunks)], "dp", peer).start()

    def wait_y(l, last):
        chunks = c.chunks - 1 if last else pl.ds(0, c.chunks - 1)
        every = s.y.at[l, pl.ds(0, n - 1), chunks]
        remote(every, every, s.y_s.at[0], s.y_r.at[int(last)], "dp", partner).wait_recv()

    def sent_all(l):
        if l:
            first(l, -1).wait_send()
        else:
            for j in range(-1, raws):
                raw_swap(j).wait_send()
        if l or c.chunks > raws:
            done = s.pair.at[l] if l else s.pair.at[l, pl.ds(raws, c.chunks - raws)]
            remote(done, done, s.first_s.at[1], s.first_r.at[0], "dp", partner).wait_send()
        for d in range(chips - 1):
            second(l, -1, d).wait_send()
            done = s.far.at[l, :, d]
            remote(done, done, s.second_s.at[1, d], s.second_r.at[0, d], "dp", others[d]).wait_send()
        third(l, -1).wait_send()
        done = s.out.at[l]
        remote(done, done, s.third_s.at[1], s.third_r.at[0], "dp", partner).wait_send()
        done = s.y.at[l, pl.ds(0, n - 1)]
        remote(done, done, s.y_s.at[0], s.y_r.at[0], "dp", partner).wait_send()

    def gather(l, j):
        at = slice(j * tile, (j + 1) * tile)
        s.gated[:, at] = jnp.zeros((c.packed, tile), BF16)
        for d in range(n):
            here = slice(d * c.own_seqs, d * c.own_seqs + c.win)
            s.gated[here, at] = s.gated[here, at] + s.y[l, d, j]

    def mix_some(l):
        before = slice(0, (c.chunks - 1) * tile)
        s.mixed[...] = dot(s.gated[:, before], s.wo[l, before])

    def mix_mul(l, run):
        per = c.parts // 2
        at = slice(run * per * c.part, (run + 1) * per * c.part)
        after = slice((c.chunks - 1) * tile, c.cols)
        val = dot(s.gated[:, after], s.wo[l, after, at])
        if c.chunks > 1:
            val = val + s.mixed[:, at]
        val = val.astype(BF16)
        for i in range(per):
            s.sent[l, run * per + i] = val[:, i * c.part : (i + 1) * c.part]
        for i in range(per):
            lines[l].start(run * per + i)

    lead = 5
    early_takes = c.parts - lead if c.direct else 0
    early_takes = min(early_takes, c.parts - c.direct)

    def mix_out(l, p):
        lines[l].relay(p)
        if 0 <= p - lead < early_takes:
            lines[l].take(p - lead)

    def mix_in(l, p):
        if not p < early_takes:
            lines[l].take(p)
        at = slice(p * c.part, (p + 1) * c.part)
        mixed = (s.h[:, at] + s.full[l, p].astype(F32)).astype(BF16)
        s.scaled[:, at] = mixed
        if l + 1 < BLOCKS:
            mixed = mixed.astype(F32)
            s.h[:, at] = mixed
            s.scaled[:, at] = (mixed * s.scaling[...].astype(F32)[l + 1 : l + 2, at]).astype(BF16)

    def place_tokens(p):
        at = slice((p - 1) * c.part, (p + 1) * c.part)
        back = dot(s.hot[...], s.scaled[:, at])
        kept = s.resid[:, :, at].reshape(c.rows, 2 * c.part).astype(F32)
        mixed = jnp.where(s.alive[:, :1] > 0.0, back, kept).astype(BF16)
        tokens[:, :, at] = mixed.reshape(c.seqs, c.slots, 2 * c.part)

    def setup():
        r = iota((2 * c.own, c.lanes), 0)
        again = r - c.own
        few = lax.rem(again, c.per_tile) + lax.div(again, c.slots * c.per_tile) * c.per_tile
        seq = jnp.where(r < c.own, lax.rem(r, c.own_seqs), few)
        slot = jnp.where(r < c.own, lax.div(r, c.own_seqs), lax.rem(lax.div(again, c.per_tile), c.slots))
        pos, live = columns(2 * c.own, seq + me * c.own_seqs, slot)
        offset = (iota((2 * c.own, c.win), 1) + me * c.own_seqs).astype(F32)
        s.pick[...] = jnp.where((offset == pos) & live, 1.0, 0.0).astype(BF16)
        s.live[...] = jnp.broadcast_to(jnp.where(live, 1.0, 0.0)[: c.own], s.live.shape)
        shape = (c.lanes, c.own)
        pos, live = rows_of(
            lax.rem(iota(shape, 1), c.own_seqs) + me * c.own_seqs, lax.div(iota(shape, 1), c.own_seqs)
        )
        offset = (iota((c.win, c.own), 0) + me * c.own_seqs).astype(F32)
        s.place[...] = jnp.where((offset == pos) & live, 1.0, 0.0).astype(BF16)
        r = iota((c.rows, c.lanes), 0)
        pos, live = columns(c.rows, lax.div(r, c.slots), lax.rem(r, c.slots))
        offset = iota((c.rows, c.packed), 1).astype(F32)
        s.alive[...] = jnp.broadcast_to(jnp.where(live, 1.0, 0.0), s.alive.shape)
        s.hot[...] = jnp.where((offset == pos) & live, 1.0, 0.0).astype(BF16)
        fold = (iota((c.size, tile), 0) == lax.rem(iota((c.size, tile), 1), c.size)).astype(BF16)
        for l in range(BLOCKS):
            channels = jnp.broadcast_to(s.channel[...].astype(F32)[l : l + 1], (8, c.size)).astype(BF16)
            s.gain[l] = dot(channels, fold)

    def write_states(l, j):
        at = slice(j * tile, (j + 1) * tile)
        shape = (c.per_tile * c.own, tile)
        same = (lax.div(iota(shape, 0), c.own) == lax.div(iota(shape, 1), c.size)).astype(BF16)
        fold = (iota((c.size, tile), 0) == lax.rem(iota((c.size, tile), 1), c.size)).astype(BF16)
        keys = lax.dot_general(
            fold, tiles(s.k[l, :, at], c.per_tile) * same, (((1,), (1,)), ((), ())), preferred_element_type=F32
        ).astype(BF16)
        fresh = tiles(s.u[l, :, at], c.per_tile) * same
        owner = lax.rem(iota((c.size, c.per_tile * c.own), 1), c.own_seqs)
        batch = 4
        for first_seq in range(0, c.own_seqs, batch):
            lhs = jnp.concatenate(
                [keys * (owner == first_seq + i).astype(BF16) for i in range(batch)], axis=0
            )
            added = dot(lhs, fresh)
            for i in range(batch):
                seq = first_seq + i
                new[l, seq, :, at] = (
                    new[l, seq, :, at] * s.decay[l, seq : seq + 1, at] + added[i * c.size : (i + 1) * c.size]
                )

    def round_states(l):
        state_loads[l].wait()
        for i in range(c.own_seqs):
            s.states16[l, i * c.size : (i + 1) * c.size] = new[l, i].astype(BF16)

    for l in range(BLOCKS):
        if l:
            for j in range(c.chunks):
                wait_weights(l, j)
            for p in range(c.parts):
                mix_in(l - 1, p)
                if p % 2 and p + 1 < c.parts:
                    at = slice((p - 1) * c.part, (p + 1) * c.part)
                    piece = s.scaled[:, at]
                    for j in range(c.chunks):
                        val = dot(piece, s.w[l, j, at])
                        s.acc[j] = val if p == 1 else s.acc[j] + val
                    val = narrow(piece, s.wab[l, :, at])
                    s.acc_small[...] = val if p == 1 else s.acc_small[...] + val
        if l:
            produce_small(l)
            for j in range(c.chunks):
                produce(l, j)
                if j:
                    cross(l, j - 2)
            for j in range(c.chunks - 2, c.chunks):
                cross(l, j)
        else:
            for j in range(-1, raws):
                raw_cross(j)
            pack_rest()
            for j in range(raws, c.chunks):
                produce(l, j)
            for copy in late:
                copy.wait()
            setup()
            round_states(0)
            for j in range(raws, c.chunks):
                if j + 1 == c.chunks:
                    finish(l, -1)
                cross(l, j)
            if c.chunks == raws:
                finish(l, -1)
        if l == 0:
            for j in range(c.chunks):
                load_weights(1, j)
            load_rest(1)
        else:
            finish(l, -1)
        finish(l, 0)
        prepare(l)
        for j in range(1, c.chunks):
            finish(l, j)
            recur(l, j - 1)
        recur(l, c.chunks - 1)
        for j in range(c.chunks - 1):
            write_states(l, j)
        wo_loads[l].wait()
        if c.chunks > 1:
            wait_y(l, False)
            for j in range(c.chunks - 1):
                gather(l, j)
            mix_some(l)
        wait_y(l, True)
        gather(l, c.chunks - 1)
        mix_mul(l, 0)
        mix_mul(l, 1)
        write_states(l, c.chunks - 1)
        if l == 0:
            round_states(1)
        if l:
            lines[l - 1].end()
        for p in range(c.parts):
            mix_out(l, p)
        sent_all(l)
    for p in range(c.parts):
        mix_in(BLOCKS - 1, p)
        if p % 2:
            place_tokens(p)
    lines[BLOCKS - 1].end()


def run_main(c, args):
    ab = 2 * args[6].shape[1]
    half = 2 * c.tile
    chips, n = c.chips, c.n
    dma = lambda *shape: pltpu.SemaphoreType.DMA(shape)
    buf = lambda *shape: pltpu.VMEM(shape, BF16)
    wide = lambda *shape: pltpu.VMEM(shape, F32)
    every = 1 + c.chunks
    scratch = dict(
        resid=buf(c.seqs, c.slots, c.feat),
        k=buf(BLOCKS, c.own, c.cols),
        u=buf(BLOCKS, c.own, c.cols),
        decay=wide(BLOCKS, c.own_seqs, c.cols),
        scaling=buf(BLOCKS, c.feat),
        wab=buf(BLOCKS, ab, c.feat),
        speed=wide(BLOCKS, c.heads),
        bias=wide(BLOCKS, c.heads),
        channel=buf(BLOCKS, c.size),
        shrink=wide(BLOCKS, c.own_seqs, c.slots, c.heads),
        w=buf(BLOCKS, c.chunks, c.feat, 4 * c.tile),
        raw=buf(min(2, c.chunks), 2, c.rows, half),
        raw_small=buf(2, c.rows, ab),
        raw_pair=buf(min(2, c.chunks), c.rows, half),
        raw_pair_small=buf(c.rows, ab),
        hot=buf(c.rows, c.packed),
        alive=wide(c.rows, 128),
        **{name: buf(BLOCKS, c.parts, c.packed, c.part) for name in ("sent", "mid", "came", "over", "full")},
        bent=buf(c.rows, c.feat),
        into=buf(c.packed, c.rows),
        wo=buf(BLOCKS, c.cols, c.feat),
        states16=buf(BLOCKS, c.own_seqs * c.size, c.cols),
        counts=pltpu.VMEM((n, 8, c.lanes), jnp.int32),
        blocks=buf(c.tile, c.tile),
        mask=buf(c.per_tile * 2 * c.slots * c.per_tile, c.tile),
        gain=wide(BLOCKS, 8, c.tile),
        pick=buf(2 * c.own, c.win),
        place=buf(c.win, c.own),
        live=wide(c.own, 128),
        factor=wide(2 * c.own, 128),
        dec=wide(c.own, c.cols),
        beta=wide(c.own, c.cols),
        h=wide(c.packed, c.feat),
        scaled=buf(c.packed, c.feat),
        acc=wide(c.chunks, c.packed, 4 * c.tile),
        acc_small=wide(c.packed, ab),
        x=buf(BLOCKS, c.chunks, 2, c.packed, half),
        pair=buf(BLOCKS, c.chunks, c.packed, half),
        sum=buf(BLOCKS, c.chunks, c.packed, half),
        far=buf(BLOCKS, c.chunks, chips - 1, c.chip_win, half),
        out=buf(BLOCKS, c.chunks, c.win, half),
        fin=buf(BLOCKS, c.chunks, 2, c.win, half),
        x_small=buf(BLOCKS, 2, c.packed, ab),
        pair_small=buf(BLOCKS, c.packed, ab),
        sum_small=buf(BLOCKS, c.packed, ab),
        far_small=buf(BLOCKS, chips - 1, c.chip_win, ab),
        out_small=buf(BLOCKS, c.win, ab),
        fin_small=buf(BLOCKS, 2, c.win, ab),
        y=buf(BLOCKS, n, c.chunks, c.win, c.tile),
        gated=buf(c.packed, c.cols),
        mixed=wide(c.packed, c.feat),
        own_counts=pltpu.SMEM((c.own_seqs,), jnp.int32),
        small_sem=dma(9),
        w_sem=dma(c.chunks),
        wo_sem=dma(BLOCKS),
        state_sem=dma(BLOCKS),
        count_sem=dma(2),
        raw_s=dma(1 + min(2, c.chunks)),
        first_s=dma(2),
        first_r=dma(every),
        second_s=dma(2, chips - 1),
        second_r=dma(every, chips - 1),
        third_s=dma(2),
        third_r=dma(every),
        y_s=dma(1),
        y_r=dma(2),
        line_s=dma(4),
        early_r=dma(BLOCKS),
        in_r=dma(c.parts),
        full_r=dma(c.parts - c.direct),
        over_r=dma(BLOCKS, c.parts),
    )
    c.names = list(scratch)
    return pl.pallas_call(
        functools.partial(main_kernel, c),
        out_shape=[
            pltpu.VMEM(args[1].shape, BF16),
            pltpu.VMEM(args[-1].shape, F32),
        ],
        in_specs=[HBM] * 15,
        out_specs=[VMEM] * 2,
        scratch_shapes=list(scratch.values()),
        compiler_params=pltpu.CompilerParams(
            collective_id=1, has_side_effects=True, vmem_limit_bytes=46 * 1024 * 1024
        ),
        name="blocks",
    )(*[pltpu.with_memory_space_constraint(x, pltpu.HBM) for x in args])


def store_kernel(pieces, tokens, new, tokens_out, new_out, sem):
    copies = [pltpu.make_async_copy(tokens, tokens_out, sem.at[pieces])]
    size = new.shape[1] * new.shape[0] // pieces
    for i in range(pieces):
        l, at = divmod(i * size, new.shape[1])
        at = pl.ds(at, size)
        copies.append(pltpu.make_async_copy(new.at[l, at], new_out.at[l, at], sem.at[i]))
    for copy in copies:
        copy.start()
    for copy in copies:
        copy.wait()


def store(tokens, new):
    pieces = 8
    return pl.pallas_call(
        functools.partial(store_kernel, pieces),
        out_shape=[jax.ShapeDtypeStruct(a.shape, a.dtype) for a in (tokens, new)],
        in_specs=[VMEM] * 2,
        out_specs=[HBM] * 2,
        scratch_shapes=[pltpu.SemaphoreType.DMA((pieces + 1,))],
        compiler_params=pltpu.CompilerParams(vmem_limit_bytes=1024 * 1024),
        name="store",
    )(tokens, new)


def body(
    n, m, resid, counts, wq, wk, wv, wz, wa, wb, wo, speed, bias, scaling, channel, shrink, states,
):
    c = sizes(n, m, resid, counts, wq, speed)
    turned = [jnp.swapaxes(w, 1, 2) for w in (wa, wb)]
    tokens, new = run_main(
        c, (counts, resid, wq, wk, wv, wz, *turned, wo, speed, bias, scaling, channel, shrink, states)
    )
    return store(tokens, new)


def solution(mesh):
    in_specs = (
        P("grp", None, "dp"),
        P(("grp", "dp")),
        P(None, "dp", "tp"),
        P(None, "dp", "tp"),
        P(None, "dp", "tp"),
        P(None, "dp", "tp"),
        P(),
        P(),
        P(None, "tp", "dp"),
        P(None, "tp"),
        P(None, "tp"),
        P(None, "dp"),
        P(),
        P(None, ("grp", "dp"), None, "tp"),
        P(None, ("grp", "dp"), None, "tp"),
    )
    out_specs = (P("grp", None, "dp"), P(None, ("grp", "dp"), None, "tp"))
    run = functools.partial(body, mesh.shape["dp"], mesh.shape["tp"])
    return jax.shard_map(run, mesh=mesh, in_specs=in_specs, out_specs=out_specs, check_vma=False)
```
